32 devices in a mesh: grp: 2 (over y), sp: 4 (over z), tp: 4 (over x, core).
Axes of the slice: x: 2, y: 2, z: 4, core: 2. Of those that a mesh axis runs over, the one named last changes fastest.
Arguments:
- tokens: bfloat16 [2048, 4096], P(('grp', 'sp')), parts along dimension 0, may hold values from -6 to 6
- norm_gain: bfloat16 [2, 4096], replicated, may hold values from 0.099609375 to 1.8984375
- w_query: bfloat16 [2, 4096, 2048], P(None, 'sp', 'tp'), may hold values from -0.09375 to 0.09375
- w_key: bfloat16 [2, 4096, 2048], P(None, 'sp', 'tp'), may hold values from -0.09375 to 0.09375
- w_value: bfloat16 [2, 4096, 2048], P(None, 'sp', 'tp'), may hold values from -0.09375 to 0.09375
- w_out: bfloat16 [2, 2048, 4096], P(None, 'tp', 'sp'), may hold values from -0.125 to 0.125
- offset_bias: float32 [2, 16, 15, 31], P(None, 'tp'), may hold values from -4 to 300
Outputs:
- mixed: bfloat16 [2048, 4096], P(('grp', 'sp')), parts along dimension 0
The draws below stay inside these ranges and needn't reach their ends.
There are 2 independent parts, one for each index of `grp`. The reference program is written for one: setup_inputs(seed, part) draws one part's arguments, and reference() takes and returns one part's arrays. A program takes and returns all parts, laid end to end along the dimension named above; an argument that names none is the same for every part. Nothing has to cross between parts.
All inputs are finite; a program needn't handle non-finite values.
Results may differ from the reference program's by a relative error of at most 0.013.
Values may be sent and summed in bfloat16 or wider, within the bound.
A program may use at most 128 MiB of HBM per device.

```python
import jax
import jax.numpy as jnp
from jax import lax

D = 4096
HEADS = 16
HD = 128
GRID_W = 64
KR = 8
KC = 16
LAYERS = 2
ROWS_DEV = 4
TOKENS = 1024
N_SP = 4
N_TP = 4


def draw_offset_bias(key, part):
    shape = (LAYERS, HEADS, 2 * KR - 1, 2 * KC - 1)
    first_key, second_key = jax.random.split(jax.random.fold_in(key, 17))
    base = jnp.clip(jax.random.normal(first_key, shape, jnp.float32), -4.0, 4.0)
    return base


def steps_of(key, shape, shards, least, largest):
    factor_of, own = 1.0, jax.random.fold_in(key, 6)
    for position, parts in shards:
        heights = jnp.exp(jax.random.uniform(jax.random.fold_in(own, position), (parts,), jnp.float32, least / len(shards), largest / len(shards)))
        factor_of = factor_of * jnp.repeat(heights, shape[position] // parts).reshape([-1 if axis == position else 1 for axis in range(len(shape))])
    return factor_of


def scatter_about(own_key, dims, scale, most, pieces=(), kind=jnp.bfloat16):
    values = jax.random.normal(own_key, dims, jnp.float32) * scale
    if len(pieces) > 0:
        values = steps_of(own_key, dims, pieces, -0.22, 0.18) * values
    return jnp.clip(values, min=-most, max=most).astype(kind)


def setup_inputs(seed: int = 0, part: int = 0) -> dict:
    key_list = jax.random.split(jax.random.key(seed), 8)
    part_keys = jax.random.split(jax.random.fold_in(key_list[7], part), 8)
    tokens = scatter_about(part_keys[0], (TOKENS, D), 1.0, 6.0, ((0, 4),))
    norm_gain = jnp.clip(1.0 + 0.18 * jax.random.normal(key_list[1], (LAYERS, D), jnp.float32), 0.099609375, 1.8984375).astype(jnp.bfloat16)
    w_query = scatter_about(key_list[2], (LAYERS, D, HEADS * HD), D ** -0.5, 0.09375, ((1, 4), (2, 4)))
    w_key = scatter_about(key_list[3], (LAYERS, D, HEADS * HD), D ** -0.5, 0.09375, ((1, 4), (2, 4)))
    w_value = scatter_about(key_list[4], (LAYERS, D, HEADS * HD), D ** -0.5, 0.09375, ((1, 4), (2, 4)))
    w_out = scatter_about(key_list[5], (LAYERS, HEADS * HD, D), (HEADS * HD) ** -0.5, 0.125, ((1, 4), (2, 4)))
    offset_bias = draw_offset_bias(jax.random.fold_in(key_list[7], 71), part)
    return dict(tokens=tokens, norm_gain=norm_gain, w_query=w_query, w_key=w_key, w_value=w_value, w_out=w_out, offset_bias=offset_bias)


norm_eps = 1e-06

def rms_rows(values, gain):
    wide = values.astype(jnp.float32)
    scaled = wide * lax.rsqrt(lax.optimization_barrier(jnp.mean(wide * wide, axis=-1, keepdims=True)) + norm_eps)
    return (scaled * gain.astype(jnp.float32)).astype(jnp.bfloat16)

def reference(tokens, norm_gain, w_query, w_key, w_value, w_out, offset_bias):
    grid_rows = ROWS_DEV * N_SP
    group_width = HEADS // N_TP * HD
    scale = HD ** (-0.5)
    columns = jnp.arange(GRID_W, dtype=jnp.int32)
    col_first = jnp.clip(columns - KC // 2, 0, GRID_W - KC)
    col_inside = (columns[None, :] >= col_first[:, None]) & (columns[None, :] < col_first[:, None] + KC)
    col_offset = jnp.clip(columns[None, :] - columns[:, None], 1 - KC, KC - 1) + KC - 1
    row_first = jnp.clip(jnp.arange(grid_rows, dtype=jnp.int32) - KR // 2, 0, grid_rows - KR)
    residual = tokens
    for layer_index in range(LAYERS):
        normed = rms_rows(residual, norm_gain[layer_index])
        queries = jnp.dot(normed, w_query[layer_index], preferred_element_type=jnp.float32).astype(jnp.bfloat16)
        keys = jnp.dot(normed, w_key[layer_index], preferred_element_type=jnp.float32).astype(jnp.bfloat16)
        values = jnp.dot(normed, w_value[layer_index], preferred_element_type=jnp.float32).astype(jnp.bfloat16)
        queries = queries.reshape(grid_rows, GRID_W, HEADS, HD)
        keys = keys.reshape(grid_rows, GRID_W, HEADS, HD)
        values = values.reshape(grid_rows, GRID_W, HEADS, HD)
        col_bias = offset_bias[layer_index].astype(jnp.float32)[:, :, col_offset]

        def attend_row(packed, keys=keys, values=values, col_bias=col_bias):
            row_index, row_queries = packed
            row_begin = row_first[row_index].astype(jnp.int32)
            row_keys = lax.dynamic_slice_in_dim(keys, row_begin, KR, 0).astype(jnp.float32)
            row_values = lax.dynamic_slice_in_dim(values, row_begin, KR, 0).astype(jnp.float32)
            picked = row_begin + jnp.arange(KR, dtype=jnp.int32) - row_index + KR - 1
            bias = jnp.transpose(col_bias[:, picked], (0, 2, 1, 3))
            scores = jnp.einsum('qhd,jkhd->hqjk', row_queries.astype(jnp.float32), row_keys) * scale + bias
            scores = jnp.where(col_inside[None, :, None, :], scores, -jnp.inf)
            weights = jax.nn.softmax(scores.reshape(HEADS, GRID_W, KR * GRID_W), axis=-1).astype(jnp.bfloat16)
            weights = lax.optimization_barrier(weights)
            weights = weights.reshape(HEADS, GRID_W, KR, GRID_W).astype(jnp.float32)
            return jnp.einsum('hqjk,jkhd->qhd', weights, row_values).astype(jnp.bfloat16)
        attended = lax.map(attend_row, (jnp.arange(grid_rows, dtype=jnp.int32), queries))
        attended = attended.reshape(grid_rows * GRID_W, HEADS * HD)
        branch = jnp.zeros(residual.shape, jnp.float32)
        for group_index in range(N_TP):
            lower = group_index * group_width
            rounded = jnp.dot(attended[:, lower:lower + group_width], w_out[layer_index][lower:lower + group_width], preferred_element_type=jnp.float32).astype(jnp.bfloat16)
            branch = branch + lax.optimization_barrier(rounded).astype(jnp.float32)
        residual = (residual.astype(jnp.float32) + branch).astype(jnp.bfloat16)
    return residual
```

```python
import functools

import jax
import jax.numpy as jnp
from jax import lax
from jax.experimental import pallas as pl
from jax.experimental.pallas import tpu as pltpu
from jax.sharding import PartitionSpec as P

HD = 128
GRID_W = 64
KR = 8
KC = 16
LAYERS = 2


norm_eps = 1e-06


def with_halo(block, sides, width):
    for axis, dim in sides:
        count = lax.axis_size(axis)
        forward = [(i, i + 1) for i in range(count - 1)]
        backward = [(target, source) for source, target in forward]
        low = lax.ppermute(
            lax.slice_in_dim(block, block.shape[dim] - width, None, axis=dim), axis, forward
        )
        high = lax.ppermute(lax.slice_in_dim(block, 0, width, axis=dim), axis, backward)
        block = jnp.concatenate([low, block, high], axis=dim)
    return block


def rms_rows(values, gain):
    wide = values.astype(jnp.float32)
    scaled = wide * lax.rsqrt(jnp.mean(wide * wide, axis=-1, keepdims=True) + norm_eps)
    return (scaled * gain.astype(jnp.float32)).astype(jnp.bfloat16)


def general(tokens, norm_gain, w_query, w_key, w_value, w_out, offset_bias):
    sp_count = lax.axis_size("sp")
    sp_index = lax.axis_index("sp")
    tok_rows = tokens.shape[0]
    local_rows = tok_rows // GRID_W
    grid_rows = local_rows * sp_count
    heads_here = offset_bias.shape[1]
    head_width = heads_here * HD
    reach = KR // 2
    scale = HD ** (-0.5)
    columns = jnp.arange(GRID_W, dtype=jnp.int32)
    col_first = jnp.clip(columns - KC // 2, 0, GRID_W - KC)
    col_inside = (columns[None, :] >= col_first[:, None]) & (
        columns[None, :] < col_first[:, None] + KC
    )
    col_offset = jnp.clip(columns[None, :] - columns[:, None], 1 - KC, KC - 1) + KC - 1
    col_onehot = (
        jnp.arange(2 * KC - 1, dtype=jnp.int32)[:, None, None] == col_offset[None, :, :]
    ).astype(jnp.float32)
    first_row = sp_index * local_rows
    own_rows = first_row + jnp.arange(local_rows, dtype=jnp.int32)
    row_first = jnp.clip(own_rows - reach, 0, grid_rows - KR)
    band_start = row_first - first_row + reach
    row_offset = (
        row_first[:, None] + jnp.arange(KR, dtype=jnp.int32)[None, :] - own_rows[:, None] + KR - 1
    )
    row_onehot = (
        row_offset[:, :, None] == jnp.arange(2 * KR - 1, dtype=jnp.int32)[None, None, :]
    ).astype(jnp.float32)
    qkv_weight = jnp.concatenate([w_query, w_key, w_value], axis=2)
    residual = lax.all_to_all(tokens, "sp", split_axis=1, concat_axis=0, tiled=True)
    width = residual.shape[1]
    features = width * sp_count
    for layer_index in range(LAYERS):
        wide = residual.astype(jnp.float32)
        squares = lax.psum_scatter(
            jnp.sum(wide * wide, axis=-1, keepdims=True), "sp", scatter_dimension=0, tiled=True
        )
        inverse = lax.rsqrt(squares / features + norm_eps)
        gain = lax.dynamic_slice_in_dim(norm_gain[layer_index], sp_index * width, width, 0)
        gained = (wide * gain.astype(jnp.float32)).astype(jnp.bfloat16)
        partial = jnp.dot(gained, qkv_weight[layer_index], preferred_element_type=jnp.float32)
        mine = lax.psum_scatter(
            partial.astype(jnp.bfloat16), "sp", scatter_dimension=0, tiled=True
        )
        mine = (mine.astype(jnp.float32) * inverse).astype(jnp.bfloat16)
        queries = mine[:, :head_width].reshape(local_rows, GRID_W, heads_here, HD)
        key_values = mine[:, head_width:].reshape(local_rows, GRID_W, 2 * head_width)
        padded = with_halo(key_values, (("sp", 0),), reach)
        bands = jax.vmap(lambda band_begin: lax.dynamic_slice_in_dim(padded, band_begin, KR, 0))(
            band_start
        )
        band_keys = bands[..., :head_width].reshape(local_rows, KR, GRID_W, heads_here, HD)
        band_values = bands[..., head_width:].reshape(local_rows, KR, GRID_W, heads_here, HD)
        col_bias = jnp.einsum(
            "hro,oqk->hrqk", offset_bias[layer_index], col_onehot, precision=lax.Precision.HIGHEST
        )
        full_bias = jnp.einsum(
            "ijr,hrqk->hiqjk", row_onehot, col_bias, precision=lax.Precision.HIGHEST
        )
        scores = jnp.einsum(
            "iqhd,ijkhd->hiqjk", queries, band_keys, preferred_element_type=jnp.float32
        )
        scores = scores * scale + full_bias
        scores = jnp.where(col_inside[None, None, :, None, :], scores, -jnp.inf)
        flattened = scores.reshape(heads_here, local_rows, GRID_W, KR * GRID_W)
        weights = jax.nn.softmax(flattened, axis=-1).astype(jnp.bfloat16)
        weights = weights.reshape(heads_here, local_rows, GRID_W, KR, GRID_W)
        attended = jnp.einsum(
            "hiqjk,ijkhd->iqhd", weights, band_values, preferred_element_type=jnp.float32
        )
        attended = attended.astype(jnp.bfloat16).reshape(tok_rows, head_width)
        every = lax.all_gather(attended, "sp", axis=0, tiled=True)
        share = jnp.dot(every, w_out[layer_index], preferred_element_type=jnp.float32)
        branch = lax.psum(share.astype(jnp.bfloat16), "tp").astype(jnp.float32)
        residual = (residual.astype(jnp.float32) + branch).astype(jnp.bfloat16)
    return lax.all_to_all(residual, "sp", split_axis=0, concat_axis=1, tiled=True)


MESH = pl.DeviceIdType.MESH
VMEM_MOST = 63 * 2**20
CHUNK = GRID_W
HOP = 2
LEAD = 4


def greet(peers):
    barrier = pltpu.get_barrier_semaphore()
    for axis, index in peers:
        pl.semaphore_signal(barrier, inc=1, device_id={axis: index}, device_id_type=MESH)
    pl.semaphore_wait(barrier, len(peers))


def remote(src, dst, send, recv, axis, index):
    return pltpu.make_async_remote_copy(
        src_ref=src, dst_ref=dst, send_sem=send, recv_sem=recv,
        device_id={axis: index}, device_id_type=MESH,
    )


def span(start, size):
    return pl.ds(pl.multiple_of(start, size), size)


def row_plan(count, last):
    if not last:
        return [(r, 1) for r in range(count)]
    need = [min(max(r + KR - 1 - KR // 2, KR - 1), count - 1) - KR + 1 for r in range(count)]
    plan, done = [], 0
    for tick in range(need[-1] + 1):
        ready = sum(v <= tick for v in need) - done
        take = ready if tick == need[-1] else min(ready, 2)
        plan.append((done, take))
        done += take
    return plan


def pick(table, index):
    value = jnp.int32(table[-1])
    for i in range(len(table) - 2, -1, -1):
        value = jnp.where(index <= i, jnp.int32(table[i]), value)
    return value


def pipeline_kernel(
    n, m, tok_ref, gain_ref, base_ref, wq_any, wk_any, wv_any, wo_any, out_ref,
    wq, wk, wv, wo, xs, part, outbox, inbox, qkv, bias, sq_own, sq_in, box,
    give, take, pair, cross_in, fin,
    w_sem, sp_s, sp_r, spx_s, spx_r, fresh_s, fresh_r, ch_s, ch_r, sq_s, sq_r,
    at_s, at_r, gv_s, gv_r, cr_s, cr_r, fin_s, fin_r, fx_s, fx_r, fp_s, fp_r,
):
    me, t = lax.axis_index("sp"), lax.axis_index("tp")
    core = lax.rem(t, 2)
    side = lax.div(t, 2)
    partner = t + 1 - 2 * core
    cross = lax.rem(t + m // 2, m)
    layers, tokens, width = xs.shape
    own, features = tok_ref.shape
    cols = box.shape[3]
    heads = cols // HD
    half, quarter = width // 2, width // 4
    count, per = tokens // CHUNK, own // CHUNK
    scale = HD ** (-0.5)
    at_end = (me == 0) | (me == n - 1)
    ends = (n - 1, 0)
    lanes = span(core * half, half)
    other = span((1 - core) * half, half)
    mine_q = core * half + side * quarter
    their_q = core * half + (1 - side) * quarter
    places = (me, n - 1 - me)
    afters = (me + 1, me - 1)

    weights = []
    for layer in range(layers):
        for i, (any_ref, ref) in enumerate(((wq_any, wq), (wk_any, wk), (wv_any, wv), (wo_any, wo))):
            copy = pltpu.make_async_copy(any_ref.at[layer], ref.at[layer], w_sem.at[layer, i])
            copy.start()
            weights.append(copy)
    greet(
        [("sp", lax.rem(me + k, n)) for k in range(1, n)] + [("tp", partner), ("tp", cross)]
    )

    def rows_of(c):
        return span(c * CHUNK, CHUNK)

    def scatter(c):
        @pl.when(lax.div(c, per) == me)
        def _():
            here = span((c - me * per) * CHUNK, CHUNK)
            for k in range(1, n):
                to = lax.rem(me + k, n)
                remote(
                    tok_ref.at[here, span(to * width + mine_q, quarter)],
                    xs.at[0, rows_of(c), span(mine_q, quarter)],
                    sp_s, sp_r.at[c], "sp", to,
                ).start()
            xs[0, rows_of(c), :] = tok_ref[here, span(me * width, width)]

    def pass_cross(c):
        @pl.when(lax.div(c, per) != me)
        def _():
            here = xs.at[0, rows_of(c), span(mine_q, quarter)]
            remote(here, here, sp_s, sp_r.at[c], "tp", cross).wait_recv()
            remote(here, here, spx_s, spx_r.at[c], "tp", cross).start()

    def pass_partner(c):
        @pl.when(lax.div(c, per) != me)
        def _():
            there = xs.at[0, rows_of(c), span(their_q, quarter)]
            remote(there, there, spx_s, spx_r.at[c], "tp", cross).wait_recv()
            here = xs.at[0, rows_of(c), lanes]
            remote(here, here, fresh_s.at[0], fresh_r.at[0, c], "tp", partner).start()

    def prepare(layer, c):
        rows = rows_of(c)

        def arrived():
            there = xs.at[layer, rows, other]
            remote(there, there, fresh_s.at[layer], fresh_r.at[layer, c], "tp", partner).wait_recv()

        if layer == 0:
            pl.when(lax.div(c, per) != me)(arrived)
        else:
            arrived()
        gain = gain_ref[layer:layer + 1, span(me * width, width)].astype(jnp.float32)
        wide = xs[layer, rows, :].astype(jnp.float32)
        gained = (wide * gain).astype(jnp.bfloat16)
        for way in range(2):
            lo = (1 - way) * cols
            for j, w_ref in enumerate((wq, wk, wv)):
                part[way, rows, j * cols:(j + 1) * cols] = jnp.dot(
                    gained, w_ref[layer, :, lo:lo + cols], preferred_element_type=jnp.float32
                )
        squares = wide * wide
        high = squares.astype(jnp.bfloat16)
        low = (squares - high.astype(jnp.float32)).astype(jnp.bfloat16)
        ones = jnp.ones((8, width), jnp.bfloat16)
        nt = (((1,), (1,)), ((), ()))
        total = lax.dot_general(
            ones, high, nt, preferred_element_type=jnp.float32
        ) + lax.dot_general(ones, low, nt, preferred_element_type=jnp.float32)
        sq_own[layer, c] = jnp.concatenate([total] * (128 // CHUNK), axis=1)
        for e, end in enumerate(ends):
            @pl.when(me != end)
            def _(e=e, end=end):
                remote(
                    sq_own.at[layer, c], sq_in.at[layer, me, c],
                    sq_s.at[layer, e], sq_r.at[layer, me, c], "sp", end,
                ).start()

    def chain_copy(layer, way, c):
        rows = rows_of(c)
        return remote(
            outbox.at[layer, way, rows, :], inbox.at[layer, way, rows, :],
            ch_s.at[layer, way], ch_r.at[layer, way, c], "sp", afters[way],
        )

    def first_link(layer, c):
        for way in range(2):
            @pl.when(places[way] == 0)
            def _(way=way):
                outbox[layer, way, rows_of(c), :] = part[way, rows_of(c), :].astype(jnp.bfloat16)
                chain_copy(layer, way, c).start()

    def link(way, layer, c):
        rows = rows_of(c)
        place = places[way]
        chain_copy(layer, way, c).wait_recv()

        def total():
            return part[way, rows, :] + inbox[layer, way, rows, :].astype(jnp.float32)

        @pl.when(place < n - 1)
        def _():
            outbox[layer, way, rows, :] = total().astype(jnp.bfloat16)
            chain_copy(layer, way, c).start()

        @pl.when(place == n - 1)
        def _():
            squares = sq_own[layer, c]
            for k in range(1, n):
                source = lax.rem(me + k, n)
                remote(
                    sq_own.at[layer, c], sq_in.at[layer, source, c],
                    sq_s.at[layer, 0], sq_r.at[layer, source, c], "sp", source,
                ).wait_recv()
                squares = squares + sq_in[layer, source, c]
            scaled = lax.rsqrt(squares / features + norm_eps)
            inverse = jnp.concatenate([scaled] * 16, axis=0).T[:CHUNK, :1]
            qkv[layer, rows, :] = (total() * inverse).astype(jnp.bfloat16)

    def make_bias():
        first_head = jnp.where(me == n - 1, heads, 0)
        lane = lax.broadcasted_iota(jnp.int32, (CHUNK, 2 * GRID_W), 1)
        query = lax.broadcasted_iota(jnp.int32, (CHUNK, 2 * GRID_W), 0)
        key = jnp.where(lane < GRID_W, lane, lane - GRID_W)
        begin = jnp.clip(query - KC // 2, 0, GRID_W - KC)
        inside = (key >= begin) & (key < begin + KC)
        for layer in range(layers):
            for h in range(heads):
                @pl.loop(0, 2 * KR - 2)
                def _(o):
                    def rolled(i, shift):
                        row = base_ref[layer, first_head + h, pl.ds(i, 1), :]
                        return pltpu.roll(
                            jnp.broadcast_to(row, (CHUNK, 2 * GRID_W)), shift, 1, stride=1, stride_axis=0
                        )

                    both = jnp.where(lane < GRID_W, rolled(o, 0), rolled(o + 1, GRID_W))
                    bias[layer, h, o] = jnp.where(inside, both, -jnp.inf)

    way_here = jnp.where(me == 0, 0, 1)
    after_here = jnp.where(me == 0, 1, n - 2)

    def attend(layer, r):
        @pl.when(at_end)
        def _():
            first = jnp.clip(r - KR // 2, 0, count - KR)
            a = first - r + KR - 1
            rows = rows_of(r)
            band = pl.ds(pl.multiple_of(first * CHUNK, CHUNK), KR * CHUNK)
            outs = []
            for h in range(heads):
                at = [j * cols + h * HD for j in range(3)]
                q = qkv[layer, rows, at[0]:at[0] + HD]
                k = qkv[layer, band, at[1]:at[1] + HD]
                v = qkv[layer, band, at[2]:at[2] + HD]
                scores = lax.dot_general(
                    q, k, (((1,), (1,)), ((), ())), preferred_element_type=jnp.float32
                )
                table = jnp.concatenate([bias[layer, h, a + 2 * i] for i in range(KR // 2)], axis=1)
                scores = scores * scale + table
                scores = jnp.exp(scores - jnp.max(scores, axis=-1, keepdims=True))
                total = jnp.sum(scores, axis=-1, keepdims=True)
                out = jnp.dot(scores.astype(jnp.bfloat16), v, preferred_element_type=jnp.float32)
                outs.append(out / total)
            box[layer, way_here, rows, :] = jnp.concatenate(outs, axis=1).astype(jnp.bfloat16)
            here = box.at[layer, way_here, rows, :]
            remote(
                here, here, at_s.at[layer, way_here], at_r.at[layer, way_here, r], "sp", after_here
            ).start()

    def box_copy(layer, way, r):
        here = box.at[layer, way, rows_of(r), :]
        return remote(here, here, at_s.at[layer, way], at_r.at[layer, way, r], "sp", afters[way])

    def relay(way, layer, r):
        box_copy(layer, way, r).wait_recv()
        box_copy(layer, way, r).start()

    def give_copy(layer, r):
        rows = rows_of(r)
        return remote(
            give.at[layer, rows, :], take.at[layer, rows, :],
            gv_s.at[layer], gv_r.at[layer, r], "tp", partner,
        )

    def cross_copy(layer, r):
        rows = rows_of(r)
        return remote(
            pair.at[layer, rows, :], cross_in.at[layer, rows, :],
            cr_s.at[layer], cr_r.at[layer, r], "tp", cross,
        )

    def multiply(layer, r):
        for way in range(2):
            @pl.when(places[way] == n - 1)
            def _(way=way):
                box_copy(layer, way, r).wait_recv()
        rows = rows_of(r)

        def share(at):
            return jnp.dot(
                box[layer, 0, rows, :], wo[layer, :cols, at], preferred_element_type=jnp.float32
            ) + jnp.dot(box[layer, 1, rows, :], wo[layer, cols:, at], preferred_element_type=jnp.float32)

        give[layer, rows, :] = share(other).astype(jnp.bfloat16)
        give_copy(layer, r).start()
        pair[layer, rows, :] = share(lanes).astype(jnp.bfloat16)

    def meet(layer, r):
        rows = rows_of(r)
        give_copy(layer, r).wait_recv()
        pair[layer, rows, :] = (
            pair[layer, rows, :].astype(jnp.float32) + take[layer, rows, :].astype(jnp.float32)
        ).astype(jnp.bfloat16)
        cross_copy(layer, r).start()

    def out_at(q, lane, size):
        return out_ref.at[span(q * CHUNK, CHUNK), span(lane, size)]

    def finish(layer, r):
        rows = rows_of(r)
        cross_copy(layer, r).wait_recv()

        def new(at, sub):
            branch = pair[layer, rows, sub].astype(jnp.float32) + cross_in[layer, rows, sub].astype(jnp.float32)
            return (xs[layer, rows, at].astype(jnp.float32) + branch).astype(jnp.bfloat16)

        if layer < layers - 1:
            here = xs.at[layer + 1, rows, lanes]
            here[...] = new(lanes, slice(None))
            remote(here, here, fresh_s.at[layer + 1], fresh_r.at[layer + 1, r], "tp", partner).start()
            return
        owner, q = lax.div(r, per), lax.rem(r, per)

        @pl.when(owner == me)
        def _():
            here = out_at(q, me * width + core * half, half)
            here[...] = new(lanes, slice(None))
            remote(here, here, fp_s, fp_r.at[me, q], "tp", partner).start()

        @pl.when(owner != me)
        def _():
            fin[rows, :] = new(span(mine_q, quarter), span(side * quarter, quarter))
            remote(
                fin.at[rows, :], out_at(q, me * width + mine_q, quarter),
                fin_s, fin_r.at[me, q], "sp", owner,
            ).start()

    def hand_cross(layer, r):
        owner, q = lax.div(r, per), lax.rem(r, per)

        @pl.when(owner == me)
        def _():
            for k in range(1, n):
                source = lax.rem(me + k, n)
                here = out_at(q, source * width + mine_q, quarter)
                remote(here, here, fin_s, fin_r.at[source, q], "sp", source).wait_recv()
                remote(here, here, fx_s, fx_r.at[source, q], "tp", cross).start()

    def hand_partner(layer, r):
        owner, q = lax.div(r, per), lax.rem(r, per)

        @pl.when(owner == me)
        def _():
            for k in range(1, n):
                source = lax.rem(me + k, n)
                there = out_at(q, source * width + their_q, quarter)
                remote(there, there, fx_s, fx_r.at[source, q], "tp", cross).wait_recv()
                here = out_at(q, source * width + core * half, half)
                remote(here, here, fp_s, fp_r.at[source, q], "tp", partner).start()

    through = (n - 1) * HOP
    settle = n + 4
    starts = [layer * (through + KR - 1 + settle) for layer in range(layers)]
    plans = [row_plan(count, layer == layers - 1) for layer in range(layers)]
    final = starts[-1] + through + KR - 1 + len(plans[-1]) + n + 6

    @pl.loop(-LEAD, final)
    def _(tick):
        def chunks(stage, late, layer, extra=True):
            c = tick - late - starts[layer]

            @pl.when((c >= 0) & (c < count) & extra)
            def _():
                stage(layer, c)

        def grid_rows(stage, late, layer, extra=True):
            j = tick - late - starts[layer] - through - (KR - 1)
            plan = plans[layer]

            @pl.when((j >= 0) & (j < len(plan)) & extra)
            def _():
                if all(size == 1 for _, size in plan):
                    stage(layer, j)
                    return
                first, size = pick([p[0] for p in plan], j), pick([p[1] for p in plan], j)

                @pl.loop(first, first + size)
                def _(r):
                    stage(layer, r)

        @pl.when(tick == 0)
        def _():
            for copy in weights:
                copy.wait()

        for layer in range(layers):
            for way in range(2):
                inner = (places[way] > 0) & (places[way] < n - 1)
                grid_rows(functools.partial(relay, way), 1 + places[way], layer, inner)
        for layer in range(layers):
            for way in range(2):
                chunks(functools.partial(link, way), HOP * places[way], layer, places[way] > 0)
        grid_rows(hand_partner, n + 6, layers - 1)
        grid_rows(hand_cross, n + 5, layers - 1)
        for layer in range(layers):
            grid_rows(finish, n + 3, layer)
            grid_rows(meet, n + 1, layer)
            grid_rows(multiply, n, layer)

        chunks(lambda _, c: pass_partner(c), -1, 0)
        chunks(lambda _, c: pass_cross(c), -2, 0)
        chunks(lambda _, c: scatter(c), -LEAD, 0)

        @pl.when((tick == 1 - LEAD) & at_end)
        def _():
            make_bias()

        for layer in range(layers):
            chunks(prepare, jnp.where(at_end, 0, HOP - 1), layer)
            chunks(first_link, 0, layer, at_end)
        for layer in range(layers):
            grid_rows(attend, 0, layer)

    for q in range(per):
        for source in range(n):
            there = out_at(q, source * width + (1 - core) * half, half)
            remote(there, there, fp_s, fp_r.at[source, q], "tp", partner).wait_recv()

    def sent(ref, sem, recv):
        remote(ref, ref, sem, recv, "tp", partner).wait_send()

    away = fin.at[0:tokens - own, :]
    sent(away, sp_s, sp_r.at[0])
    sent(away, spx_s, spx_r.at[0])
    sent(away, fin_s, fin_r.at[0, 0])
    sent(away, fx_s, fx_r.at[0, 0])
    sent(xs.at[0, :, 0:half], fp_s, fp_r.at[0, 0])
    sent(xs.at[0, 0:tokens - own, 0:half], fresh_s.at[0], fresh_r.at[0, 0])
    for layer in range(layers):
        if layer > 0:
            sent(xs.at[layer, :, 0:half], fresh_s.at[layer], fresh_r.at[layer, 0])
        sent(give.at[layer], gv_s.at[layer], gv_r.at[layer, 0])
        sent(pair.at[layer], cr_s.at[layer], cr_r.at[layer, 0])
        for way in range(2):
            @pl.when(places[way] < n - 1)
            def _(way=way):
                sent(outbox.at[layer, way], ch_s.at[layer, way], ch_r.at[layer, way, 0])
                sent(box.at[layer, way], at_s.at[layer, way], at_r.at[layer, way, 0])

            @pl.when(me != ends[way])
            def _(way=way):
                sent(sq_own.at[layer], sq_s.at[layer, way], sq_r.at[layer, 0, 0])


def staged(tokens, norm_gain, w_query, w_key, w_value, w_out, offset_bias):
    n, m = lax.axis_size("sp"), lax.axis_size("tp")
    own, features = tokens.shape
    layers = norm_gain.shape[0]
    width, total = features // n, own * n
    heads = offset_bias.shape[1] // 2
    cols = heads * HD
    count, per = total // CHUNK, own // CHUNK
    dma = pltpu.SemaphoreType.DMA
    bf16, f32 = jnp.bfloat16, jnp.float32
    gap = jnp.zeros((*offset_bias.shape[:3], 2 * GRID_W - 2 * KC + 1), f32)
    base = jnp.concatenate([offset_bias[..., KC - 1:], gap, offset_bias[..., :KC - 1]], axis=-1)
    base = jnp.pad(base, ((0, 0), (0, 0), (0, 1), (0, 0)))
    space = pltpu.VMEM
    whole, anywhere = pl.BlockSpec(memory_space=space), pl.BlockSpec(memory_space=pl.ANY)
    return pl.pallas_call(
        functools.partial(pipeline_kernel, n, m),
        out_shape=jax.ShapeDtypeStruct((own, features), bf16),
        in_specs=[whole] * 3 + [anywhere] * 4,
        out_specs=whole,
        scratch_shapes=[
            *[space(w.shape, bf16) for w in (w_query, w_key, w_value, w_out)],
            space((layers, total, width), bf16),
            space((2, total, 3 * cols), f32),
            space((layers, 2, total, 3 * cols), bf16),
            space((layers, 2, total, 3 * cols), bf16),
            space((layers, total, 3 * cols), bf16),
            space((layers, heads, 2 * KR - 2, CHUNK, 2 * GRID_W), f32),
            space((layers, count, 8, 128), f32),
            space((layers, n, count, 8, 128), f32),
            space((layers, 2, total, cols), bf16),
            *[space((layers, total, width // 2), bf16)] * 4,
            space((total, width // 4), bf16),
            dma((layers, 4)),
            dma, dma((count,)), dma, dma((count,)), dma((layers,)), dma((layers, count)),
            dma((layers, 2)), dma((layers, 2, count)), dma((layers, 2)), dma((layers, n, count)),
            dma((layers, 2)), dma((layers, 2, count)),
            dma((layers,)), dma((layers, count)), dma((layers,)), dma((layers, count)),
            dma, dma((n, per)), dma, dma((n, per)), dma, dma((n, per)),
        ],
        compiler_params=pltpu.CompilerParams(
            collective_id=1, has_side_effects=True, vmem_limit_bytes=VMEM_MOST
        ),
        name="pipeline",
    )(tokens, norm_gain, base, w_query, w_key, w_value, w_out)


def on_device(tokens, norm_gain, w_query, w_key, w_value, w_out, offset_bias):
    n, m = lax.axis_size("sp"), lax.axis_size("tp")
    own, features = tokens.shape
    total, width = own * n, features // n
    fits = total * (20 * width + 60 * w_query.shape[2]) < VMEM_MOST
    even = offset_bias.shape[1] % 2 == 0 and m == 4 and n > 2
    if fits and even and own % CHUNK == 0 and width % 512 == 0 and total >= KR * GRID_W:
        return staged(tokens, norm_gain, w_query, w_key, w_value, w_out, offset_bias)
    return general(tokens, norm_gain, w_query, w_key, w_value, w_out, offset_bias)


def solution(mesh):
    return jax.shard_map(
        on_device,
        mesh=mesh,
        in_specs=(
            P(("grp", "sp"), None),
            P(),
            P(None, "sp", "tp"),
            P(None, "sp", "tp"),
            P(None, "sp", "tp"),
            P(None, "tp", "sp"),
            P(None, "tp", None, None),
        ),
        out_specs=P(("grp", "sp"), None),
        check_vma=False,
    )
```

```python
import functools

import jax
import jax.numpy as jnp
from jax import lax
from jax.experimental import pallas as pl
from jax.experimental.pallas import tpu as pltpu
from jax.sharding import PartitionSpec as P

HD = 128
GRID_W = 64
KR = 8
KC = 16
LAYERS = 2


norm_eps = 1e-06


def with_halo(block, sides, width):
    for axis, dim in sides:
        count = lax.axis_size(axis)
        forward = [(i, i + 1) for i in range(count - 1)]
        backward = [(target, source) for source, target in forward]
        low = lax.ppermute(
            lax.slice_in_dim(block, block.shape[dim] - width, None, axis=dim), axis, forward
        )
        high = lax.ppermute(lax.slice_in_dim(block, 0, width, axis=dim), axis, backward)
        block = jnp.concatenate([low, block, high], axis=dim)
    return block


def rms_rows(values, gain):
    wide = values.astype(jnp.float32)
    scaled = wide * lax.rsqrt(jnp.mean(wide * wide, axis=-1, keepdims=True) + norm_eps)
    return (scaled * gain.astype(jnp.float32)).astype(jnp.bfloat16)


def general(tokens, norm_gain, w_query, w_key, w_value, w_out, offset_bias):
    sp_count = lax.axis_size("sp")
    sp_index = lax.axis_index("sp")
    tok_rows = tokens.shape[0]
    local_rows = tok_rows // GRID_W
    grid_rows = local_rows * sp_count
    heads_here = offset_bias.shape[1]
    head_width = heads_here * HD
    reach = KR // 2
    scale = HD ** (-0.5)
    columns = jnp.arange(GRID_W, dtype=jnp.int32)
    col_first = jnp.clip(columns - KC // 2, 0, GRID_W - KC)
    col_inside = (columns[None, :] >= col_first[:, None]) & (
        columns[None, :] < col_first[:, None] + KC
    )
    col_offset = jnp.clip(columns[None, :] - columns[:, None], 1 - KC, KC - 1) + KC - 1
    col_onehot = (
        jnp.arange(2 * KC - 1, dtype=jnp.int32)[:, None, None] == col_offset[None, :, :]
    ).astype(jnp.float32)
    first_row = sp_index * local_rows
    own_rows = first_row + jnp.arange(local_rows, dtype=jnp.int32)
    row_first = jnp.clip(own_rows - reach, 0, grid_rows - KR)
    band_start = row_first - first_row + reach
    row_offset = (
        row_first[:, None] + jnp.arange(KR, dtype=jnp.int32)[None, :] - own_rows[:, None] + KR - 1
    )
    row_onehot = (
        row_offset[:, :, None] == jnp.arange(2 * KR - 1, dtype=jnp.int32)[None, None, :]
    ).astype(jnp.float32)
    qkv_weight = jnp.concatenate([w_query, w_key, w_value], axis=2)
    residual = lax.all_to_all(tokens, "sp", split_axis=1, concat_axis=0, tiled=True)
    width = residual.shape[1]
    features = width * sp_count
    for layer_index in range(LAYERS):
        wide = residual.astype(jnp.float32)
        squares = lax.psum_scatter(
            jnp.sum(wide * wide, axis=-1, keepdims=True), "sp", scatter_dimension=0, tiled=True
        )
        inverse = lax.rsqrt(squares / features + norm_eps)
        gain = lax.dynamic_slice_in_dim(norm_gain[layer_index], sp_index * width, width, 0)
        gained = (wide * gain.astype(jnp.float32)).astype(jnp.bfloat16)
        partial = jnp.dot(gained, qkv_weight[layer_index], preferred_element_type=jnp.float32)
        mine = lax.psum_scatter(
            partial.astype(jnp.bfloat16), "sp", scatter_dimension=0, tiled=True
        )
        mine = (mine.astype(jnp.float32) * inverse).astype(jnp.bfloat16)
        queries = mine[:, :head_width].reshape(local_rows, GRID_W, heads_here, HD)
        key_values = mine[:, head_width:].reshape(local_rows, GRID_W, 2 * head_width)
        padded = with_halo(key_values, (("sp", 0),), reach)
        bands = jax.vmap(lambda band_begin: lax.dynamic_slice_in_dim(padded, band_begin, KR, 0))(
            band_start
        )
        band_keys = bands[..., :head_width].reshape(local_rows, KR, GRID_W, heads_here, HD)
        band_values = bands[..., head_width:].reshape(local_rows, KR, GRID_W, heads_here, HD)
        col_bias = jnp.einsum(
            "hro,oqk->hrqk", offset_bias[layer_index], col_onehot, precision=lax.Precision.HIGHEST
        )
        full_bias = jnp.einsum(
            "ijr,hrqk->hiqjk", row_onehot, col_bias, precision=lax.Precision.HIGHEST
        )
        scores = jnp.einsum(
            "iqhd,ijkhd->hiqjk", queries, band_keys, preferred_element_type=jnp.float32
        )
        scores = scores * scale + full_bias
        scores = jnp.where(col_inside[None, None, :, None, :], scores, -jnp.inf)
        flattened = scores.reshape(heads_here, local_rows, GRID_W, KR * GRID_W)
        weights = jax.nn.softmax(flattened, axis=-1).astype(jnp.bfloat16)
        weights = weights.reshape(heads_here, local_rows, GRID_W, KR, GRID_W)
        attended = jnp.einsum(
            "hiqjk,ijkhd->iqhd", weights, band_values, preferred_element_type=jnp.float32
        )
        attended = attended.astype(jnp.bfloat16).reshape(tok_rows, head_width)
        every = lax.all_gather(attended, "sp", axis=0, tiled=True)
        share = jnp.dot(every, w_out[layer_index], preferred_element_type=jnp.float32)
        branch = lax.psum(share.astype(jnp.bfloat16), "tp").astype(jnp.float32)
        residual = (residual.astype(jnp.float32) + branch).astype(jnp.bfloat16)
    return lax.all_to_all(residual, "sp", split_axis=0, concat_axis=1, tiled=True)


MESH = pl.DeviceIdType.MESH
VMEM_MOST = 63 * 2**20
CHUNK = GRID_W
HOP = 2
LEAD, OWN_LEAD, TURN, PASS = 6, 4, 2, 1
PARTS = 3
FIRST, RELAY = 2, 1
MEET, CROSS, FRESH = 0, 2, 0
HOLD = 6


def greet(peers):
    barrier = pltpu.get_barrier_semaphore()
    for axis, index in peers:
        pl.semaphore_signal(barrier, inc=1, device_id={axis: index}, device_id_type=MESH)
    pl.semaphore_wait(barrier, len(peers))


def remote(src, dst, send, recv, axis, index):
    return pltpu.make_async_remote_copy(
        src_ref=src, dst_ref=dst, send_sem=send, recv_sem=recv,
        device_id={axis: index}, device_id_type=MESH,
    )


def span(start, size):
    return pl.ds(pl.multiple_of(start, size), size)


def row_plan(count, last):
    if not last:
        return [(r, 1) for r in range(count)]
    need = [min(max(r + KR - 1 - KR // 2, KR - 1), count - 1) - KR + 1 for r in range(count)]
    ticks = need[-1]
    early = sum(v < ticks for v in need)
    sizes = [early // ticks + (t >= ticks - early % ticks) for t in range(ticks)] + [count - early]
    starts = [sum(sizes[:t]) for t in range(ticks + 1)]
    return list(zip(starts, sizes))


def pick(table, index):
    value = jnp.int32(table[-1])
    for i in range(len(table) - 2, -1, -1):
        value = jnp.where(index <= i, jnp.int32(table[i]), value)
    return value


def pipeline_kernel(
    n, m, tok_ref, gain_ref, base_ref, wq_any, wk_any, wv_any, wo_any, out_ref,
    wq, wk, wv, wo, xs, part, outbox, inbox, qkv, bias, sq_own, sq_in, box,
    give, take, pair, cross_in, fin,
    w_sem, sp_s, sp_r, spx_s, spx_r, fresh_s, fresh_r, ch_s, ch_r, sq_s, sq_r,
    at_s, at_r, gv_s, gv_r, cr_s, cr_r, fin_s, fin_r, fx_s, fx_r, fp_s, fp_r,
):
    me, t = lax.axis_index("sp"), lax.axis_index("tp")
    core = lax.rem(t, 2)
    side = lax.div(t, 2)
    partner = t + 1 - 2 * core
    cross = lax.rem(t + m // 2, m)
    layers, tokens, width = xs.shape
    own, features = tok_ref.shape
    cols = box.shape[3]
    heads = cols // HD
    half, quarter = width // 2, width // 4
    count, per = tokens // CHUNK, own // CHUNK
    scale = HD ** (-0.5)
    at_end = (me == 0) | (me == n - 1)
    ends = (n - 1, 0)
    lanes = span(core * half, half)
    other = span((1 - core) * half, half)
    mine_q = core * half + side * quarter
    their_q = core * half + (1 - side) * quarter
    places = (me, n - 1 - me)
    afters = (me + 1, me - 1)

    weights = []
    for layer in range(layers):
        for i, (any_ref, ref) in enumerate(((wq_any, wq), (wk_any, wk), (wv_any, wv), (wo_any, wo))):
            copy = pltpu.make_async_copy(any_ref.at[layer], ref.at[layer], w_sem.at[layer, i])
            copy.start()
            weights.append(copy)
    greet(
        [("sp", lax.rem(me + k, n)) for k in range(1, n)] + [("tp", partner), ("tp", cross)]
    )

    def rows_of(c):
        return span(c * CHUNK, CHUNK)

    def scatter(c):
        @pl.when(lax.div(c, per) == me)
        def _():
            here = span((c - me * per) * CHUNK, CHUNK)
            for k in range(1, n):
                to = jnp.where(me < n // 2, n - k + jnp.where(n - k > me, 0, -1), k - 1 + jnp.where(k > me, 1, 0))
                remote(
                    tok_ref.at[here, span(to * width + mine_q, quarter)],
                    xs.at[0, rows_of(c), span(mine_q, quarter)],
                    sp_s, sp_r.at[c], "sp", to,
                ).start()
            xs[0, rows_of(c), :] = tok_ref[here, span(me * width, width)]

    def pass_cross(c):
        @pl.when(lax.div(c, per) != me)
        def _():
            here = xs.at[0, rows_of(c), span(mine_q, quarter)]
            remote(here, here, sp_s, sp_r.at[c], "tp", cross).wait_recv()
            remote(here, here, spx_s, spx_r.at[c], "tp", cross).start()

    def pass_partner(c):
        @pl.when(lax.div(c, per) != me)
        def _():
            there = xs.at[0, rows_of(c), span(their_q, quarter)]
            remote(there, there, spx_s, spx_r.at[c], "tp", cross).wait_recv()
            here = xs.at[0, rows_of(c), lanes]
            remote(here, here, fresh_s.at[0], fresh_r.at[0, c], "tp", partner).start()

    def prepare(layer, c):
        rows = rows_of(c)

        def arrived():
            there = xs.at[layer, rows, other]
            remote(there, there, fresh_s.at[layer], fresh_r.at[layer, c], "tp", partner).wait_recv()

        if layer == 0:
            pl.when(lax.div(c, per) != me)(arrived)
        else:
            arrived()
        gain = gain_ref[layer:layer + 1, span(me * width, width)].astype(jnp.float32)
        wide = xs[layer, rows, :].astype(jnp.float32)
        gained = (wide * gain).astype(jnp.bfloat16)
        for way in range(2):
            lo = (1 - way) * cols
            for j, w_ref in enumerate((wq, wk, wv)):
                part[way, rows, j * cols:(j + 1) * cols] = jnp.dot(
                    gained, w_ref[layer, :, lo:lo + cols], preferred_element_type=jnp.float32
                )
        squares = wide * wide
        high = squares.astype(jnp.bfloat16)
        low = (squares - high.astype(jnp.float32)).astype(jnp.bfloat16)
        ones = jnp.ones((8, width), jnp.bfloat16)
        nt = (((1,), (1,)), ((), ()))
        total = lax.dot_general(
            ones, high, nt, preferred_element_type=jnp.float32
        ) + lax.dot_general(ones, low, nt, preferred_element_type=jnp.float32)
        sq_own[layer, c] = jnp.concatenate([total] * (128 // CHUNK), axis=1)
        for e, end in enumerate(ends):
            @pl.when(me != end)
            def _(e=e, end=end):
                remote(
                    sq_own.at[layer, c], sq_in.at[layer, me, c],
                    sq_s.at[layer, e], sq_r.at[layer, me, c], "sp", end,
                ).start()

    pieces = [slice(i * 3 * cols // PARTS, (i + 1) * 3 * cols // PARTS) for i in range(PARTS)]

    def chain_copy(layer, way, c, i):
        rows = rows_of(c)
        return remote(
            outbox.at[layer, way, rows, pieces[i]], inbox.at[layer, way, rows, pieces[i]],
            ch_s.at[layer, way], ch_r.at[layer, way, c, i], "sp", afters[way],
        )

    def first_link(layer, c):
        for way in range(2):
            @pl.when(places[way] == 0)
            def _(way=way):
                for i, at in enumerate(pieces):
                    outbox[layer, way, rows_of(c), at] = part[way, rows_of(c), at].astype(jnp.bfloat16)
                    chain_copy(layer, way, c, i).start()

    def link(way, layer, c):
        rows = rows_of(c)
        place = places[way]

        def total(i):
            chain_copy(layer, way, c, i).wait_recv()
            return part[way, rows, pieces[i]] + inbox[layer, way, rows, pieces[i]].astype(jnp.float32)

        @pl.when(place < n - 1)
        def _():
            for i, at in enumerate(pieces):
                outbox[layer, way, rows, at] = total(i).astype(jnp.bfloat16)
                chain_copy(layer, way, c, i).start()

        @pl.when(place == n - 1)
        def _():
            squares = sq_own[layer, c]
            for k in range(1, n):
                source = lax.rem(me + k, n)
                remote(
                    sq_own.at[layer, c], sq_in.at[layer, source, c],
                    sq_s.at[layer, 0], sq_r.at[layer, source, c], "sp", source,
                ).wait_recv()
                squares = squares + sq_in[layer, source, c]
            scaled = lax.rsqrt(squares / features + norm_eps)
            inverse = jnp.concatenate([scaled] * 16, axis=0).T[:CHUNK, :1]
            for i, at in enumerate(pieces):
                qkv[layer, rows, at] = (total(i) * inverse).astype(jnp.bfloat16)

    def make_bias(o):
        first_head = jnp.where(me == n - 1, heads, 0)
        lane = lax.broadcasted_iota(jnp.int32, (CHUNK, 2 * GRID_W), 1)
        query = lax.broadcasted_iota(jnp.int32, (CHUNK, 2 * GRID_W), 0)
        key = jnp.where(lane < GRID_W, lane, lane - GRID_W)
        begin = jnp.clip(query - KC // 2, 0, GRID_W - KC)
        inside = (key >= begin) & (key < begin + KC)
        for layer in range(layers):
            for h in range(heads):
                def rolled(i, shift, layer=layer, h=h):
                    row = base_ref[layer, first_head + h, pl.ds(i, 1), :]
                    return pltpu.roll(
                        jnp.broadcast_to(row, (CHUNK, 2 * GRID_W)), shift, 1, stride=1, stride_axis=0
                    )

                both = jnp.where(lane < GRID_W, rolled(o, 0), rolled(o + 1, GRID_W))
                bias[layer, h, o] = jnp.where(inside, both, -jnp.inf)

    way_here = jnp.where(me == 0, 0, 1)
    after_here = jnp.where(me == 0, 1, n - 2)

    def attend(layer, r):
        @pl.when(at_end)
        def _():
            first = jnp.clip(r - KR // 2, 0, count - KR)
            a = first - r + KR - 1
            rows = rows_of(r)
            band = pl.ds(pl.multiple_of(first * CHUNK, CHUNK), KR * CHUNK)
            outs = []
            for h in range(heads):
                at = [j * cols + h * HD for j in range(3)]
                q = qkv[layer, rows, at[0]:at[0] + HD]
                k = qkv[layer, band, at[1]:at[1] + HD]
                v = qkv[layer, band, at[2]:at[2] + HD]
                scores = lax.dot_general(
                    q, k, (((1,), (1,)), ((), ())), preferred_element_type=jnp.float32
                )
                table = jnp.concatenate([bias[layer, h, a + 2 * i] for i in range(KR // 2)], axis=1)
                scores = scores * scale + table
                scores = jnp.exp(scores - jnp.max(scores, axis=-1, keepdims=True))
                total = jnp.sum(scores, axis=-1, keepdims=True)
                out = jnp.dot(scores.astype(jnp.bfloat16), v, preferred_element_type=jnp.float32)
                outs.append(out / total)
            box[layer, way_here, rows, :] = jnp.concatenate(outs, axis=1).astype(jnp.bfloat16)
            here = box.at[layer, way_here, rows, :]
            remote(
                here, here, at_s.at[layer, way_here], at_r.at[layer, way_here, r], "sp", after_here
            ).start()

    def box_copy(layer, way, r):
        here = box.at[layer, way, rows_of(r), :]
        return remote(here, here, at_s.at[layer, way], at_r.at[layer, way, r], "sp", afters[way])

    def relay(way, layer, r):
        box_copy(layer, way, r).wait_recv()
        box_copy(layer, way, r).start()

    def give_copy(layer, r):
        rows = rows_of(r)
        return remote(
            give.at[layer, rows, :], take.at[layer, rows, :],
            gv_s.at[layer], gv_r.at[layer, r], "tp", partner,
        )

    def cross_copy(layer, r):
        at = slice(None) if layer < layers - 1 else span((1 - side) * quarter, quarter)
        rows = rows_of(r)
        return remote(
            pair.at[layer, rows, at], cross_in.at[layer, rows, at],
            cr_s.at[layer], cr_r.at[layer, r], "tp", cross,
        )

    def multiply(layer, r):
        for way in range(2):
            @pl.when(places[way] == n - 1)
            def _(way=way):
                box_copy(layer, way, r).wait_recv()
        rows = rows_of(r)

        def share(at):
            return jnp.dot(
                box[layer, 0, rows, :], wo[layer, :cols, at], preferred_element_type=jnp.float32
            ) + jnp.dot(box[layer, 1, rows, :], wo[layer, cols:, at], preferred_element_type=jnp.float32)

        give[layer, rows, :] = share(other).astype(jnp.bfloat16)
        give_copy(layer, r).start()
        pair[layer, rows, :] = share(lanes).astype(jnp.bfloat16)

    def meet(layer, r):
        rows = rows_of(r)
        give_copy(layer, r).wait_recv()
        pair[layer, rows, :] = (
            pair[layer, rows, :].astype(jnp.float32) + take[layer, rows, :].astype(jnp.float32)
        ).astype(jnp.bfloat16)
        cross_copy(layer, r).start()

    def out_at(q, lane, size):
        return out_ref.at[span(q * CHUNK, CHUNK), span(lane, size)]

    def finish(layer, r):
        rows = rows_of(r)
        cross_copy(layer, r).wait_recv()

        def new(at, sub):
            branch = pair[layer, rows, sub].astype(jnp.float32) + cross_in[layer, rows, sub].astype(jnp.float32)
            return (xs[layer, rows, at].astype(jnp.float32) + branch).astype(jnp.bfloat16)

        if layer < layers - 1:
            here = xs.at[layer + 1, rows, lanes]
            here[...] = new(lanes, slice(None))
            remote(here, here, fresh_s.at[layer + 1], fresh_r.at[layer + 1, r], "tp", partner).start()
            return
        owner, q = lax.div(r, per), lax.rem(r, per)
        here = out_at(q, me * width + mine_q, quarter)
        value = new(span(mine_q, quarter), span(side * quarter, quarter))

        @pl.when(owner == me)
        def _():
            here[...] = value
            remote(here, here, fx_s, fx_r.at[me, q], "tp", cross).start()

        @pl.when(owner != me)
        def _():
            fin[rows, :] = value
            remote(fin.at[rows, :], here, fin_s, fin_r.at[me, q], "sp", owner).start()

    def hand_cross(q):
        for k in range(1, n):
            source = lax.rem(me + k, n)
            here = out_at(q, source * width + mine_q, quarter)
            remote(here, here, fin_s, fin_r.at[source, q], "sp", source).wait_recv()
            remote(here, here, fx_s, fx_r.at[source, q], "tp", cross).start()

    def hand_partner(q):
        for k in range(n):
            source = lax.rem(me + k, n)
            there = out_at(q, source * width + their_q, quarter)
            remote(there, there, fx_s, fx_r.at[source, q], "tp", cross).wait_recv()
            here = out_at(q, source * width + core * half, half)
            remote(here, here, fp_s, fp_r.at[source, q], "tp", partner).start()

    through = (n - 1) * HOP
    share_at = FIRST + (n - 2) * RELAY
    meet_at = share_at + MEET
    finish_at = meet_at + CROSS
    settle = finish_at + FRESH
    starts = [layer * (through + KR - 1 + settle) for layer in range(layers)]
    plans = [row_plan(count, layer == layers - 1) for layer in range(layers)]
    final = starts[-1] + through + KR - 1 + len(plans[-1]) + finish_at

    @pl.loop(-LEAD, final)
    def _(tick):
        def chunks(stage, late, layer, extra=True):
            c = tick - late - starts[layer]

            @pl.when((c >= 0) & (c < count) & extra)
            def _():
                stage(layer, c)

        def grid_rows(stage, late, layer, extra=True, plan=None):
            j = tick - late - starts[layer] - through - (KR - 1)
            plan = plan or plans[layer]

            @pl.when((j >= 0) & (j < len(plan)) & extra)
            def _():
                if all(size == 1 for _, size in plan):
                    stage(layer, j)
                    return
                first, size = pick([p[0] for p in plan], j), pick([p[1] for p in plan], j)

                @pl.loop(first, first + size)
                def _(r):
                    stage(layer, r)

        def relays(low, high):
            for layer in range(layers):
                for way in range(2):
                    place = places[way]
                    inner = (place >= low) & (place < high)
                    grid_rows(functools.partial(relay, way), FIRST + (place - 1) * RELAY, layer, inner)

        @pl.when(tick == 0)
        def _():
            for copy in weights:
                copy.wait()

        last = layers - 1
        relays(1, 2)
        chunks(lambda _, c: pass_cross(c), -TURN, 0)
        for layer in range(layers):
            for way in range(2):
                chunks(functools.partial(link, way), HOP * places[way], layer, places[way] > 0)
        for layer in range(last):
            grid_rows(finish, finish_at, layer)
        held = plans[last][HOLD + 1:]
        held = [(0, held[0][0])] + held
        grid_rows(finish, finish_at + HOLD, last, plan=held)
        for layer in range(layers):
            grid_rows(attend, 0, layer)
        relays(2, n - 1)
        for layer in range(layers):
            grid_rows(multiply, share_at, layer)

        chunks(lambda _, c: pass_partner(c), -PASS, 0)
        chunks(lambda _, c: scatter(c), -jnp.where(me == 0, OWN_LEAD, LEAD), 0)

        @pl.when((tick >= -1) & (tick < 2 * KR - 3) & at_end)
        def _():
            make_bias(tick + 1)

        for layer in range(layers):
            chunks(prepare, jnp.where(at_end, 0, HOP - 1), layer)
            chunks(first_link, 0, layer, at_end)
        for layer in range(layers):
            grid_rows(meet, meet_at, layer)

    @pl.loop(0, per)
    def _(q):
        hand_cross(q)

    @pl.loop(0, per)
    def _(q):
        hand_partner(q)

    for q in range(per):
        for source in range(n):
            there = out_at(q, source * width + (1 - core) * half, half)
            remote(there, there, fp_s, fp_r.at[source, q], "tp", partner).wait_recv()

    def sent(ref, sem, recv):
        remote(ref, ref, sem, recv, "tp", partner).wait_send()

    away = fin.at[0:tokens - own, :]
    sent(away, sp_s, sp_r.at[0])
    sent(away, spx_s, spx_r.at[0])
    sent(away, fin_s, fin_r.at[0, 0])
    sent(fin, fx_s, fx_r.at[0, 0])
    sent(xs.at[0, :, 0:half], fp_s, fp_r.at[0, 0])
    sent(xs.at[0, 0:tokens - own, 0:half], fresh_s.at[0], fresh_r.at[0, 0])
    for layer in range(layers):
        if layer > 0:
            sent(xs.at[layer, :, 0:half], fresh_s.at[layer], fresh_r.at[layer, 0])
        sent(give.at[layer], gv_s.at[layer], gv_r.at[layer, 0])
        swapped = pair.at[layer] if layer < layers - 1 else pair.at[layer, :, 0:quarter]
        sent(swapped, cr_s.at[layer], cr_r.at[layer, 0])
        for way in range(2):
            @pl.when(places[way] < n - 1)
            def _(way=way):
                sent(outbox.at[layer, way], ch_s.at[layer, way], ch_r.at[layer, way, 0, 0])
                sent(box.at[layer, way], at_s.at[layer, way], at_r.at[layer, way, 0])

            @pl.when(me != ends[way])
            def _(way=way):
                sent(sq_own.at[layer], sq_s.at[layer, way], sq_r.at[layer, 0, 0])


def staged(tokens, norm_gain, w_query, w_key, w_value, w_out, offset_bias):
    n, m = lax.axis_size("sp"), lax.axis_size("tp")
    own, features = tokens.shape
    layers = norm_gain.shape[0]
    width, total = features // n, own * n
    heads = offset_bias.shape[1] // 2
    cols = heads * HD
    count, per = total // CHUNK, own // CHUNK
    dma = pltpu.SemaphoreType.DMA
    bf16, f32 = jnp.bfloat16, jnp.float32
    gap = jnp.zeros((*offset_bias.shape[:3], 2 * GRID_W - 2 * KC + 1), f32)
    base = jnp.concatenate([offset_bias[..., KC - 1:], gap, offset_bias[..., :KC - 1]], axis=-1)
    base = jnp.pad(base, ((0, 0), (0, 0), (0, 1), (0, 0)))
    space = pltpu.VMEM
    whole, anywhere = pl.BlockSpec(memory_space=space), pl.BlockSpec(memory_space=pl.ANY)
    return pl.pallas_call(
        functools.partial(pipeline_kernel, n, m),
        out_shape=jax.ShapeDtypeStruct((own, features), bf16),
        in_specs=[whole] * 3 + [anywhere] * 4,
        out_specs=whole,
        scratch_shapes=[
            *[space(w.shape, bf16) for w in (w_query, w_key, w_value, w_out)],
            space((layers, total, width), bf16),
            space((2, total, 3 * cols), f32),
            space((layers, 2, total, 3 * cols), bf16),
            space((layers, 2, total, 3 * cols), bf16),
            space((layers, total, 3 * cols), bf16),
            space((layers, heads, 2 * KR - 2, CHUNK, 2 * GRID_W), f32),
            space((layers, count, 8, 128), f32),
            space((layers, n, count, 8, 128), f32),
            space((layers, 2, total, cols), bf16),
            *[space((layers, total, width // 2), bf16)] * 4,
            space((total, width // 4), bf16),
            dma((layers, 4)),
            dma, dma((count,)), dma, dma((count,)), dma((layers,)), dma((layers, count)),
            dma((layers, 2)), dma((layers, 2, count, PARTS)), dma((layers, 2)), dma((layers, n, count)),
            dma((layers, 2)), dma((layers, 2, count)),
            dma((layers,)), dma((layers, count)), dma((layers,)), dma((layers, count)),
            dma, dma((n, per)), dma, dma((n, per)), dma, dma((n, per)),
        ],
        compiler_params=pltpu.CompilerParams(
            collective_id=1, has_side_effects=True, vmem_limit_bytes=VMEM_MOST
        ),
        name="pipeline",
    )(tokens, norm_gain, base, w_query, w_key, w_value, w_out)


def on_device(tokens, norm_gain, w_query, w_key, w_value, w_out, offset_bias):
    n, m = lax.axis_size("sp"), lax.axis_size("tp")
    own, features = tokens.shape
    total, width = own * n, features // n
    fits = total * (20 * width + 60 * w_query.shape[2]) < VMEM_MOST
    even = offset_bias.shape[1] % 2 == 0 and m == 4 and n > 2
    if fits and even and own % CHUNK == 0 and width % 512 == 0 and total >= KR * GRID_W:
        return staged(tokens, norm_gain, w_query, w_key, w_value, w_out, offset_bias)
    return general(tokens, norm_gain, w_query, w_key, w_value, w_out, offset_bias)


def solution(mesh):
    return jax.shard_map(
        on_device,
        mesh=mesh,
        in_specs=(
            P(("grp", "sp"), None),
            P(),
            P(None, "sp", "tp"),
            P(None, "sp", "tp"),
            P(None, "sp", "tp"),
            P(None, "tp", "sp"),
            P(None, "tp", None, None),
        ),
        out_specs=P(("grp", "sp"), None),
        check_vma=False,
    )
```

```python
import functools

import jax
import jax.numpy as jnp
from jax import lax
from jax.experimental import pallas as pl
from jax.experimental.pallas import tpu as pltpu
from jax.sharding import PartitionSpec as P

HD = 128
GRID_W = 64
KR = 8
KC = 16
LAYERS = 2


norm_eps = 1e-06


def with_halo(block, sides, width):
    for axis, dim in sides:
        count = lax.axis_size(axis)
        forward = [(i, i + 1) for i in range(count - 1)]
        backward = [(target, source) for source, target in forward]
        low = lax.ppermute(
            lax.slice_in_dim(block, block.shape[dim] - width, None, axis=dim), axis, forward
        )
        high = lax.ppermute(lax.slice_in_dim(block, 0, width, axis=dim), axis, backward)
        block = jnp.concatenate([low, block, high], axis=dim)
    return block


def rms_rows(values, gain):
    wide = values.astype(jnp.float32)
    scaled = wide * lax.rsqrt(jnp.mean(wide * wide, axis=-1, keepdims=True) + norm_eps)
    return (scaled * gain.astype(jnp.float32)).astype(jnp.bfloat16)


def general(tokens, norm_gain, w_query, w_key, w_value, w_out, offset_bias):
    sp_count = lax.axis_size("sp")
    sp_index = lax.axis_index("sp")
    tok_rows = tokens.shape[0]
    local_rows = tok_rows // GRID_W
    grid_rows = local_rows * sp_count
    heads_here = offset_bias.shape[1]
    head_width = heads_here * HD
    reach = KR // 2
    scale = HD ** (-0.5)
    columns = jnp.arange(GRID_W, dtype=jnp.int32)
    col_first = jnp.clip(columns - KC // 2, 0, GRID_W - KC)
    col_inside = (columns[None, :] >= col_first[:, None]) & (
        columns[None, :] < col_first[:, None] + KC
    )
    col_offset = jnp.clip(columns[None, :] - columns[:, None], 1 - KC, KC - 1) + KC - 1
    col_onehot = (
        jnp.arange(2 * KC - 1, dtype=jnp.int32)[:, None, None] == col_offset[None, :, :]
    ).astype(jnp.float32)
    first_row = sp_index * local_rows
    own_rows = first_row + jnp.arange(local_rows, dtype=jnp.int32)
    row_first = jnp.clip(own_rows - reach, 0, grid_rows - KR)
    band_start = row_first - first_row + reach
    row_offset = (
        row_first[:, None] + jnp.arange(KR, dtype=jnp.int32)[None, :] - own_rows[:, None] + KR - 1
    )
    row_onehot = (
        row_offset[:, :, None] == jnp.arange(2 * KR - 1, dtype=jnp.int32)[None, None, :]
    ).astype(jnp.float32)
    qkv_weight = jnp.concatenate([w_query, w_key, w_value], axis=2)
    residual = lax.all_to_all(tokens, "sp", split_axis=1, concat_axis=0, tiled=True)
    width = residual.shape[1]
    features = width * sp_count
    for layer_index in range(LAYERS):
        wide = residual.astype(jnp.float32)
        squares = lax.psum_scatter(
            jnp.sum(wide * wide, axis=-1, keepdims=True), "sp", scatter_dimension=0, tiled=True
        )
        inverse = lax.rsqrt(squares / features + norm_eps)
        gain = lax.dynamic_slice_in_dim(norm_gain[layer_index], sp_index * width, width, 0)
        gained = (wide * gain.astype(jnp.float32)).astype(jnp.bfloat16)
        partial = jnp.dot(gained, qkv_weight[layer_index], preferred_element_type=jnp.float32)
        mine = lax.psum_scatter(
            partial.astype(jnp.bfloat16), "sp", scatter_dimension=0, tiled=True
        )
        mine = (mine.astype(jnp.float32) * inverse).astype(jnp.bfloat16)
        queries = mine[:, :head_width].reshape(local_rows, GRID_W, heads_here, HD)
        key_values = mine[:, head_width:].reshape(local_rows, GRID_W, 2 * head_width)
        padded = with_halo(key_values, (("sp", 0),), reach)
        bands = jax.vmap(lambda band_begin: lax.dynamic_slice_in_dim(padded, band_begin, KR, 0))(
            band_start
        )
        band_keys = bands[..., :head_width].reshape(local_rows, KR, GRID_W, heads_here, HD)
        band_values = bands[..., head_width:].reshape(local_rows, KR, GRID_W, heads_here, HD)
        col_bias = jnp.einsum(
            "hro,oqk->hrqk", offset_bias[layer_index], col_onehot, precision=lax.Precision.HIGHEST
        )
        full_bias = jnp.einsum(
            "ijr,hrqk->hiqjk", row_onehot, col_bias, precision=lax.Precision.HIGHEST
        )
        scores = jnp.einsum(
            "iqhd,ijkhd->hiqjk", queries, band_keys, preferred_element_type=jnp.float32
        )
        scores = scores * scale + full_bias
        scores = jnp.where(col_inside[None, None, :, None, :], scores, -jnp.inf)
        flattened = scores.reshape(heads_here, local_rows, GRID_W, KR * GRID_W)
        weights = jax.nn.softmax(flattened, axis=-1).astype(jnp.bfloat16)
        weights = weights.reshape(heads_here, local_rows, GRID_W, KR, GRID_W)
        attended = jnp.einsum(
            "hiqjk,ijkhd->iqhd", weights, band_values, preferred_element_type=jnp.float32
        )
        attended = attended.astype(jnp.bfloat16).reshape(tok_rows, head_width)
        every = lax.all_gather(attended, "sp", axis=0, tiled=True)
        share = jnp.dot(every, w_out[layer_index], preferred_element_type=jnp.float32)
        branch = lax.psum(share.astype(jnp.bfloat16), "tp").astype(jnp.float32)
        residual = (residual.astype(jnp.float32) + branch).astype(jnp.bfloat16)
    return lax.all_to_all(residual, "sp", split_axis=0, concat_axis=1, tiled=True)


MESH = pl.DeviceIdType.MESH
VMEM_MOST = 56 * 2**20
CHUNK = GRID_W
HOP = 2
LEAD, OWN_LEAD, TURN, PASS = 6, 4, 2, 1
PARTS = 3
FIRST, RELAY = 2, 1
MEET, CROSS, FRESH = 0, 2, 0
HOLD = 6
FAR_FIRST = True


def greet(peers):
    barrier = pltpu.get_barrier_semaphore()
    for axis, index in peers:
        pl.semaphore_signal(barrier, inc=1, device_id={axis: index}, device_id_type=MESH)
    pl.semaphore_wait(barrier, len(peers))


def remote(src, dst, send, recv, axis, index):
    return pltpu.make_async_remote_copy(
        src_ref=src, dst_ref=dst, send_sem=send, recv_sem=recv,
        device_id={axis: index}, device_id_type=MESH,
    )


def span(start, size):
    return pl.ds(pl.multiple_of(start, size), size)


def row_plan(count, last):
    if not last:
        return [(r, 1) for r in range(count)]
    need = [min(max(r + KR - 1 - KR // 2, KR - 1), count - 1) - KR + 1 for r in range(count)]
    ticks = need[-1]
    early = sum(v < ticks for v in need)
    sizes = [early // ticks + (t >= ticks - early % ticks) for t in range(ticks)] + [count - early]
    starts = [sum(sizes[:t]) for t in range(ticks + 1)]
    return list(zip(starts, sizes))


def pick(table, index):
    value = jnp.int32(table[-1])
    for i in range(len(table) - 2, -1, -1):
        value = jnp.where(index <= i, jnp.int32(table[i]), value)
    return value


def pipeline_kernel(
    n, m, tok_ref, gain_ref, offset_ref, wq_any, wk_any, wv_any, wo_any, out_ref,
    wq, wk, wv, wo, xs, part, outbox, inbox, qkv, bias, sq_own, sq_in, box,
    give, take, pair, cross_in, fin, padded,
    w_sem, sp_s, sp_r, spx_s, spx_r, fresh_s, fresh_r, ch_s, ch_r, sq_s, sq_r,
    at_s, at_r, gv_s, gv_r, cr_s, cr_r, fin_s, fin_r, fx_s, fx_r, fp_s, fp_r,
):
    me, t = lax.axis_index("sp"), lax.axis_index("tp")
    core = lax.rem(t, 2)
    side = lax.div(t, 2)
    partner = t + 1 - 2 * core
    cross = lax.rem(t + m // 2, m)
    layers, tokens, width = xs.shape
    own, features = tok_ref.shape
    cols = box.shape[3]
    heads = cols // HD
    half, quarter = width // 2, width // 4
    count, per = tokens // CHUNK, own // CHUNK
    scale = HD ** (-0.5)
    at_end = (me == 0) | (me == n - 1)
    ends = (n - 1, 0)
    lanes = span(core * half, half)
    other = span((1 - core) * half, half)
    mine_q = core * half + side * quarter
    their_q = core * half + (1 - side) * quarter
    places = (me, n - 1 - me)
    afters = (me + 1, me - 1)

    weights = []
    for layer in range(layers):
        for i, (any_ref, ref) in enumerate(((wq_any, wq), (wk_any, wk), (wv_any, wv), (wo_any, wo))):
            copy = pltpu.make_async_copy(any_ref.at[layer], ref.at[layer], w_sem.at[layer, i])
            copy.start()
            weights.append(copy)
    greet(
        [("sp", lax.rem(me + k, n)) for k in range(1, n)] + [("tp", partner), ("tp", cross)]
    )

    def rows_of(c):
        return span(c * CHUNK, CHUNK)

    def scatter(c):
        @pl.when(lax.div(c, per) == me)
        def _():
            here = span((c - me * per) * CHUNK, CHUNK)
            for k in range(1, n):
                to = jnp.where(me < n // 2, n - k + jnp.where(n - k > me, 0, -1), k - 1 + jnp.where(k > me, 1, 0))
                remote(
                    tok_ref.at[here, span(to * width + mine_q, quarter)],
                    xs.at[0, rows_of(c), span(mine_q, quarter)],
                    sp_s, sp_r.at[c], "sp", to,
                ).start()
            xs[0, rows_of(c), :] = tok_ref[here, span(me * width, width)]

    def pass_cross(c):
        @pl.when(lax.div(c, per) != me)
        def _():
            here = xs.at[0, rows_of(c), span(mine_q, quarter)]
            remote(here, here, sp_s, sp_r.at[c], "tp", cross).wait_recv()
            remote(here, here, spx_s, spx_r.at[c], "tp", cross).start()

    def pass_partner(c):
        @pl.when(lax.div(c, per) != me)
        def _():
            there = xs.at[0, rows_of(c), span(their_q, quarter)]
            remote(there, there, spx_s, spx_r.at[c], "tp", cross).wait_recv()
            here = xs.at[0, rows_of(c), lanes]
            remote(here, here, fresh_s.at[0], fresh_r.at[c], "tp", partner).start()

    def prepare(layer, c):
        rows = rows_of(c)

        def arrived():
            there = xs.at[layer, rows, other]
            remote(there, there, fresh_s.at[layer], fresh_r.at[c], "tp", partner).wait_recv()

        if layer == 0:
            pl.when(lax.div(c, per) != me)(arrived)
        else:
            arrived()
        gain = gain_ref[layer:layer + 1, span(me * width, width)].astype(jnp.float32)
        wide = xs[layer, rows, :].astype(jnp.float32)
        gained = (wide * gain).astype(jnp.bfloat16)
        for way in range(2):
            lo = (1 - way) * cols
            for j, w_ref in enumerate((wq, wk, wv)):
                part[way, rows, j * cols:(j + 1) * cols] = jnp.dot(
                    gained, w_ref[layer, :, lo:lo + cols], preferred_element_type=jnp.float32
                )
        squares = wide * wide
        high = squares.astype(jnp.bfloat16)
        low = (squares - high.astype(jnp.float32)).astype(jnp.bfloat16)
        ones = jnp.ones((8, width), jnp.bfloat16)
        nt = (((1,), (1,)), ((), ()))
        total = lax.dot_general(
            ones, high, nt, preferred_element_type=jnp.float32
        ) + lax.dot_general(ones, low, nt, preferred_element_type=jnp.float32)
        sq_own[layer, c] = jnp.concatenate([total] * (128 // CHUNK), axis=1)
        for e, end in enumerate(ends):
            @pl.when(me != end)
            def _(e=e, end=end):
                remote(
                    sq_own.at[layer, c], sq_in.at[layer, c, me],
                    sq_s.at[layer, e], sq_r.at[c], "sp", end,
                ).start()

    pieces = [slice(i * 3 * cols // PARTS, (i + 1) * 3 * cols // PARTS) for i in range(PARTS)]

    def chain_copy(layer, way, c, i):
        rows = rows_of(c)
        return remote(
            outbox.at[layer, way, rows, pieces[i]], inbox.at[layer, way, rows, pieces[i]],
            ch_s.at[layer, way], ch_r.at[way, c, i], "sp", afters[way],
        )

    def first_link(layer, c):
        for way in range(2):
            @pl.when(places[way] == 0)
            def _(way=way):
                for i, at in enumerate(pieces):
                    outbox[layer, way, rows_of(c), at] = part[way, rows_of(c), at].astype(jnp.bfloat16)
                    chain_copy(layer, way, c, i).start()

    def link(way, layer, c):
        rows = rows_of(c)
        place = places[way]

        def total(i):
            chain_copy(layer, way, c, i).wait_recv()
            return part[way, rows, pieces[i]] + inbox[layer, way, rows, pieces[i]].astype(jnp.float32)

        @pl.when(place < n - 1)
        def _():
            for i, at in enumerate(pieces):
                outbox[layer, way, rows, at] = total(i).astype(jnp.bfloat16)
                chain_copy(layer, way, c, i).start()

        @pl.when(place == n - 1)
        def _():
            squares = sq_own[layer, c]
            others = sq_in.at[layer, c, 0:n - 1]
            remote(others, others, sq_s.at[layer, 0], sq_r.at[c], "sp", n - 1 - me).wait_recv()
            for k in range(1, n):
                squares = squares + sq_in[layer, c, lax.rem(me + k, n)]
            scaled = lax.rsqrt(squares / features + norm_eps)
            inverse = jnp.concatenate([scaled] * 16, axis=0).T[:CHUNK, :1]
            for i, at in enumerate(pieces):
                qkv[layer, rows, at] = (total(i) * inverse).astype(jnp.bfloat16)

    def make_bias(o):
        first_head = jnp.where(me == n - 1, heads, 0)
        lane = lax.broadcasted_iota(jnp.int32, (CHUNK, 2 * GRID_W), 1)
        query = lax.broadcasted_iota(jnp.int32, (CHUNK, 2 * GRID_W), 0)
        key = jnp.where(lane < GRID_W, lane, lane - GRID_W)
        begin = jnp.clip(query - KC // 2, 0, GRID_W - KC)
        inside = (key >= begin) & (key < begin + KC)
        for layer in range(layers):
            for h in range(heads):
                def rolled(i, shift, layer=layer, h=h):
                    row = padded[layer, first_head + h, pl.ds(i, 1), :]
                    return pltpu.roll(
                        jnp.broadcast_to(row, (CHUNK, 2 * GRID_W)), shift, 1, stride=1, stride_axis=0
                    )

                both = jnp.where(
                    lane < GRID_W, rolled(o, 2 * GRID_W - KC + 1), rolled(o + 1, GRID_W - KC + 1)
                )
                bias[layer, h, o] = jnp.where(inside, both, -jnp.inf)

    @pl.when(at_end)
    def _():
        padded[...] = jnp.zeros_like(padded)
        for layer in range(layers):
            for h in range(2 * heads):
                padded[layer, h, 0:2 * KR - 1, 0:2 * KC - 1] = offset_ref[layer, h]

    way_here = jnp.where(me == 0, 0, 1)
    after_here = jnp.where(me == 0, 1, n - 2)

    def attend(layer, r):
        @pl.when(at_end)
        def _():
            first = jnp.clip(r - KR // 2, 0, count - KR)
            a = first - r + KR - 1
            rows = rows_of(r)
            band = pl.ds(pl.multiple_of(first * CHUNK, CHUNK), KR * CHUNK)
            outs = []
            for h in range(heads):
                at = [j * cols + h * HD for j in range(3)]
                q = qkv[layer, rows, at[0]:at[0] + HD]
                k = qkv[layer, band, at[1]:at[1] + HD]
                v = qkv[layer, band, at[2]:at[2] + HD]
                scores = lax.dot_general(
                    q, k, (((1,), (1,)), ((), ())), preferred_element_type=jnp.float32
                )
                table = jnp.concatenate([bias[layer, h, a + 2 * i] for i in range(KR // 2)], axis=1)
                scores = scores * scale + table
                scores = jnp.exp(scores - jnp.max(scores, axis=-1, keepdims=True))
                total = jnp.sum(scores, axis=-1, keepdims=True)
                out = jnp.dot(scores.astype(jnp.bfloat16), v, preferred_element_type=jnp.float32)
                outs.append(out / total)
            box[layer, way_here, rows, :] = jnp.concatenate(outs, axis=1).astype(jnp.bfloat16)
            here = box.at[layer, way_here, rows, :]
            remote(
                here, here, at_s.at[layer, way_here], at_r.at[way_here, r], "sp", after_here
            ).start()

    def box_copy(layer, way, r):
        here = box.at[layer, way, rows_of(r), :]
        return remote(here, here, at_s.at[layer, way], at_r.at[way, r], "sp", afters[way])

    def relay(way, layer, r):
        box_copy(layer, way, r).wait_recv()
        box_copy(layer, way, r).start()

    def give_copy(layer, r):
        rows = rows_of(r)
        return remote(
            give.at[layer, rows, :], take.at[layer, rows, :],
            gv_s.at[layer], gv_r.at[r], "tp", partner,
        )

    def cross_copy(layer, r):
        at = slice(None) if layer < layers - 1 else span((1 - side) * quarter, quarter)
        rows = rows_of(r)
        return remote(
            pair.at[layer, rows, at], cross_in.at[layer, rows, at],
            cr_s.at[layer], cr_r.at[layer, r], "tp", cross,
        )

    def multiply(layer, r):
        for way in range(2):
            @pl.when(places[way] == n - 1)
            def _(way=way):
                box_copy(layer, way, r).wait_recv()
        rows = rows_of(r)

        def share(at):
            return jnp.dot(
                box[layer, 0, rows, :], wo[layer, :cols, at], preferred_element_type=jnp.float32
            ) + jnp.dot(box[layer, 1, rows, :], wo[layer, cols:, at], preferred_element_type=jnp.float32)

        give[layer, rows, :] = share(other).astype(jnp.bfloat16)
        give_copy(layer, r).start()
        pair[layer, rows, :] = share(lanes).astype(jnp.bfloat16)

    def meet(layer, r):
        rows = rows_of(r)
        give_copy(layer, r).wait_recv()
        pair[layer, rows, :] = (
            pair[layer, rows, :].astype(jnp.float32) + take[layer, rows, :].astype(jnp.float32)
        ).astype(jnp.bfloat16)
        cross_copy(layer, r).start()

    def out_at(q, lane, size):
        return out_ref.at[span(q * CHUNK, CHUNK), span(lane, size)]

    def finish(layer, r):
        rows = rows_of(r)
        cross_copy(layer, r).wait_recv()

        def new(at, sub):
            branch = pair[layer, rows, sub].astype(jnp.float32) + cross_in[layer, rows, sub].astype(jnp.float32)
            return (xs[layer, rows, at].astype(jnp.float32) + branch).astype(jnp.bfloat16)

        if layer < layers - 1:
            here = xs.at[layer + 1, rows, lanes]
            here[...] = new(lanes, slice(None))
            remote(here, here, fresh_s.at[layer + 1], fresh_r.at[r], "tp", partner).start()
            return
        owner, q = lax.div(r, per), lax.rem(r, per)
        here = out_at(q, me * width + mine_q, quarter)
        value = new(span(mine_q, quarter), span(side * quarter, quarter))

        @pl.when(owner == me)
        def _():
            here[...] = value
            remote(here, here, fx_s, fx_r.at[q], "tp", cross).start()

        @pl.when(owner != me)
        def _():
            fin[rows, :] = value
            remote(fin.at[rows, :], here, fin_s, fin_r.at[me, q], "sp", owner).start()

    def hand_cross(q):
        for k in range(1, n):
            source = lax.rem(me + k, n)
            here = out_at(q, source * width + mine_q, quarter)
            remote(here, here, fin_s, fin_r.at[source, q], "sp", source).wait_recv()
            remote(here, here, fx_s, fx_r.at[q], "tp", cross).start()

    def hand_partner(q):
        every = fin.at[0:n * CHUNK, :]
        remote(every, every, fx_s, fx_r.at[q], "tp", cross).wait_recv()
        for source in range(n):
            here = out_at(q, source * width + core * half, half)
            remote(here, here, fp_s, fp_r, "tp", partner).start()

    through = (n - 1) * HOP
    share_at = FIRST + (n - 2) * RELAY
    meet_at = share_at + MEET
    finish_at = meet_at + CROSS
    settle = finish_at + FRESH
    starts = [layer * (through + KR - 1 + settle) for layer in range(layers)]
    plans = [row_plan(count, layer == layers - 1) for layer in range(layers)]
    final = starts[-1] + through + KR - 1 + len(plans[-1]) + finish_at

    @pl.loop(-LEAD, final)
    def _(tick):
        def chunks(stage, late, layer, extra=True):
            c = tick - late - starts[layer]

            @pl.when((c >= 0) & (c < count) & extra)
            def _():
                stage(layer, c)

        def grid_rows(stage, late, layer, extra=True, plan=None):
            j = tick - late - starts[layer] - through - (KR - 1)
            plan = plan or plans[layer]

            @pl.when((j >= 0) & (j < len(plan)) & extra)
            def _():
                if all(size == 1 for _, size in plan):
                    stage(layer, j)
                    return
                first, size = pick([p[0] for p in plan], j), pick([p[1] for p in plan], j)

                @pl.loop(first, first + size)
                def _(r):
                    stage(layer, r)

        def relays(low, high, which):
            for layer in which:
                for way in range(2):
                    place = places[way]
                    inner = (place >= low) & (place < high)
                    grid_rows(functools.partial(relay, way), FIRST + (place - 1) * RELAY, layer, inner)

        @pl.when(tick == 0)
        def _():
            for copy in weights:
                copy.wait()

        last = layers - 1
        if FAR_FIRST:
            relays(2, n - 1, [last])
        relays(1, 2, range(layers))
        chunks(lambda _, c: pass_cross(c), -TURN, 0)
        for layer in range(layers):
            for way in range(2):
                chunks(functools.partial(link, way), HOP * places[way], layer, places[way] > 0)
        for layer in range(last):
            grid_rows(finish, finish_at, layer)
        held = plans[last][HOLD + 1:]
        held = [(0, held[0][0])] + held
        grid_rows(finish, finish_at + HOLD, last, plan=held)
        for layer in range(layers):
            grid_rows(attend, 0, layer)
        relays(2, n - 1, range(last) if FAR_FIRST else range(layers))
        for layer in range(layers):
            grid_rows(multiply, share_at, layer)

        chunks(lambda _, c: pass_partner(c), -PASS, 0)
        chunks(lambda _, c: scatter(c), -jnp.where(me == 0, OWN_LEAD, LEAD), 0)

        @pl.when((tick >= -1) & (tick < 2 * KR - 3) & at_end)
        def _():
            make_bias(tick + 1)

        for layer in range(layers):
            chunks(prepare, jnp.where(at_end, 0, HOP - 1), layer)
            chunks(first_link, 0, layer, at_end)
        for layer in range(layers):
            grid_rows(meet, meet_at, layer)

    @pl.loop(0, per)
    def _(q):
        hand_cross(q)

    @pl.loop(0, per)
    def _(q):
        hand_partner(q)

    every = xs.at[0, :, 0:half]
    remote(every, every, fp_s, fp_r, "tp", partner).wait_recv()

    def sent(ref, sem, recv):
        remote(ref, ref, sem, recv, "tp", partner).wait_send()

    away = fin.at[0:tokens - own, :]
    sent(away, sp_s, sp_r.at[0])
    sent(away, spx_s, spx_r.at[0])
    sent(away, fin_s, fin_r.at[0, 0])
    sent(fin, fx_s, fx_r.at[0])
    sent(xs.at[0, :, 0:half], fp_s, fp_r)
    sent(xs.at[0, 0:tokens - own, 0:half], fresh_s.at[0], fresh_r.at[0])
    for layer in range(layers):
        if layer > 0:
            sent(xs.at[layer, :, 0:half], fresh_s.at[layer], fresh_r.at[0])
        sent(give.at[layer], gv_s.at[layer], gv_r.at[0])
        swapped = pair.at[layer] if layer < layers - 1 else pair.at[layer, :, 0:quarter]
        sent(swapped, cr_s.at[layer], cr_r.at[layer, 0])
        for way in range(2):
            @pl.when(places[way] < n - 1)
            def _(way=way):
                sent(outbox.at[layer, way], ch_s.at[layer, way], ch_r.at[way, 0, 0])
                sent(box.at[layer, way], at_s.at[layer, way], at_r.at[way, 0])

            @pl.when(me != ends[way])
            def _(way=way):
                sent(sq_own.at[layer], sq_s.at[layer, way], sq_r.at[0])


def store_kernel(mixed_ref, out_ref, sem):
    copy = pltpu.make_async_copy(mixed_ref, out_ref, sem)
    copy.start()
    copy.wait()


def staged(tokens, norm_gain, w_query, w_key, w_value, w_out, offset_bias):
    n, m = lax.axis_size("sp"), lax.axis_size("tp")
    own, features = tokens.shape
    layers = norm_gain.shape[0]
    width, total = features // n, own * n
    heads = offset_bias.shape[1] // 2
    cols = heads * HD
    count, per = total // CHUNK, own // CHUNK
    dma = pltpu.SemaphoreType.DMA
    bf16, f32 = jnp.bfloat16, jnp.float32
    space = pltpu.VMEM
    whole, anywhere = pl.BlockSpec(memory_space=space), pl.BlockSpec(memory_space=pl.ANY)
    mixed = pl.pallas_call(
        functools.partial(pipeline_kernel, n, m),
        out_shape=space((own, features), bf16),
        in_specs=[whole] * 3 + [anywhere] * 4,
        out_specs=whole,
        scratch_shapes=[
            *[space(w.shape, bf16) for w in (w_query, w_key, w_value, w_out)],
            space((layers, total, width), bf16),
            space((2, total, 3 * cols), f32),
            space((layers, 2, total, 3 * cols), bf16),
            space((layers, 2, total, 3 * cols), bf16),
            space((layers, total, 3 * cols), bf16),
            space((layers, heads, 2 * KR - 2, CHUNK, 2 * GRID_W), f32),
            space((layers, count, 8, 128), f32),
            space((layers, count, n, 8, 128), f32),
            space((layers, 2, total, cols), bf16),
            *[space((layers, total, width // 2), bf16)] * 4,
            space((total, width // 4), bf16),
            space((layers, 2 * heads, 2 * KR, 2 * GRID_W), f32),
            dma((layers, 4)),
            dma, dma((count,)), dma, dma((count,)), dma((layers,)), dma((count,)),
            dma((layers, 2)), dma((2, count, PARTS)), dma((layers, 2)), dma((count,)),
            dma((layers, 2)), dma((2, count)),
            dma((layers,)), dma((count,)), dma((layers,)), dma((layers, count)),
            dma, dma((n, per)), dma, dma((per,)), dma, dma,
        ],
        compiler_params=pltpu.CompilerParams(
            collective_id=1, has_side_effects=True, vmem_limit_bytes=VMEM_MOST
        ),
        name="pipeline",
    )(tokens, norm_gain, offset_bias, w_query, w_key, w_value, w_out)
    return pl.pallas_call(
        store_kernel,
        out_shape=jax.ShapeDtypeStruct((own, features), bf16),
        in_specs=[whole],
        out_specs=anywhere,
        scratch_shapes=[dma],
        compiler_params=pltpu.CompilerParams(vmem_limit_bytes=2**20),
        name="store",
    )(mixed)


def on_device(tokens, norm_gain, w_query, w_key, w_value, w_out, offset_bias):
    n, m = lax.axis_size("sp"), lax.axis_size("tp")
    own, features = tokens.shape
    total, width = own * n, features // n
    fits = total * (20 * width + 60 * w_query.shape[2]) < VMEM_MOST
    even = offset_bias.shape[1] % 2 == 0 and m == 4 and n > 2
    if fits and even and own % CHUNK == 0 and width % 512 == 0 and total >= KR * GRID_W:
        return staged(tokens, norm_gain, w_query, w_key, w_value, w_out, offset_bias)
    return general(tokens, norm_gain, w_query, w_key, w_value, w_out, offset_bias)


def solution(mesh):
    return jax.shard_map(
        on_device,
        mesh=mesh,
        in_specs=(
            P(("grp", "sp"), None),
            P(),
            P(None, "sp", "tp"),
            P(None, "sp", "tp"),
            P(None, "sp", "tp"),
            P(None, "tp", "sp"),
            P(None, "tp", None, None),
        ),
        out_specs=P(("grp", "sp"), None),
        check_vma=False,
    )
```

```python
import functools

import jax
import jax.numpy as jnp
from jax import lax
from jax.experimental import pallas as pl
from jax.experimental.pallas import tpu as pltpu
from jax.sharding import PartitionSpec as P

HD = 128
GRID_W = 64
KR = 8
KC = 16
LAYERS = 2


norm_eps = 1e-06


def with_halo(block, sides, width):
    for axis, dim in sides:
        count = lax.axis_size(axis)
        forward = [(i, i + 1) for i in range(count - 1)]
        backward = [(target, source) for source, target in forward]
        low = lax.ppermute(
            lax.slice_in_dim(block, block.shape[dim] - width, None, axis=dim), axis, forward
        )
        high = lax.ppermute(lax.slice_in_dim(block, 0, width, axis=dim), axis, backward)
        block = jnp.concatenate([low, block, high], axis=dim)
    return block


def rms_rows(values, gain):
    wide = values.astype(jnp.float32)
    scaled = wide * lax.rsqrt(jnp.mean(wide * wide, axis=-1, keepdims=True) + norm_eps)
    return (scaled * gain.astype(jnp.float32)).astype(jnp.bfloat16)


def general(tokens, norm_gain, w_query, w_key, w_value, w_out, offset_bias):
    sp_count = lax.axis_size("sp")
    sp_index = lax.axis_index("sp")
    tok_rows = tokens.shape[0]
    local_rows = tok_rows // GRID_W
    grid_rows = local_rows * sp_count
    heads_here = offset_bias.shape[1]
    head_width = heads_here * HD
    reach = KR // 2
    scale = HD ** (-0.5)
    columns = jnp.arange(GRID_W, dtype=jnp.int32)
    col_first = jnp.clip(columns - KC // 2, 0, GRID_W - KC)
    col_inside = (columns[None, :] >= col_first[:, None]) & (
        columns[None, :] < col_first[:, None] + KC
    )
    col_offset = jnp.clip(columns[None, :] - columns[:, None], 1 - KC, KC - 1) + KC - 1
    col_onehot = (
        jnp.arange(2 * KC - 1, dtype=jnp.int32)[:, None, None] == col_offset[None, :, :]
    ).astype(jnp.float32)
    first_row = sp_index * local_rows
    own_rows = first_row + jnp.arange(local_rows, dtype=jnp.int32)
    row_first = jnp.clip(own_rows - reach, 0, grid_rows - KR)
    band_start = row_first - first_row + reach
    row_offset = (
        row_first[:, None] + jnp.arange(KR, dtype=jnp.int32)[None, :] - own_rows[:, None] + KR - 1
    )
    row_onehot = (
        row_offset[:, :, None] == jnp.arange(2 * KR - 1, dtype=jnp.int32)[None, None, :]
    ).astype(jnp.float32)
    qkv_weight = jnp.concatenate([w_query, w_key, w_value], axis=2)
    residual = lax.all_to_all(tokens, "sp", split_axis=1, concat_axis=0, tiled=True)
    width = residual.shape[1]
    features = width * sp_count
    for layer_index in range(LAYERS):
        wide = residual.astype(jnp.float32)
        squares = lax.psum_scatter(
            jnp.sum(wide * wide, axis=-1, keepdims=True), "sp", scatter_dimension=0, tiled=True
        )
        inverse = lax.rsqrt(squares / features + norm_eps)
        gain = lax.dynamic_slice_in_dim(norm_gain[layer_index], sp_index * width, width, 0)
        gained = (wide * gain.astype(jnp.float32)).astype(jnp.bfloat16)
        partial = jnp.dot(gained, qkv_weight[layer_index], preferred_element_type=jnp.float32)
        mine = lax.psum_scatter(
            partial.astype(jnp.bfloat16), "sp", scatter_dimension=0, tiled=True
        )
        mine = (mine.astype(jnp.float32) * inverse).astype(jnp.bfloat16)
        queries = mine[:, :head_width].reshape(local_rows, GRID_W, heads_here, HD)
        key_values = mine[:, head_width:].reshape(local_rows, GRID_W, 2 * head_width)
        padded = with_halo(key_values, (("sp", 0),), reach)
        bands = jax.vmap(lambda band_begin: lax.dynamic_slice_in_dim(padded, band_begin, KR, 0))(
            band_start
        )
        band_keys = bands[..., :head_width].reshape(local_rows, KR, GRID_W, heads_here, HD)
        band_values = bands[..., head_width:].reshape(local_rows, KR, GRID_W, heads_here, HD)
        col_bias = jnp.einsum(
            "hro,oqk->hrqk", offset_bias[layer_index], col_onehot, precision=lax.Precision.HIGHEST
        )
        full_bias = jnp.einsum(
            "ijr,hrqk->hiqjk", row_onehot, col_bias, precision=lax.Precision.HIGHEST
        )
        scores = jnp.einsum(
            "iqhd,ijkhd->hiqjk", queries, band_keys, preferred_element_type=jnp.float32
        )
        scores = scores * scale + full_bias
        scores = jnp.where(col_inside[None, None, :, None, :], scores, -jnp.inf)
        flattened = scores.reshape(heads_here, local_rows, GRID_W, KR * GRID_W)
        weights = jax.nn.softmax(flattened, axis=-1).astype(jnp.bfloat16)
        weights = weights.reshape(heads_here, local_rows, GRID_W, KR, GRID_W)
        attended = jnp.einsum(
            "hiqjk,ijkhd->iqhd", weights, band_values, preferred_element_type=jnp.float32
        )
        attended = attended.astype(jnp.bfloat16).reshape(tok_rows, head_width)
        every = lax.all_gather(attended, "sp", axis=0, tiled=True)
        share = jnp.dot(every, w_out[layer_index], preferred_element_type=jnp.float32)
        branch = lax.psum(share.astype(jnp.bfloat16), "tp").astype(jnp.float32)
        residual = (residual.astype(jnp.float32) + branch).astype(jnp.bfloat16)
    return lax.all_to_all(residual, "sp", split_axis=0, concat_axis=1, tiled=True)


MESH = pl.DeviceIdType.MESH
VMEM_MOST = 56 * 2**20
CHUNK = GRID_W
HOP = 2
LEAD, OWN_LEAD, TURN, PASS = 6, 4, 2, 1
PARTS = 3
FIRST, RELAY = 2, 1
MEET, CROSS, FRESH = 0, 2, 0
HOLD = 5
FAR = 1
SPREAD = 0
HOP_TWO = 0
LAST_RELAY = 1


def greet(peers):
    barrier = pltpu.get_barrier_semaphore()
    for axis, index in peers:
        pl.semaphore_signal(barrier, inc=1, device_id={axis: index}, device_id_type=MESH)
    pl.semaphore_wait(barrier, len(peers))


def remote(src, dst, send, recv, axis, index):
    return pltpu.make_async_remote_copy(
        src_ref=src, dst_ref=dst, send_sem=send, recv_sem=recv,
        device_id={axis: index}, device_id_type=MESH,
    )


def span(start, size):
    return pl.ds(pl.multiple_of(start, size), size)


def row_plan(count, last):
    if not last:
        return [(r, 1) for r in range(count)]
    need = [min(max(r + KR - 1 - KR // 2, KR - 1), count - 1) - KR + 1 for r in range(count)]
    ticks = need[-1]
    early = sum(v < ticks for v in need)
    sizes = [early // ticks + (t >= ticks - early % ticks) for t in range(ticks)] + [count - early]
    starts = [sum(sizes[:t]) for t in range(ticks + 1)]
    return list(zip(starts, sizes))


def pick(table, index):
    value = jnp.int32(table[-1])
    for i in range(len(table) - 2, -1, -1):
        value = jnp.where(index <= i, jnp.int32(table[i]), value)
    return value


def pipeline_kernel(
    n, m, tok_any, gain_ref, offset_ref, wq_any, wk_any, wv_any, wo_any, out_ref,
    tok_ref, wq, wk, wv, wo, xs, part, outbox, inbox, qkv, bias, sq_own, sq_in, box,
    give, take, pair, cross_in, fin, padded,
    w_sem, sp_s, sp_r, spx_s, spx_r, fresh_s, fresh_r, ch_s, ch_r, sq_s, sq_r,
    at_s, at_r, gv_s, gv_r, cr_s, cr_r, fin_s, fin_r, fx_s, fx_r, fp_s, fp_r,
):
    me, t = lax.axis_index("sp"), lax.axis_index("tp")
    core = lax.rem(t, 2)
    side = lax.div(t, 2)
    partner = t + 1 - 2 * core
    cross = lax.rem(t + m // 2, m)
    layers, tokens, width = xs.shape
    own, features = tok_ref.shape
    cols = box.shape[3]
    heads = cols // HD
    half, quarter = width // 2, width // 4
    count, per = tokens // CHUNK, own // CHUNK
    scale = HD ** (-0.5)
    at_end = (me == 0) | (me == n - 1)
    ends = (n - 1, 0)
    lanes = span(core * half, half)
    other = span((1 - core) * half, half)
    mine_q = core * half + side * quarter
    their_q = core * half + (1 - side) * quarter
    places = (me, n - 1 - me)
    afters = (me + 1, me - 1)

    loaded = pltpu.make_async_copy(tok_any, tok_ref, w_sem.at[0, 4])
    loaded.start()
    weights = []
    for layer in range(layers):
        for i, (any_ref, ref) in enumerate(((wq_any, wq), (wk_any, wk), (wv_any, wv), (wo_any, wo))):
            copy = pltpu.make_async_copy(any_ref.at[layer], ref.at[layer], w_sem.at[layer, i])
            copy.start()
            weights.append(copy)
    greet(
        [("sp", lax.rem(me + k, n)) for k in range(1, n)] + [("tp", partner), ("tp", cross)]
    )
    loaded.wait()

    def rows_of(c):
        return span(c * CHUNK, CHUNK)

    def scatter(c):
        @pl.when(lax.div(c, per) == me)
        def _():
            here = span((c - me * per) * CHUNK, CHUNK)
            for k in range(1, n):
                to = jnp.where(me < n // 2, n - k + jnp.where(n - k > me, 0, -1), k - 1 + jnp.where(k > me, 1, 0))
                remote(
                    tok_ref.at[here, span(to * width + mine_q, quarter)],
                    xs.at[0, rows_of(c), span(mine_q, quarter)],
                    sp_s, sp_r.at[c], "sp", to,
                ).start()
            xs[0, rows_of(c), :] = tok_ref[here, span(me * width, width)]

    def pass_cross(c):
        @pl.when(lax.div(c, per) != me)
        def _():
            here = xs.at[0, rows_of(c), span(mine_q, quarter)]
            remote(here, here, sp_s, sp_r.at[c], "tp", cross).wait_recv()
            remote(here, here, spx_s, spx_r.at[c], "tp", cross).start()

    def pass_partner(c):
        @pl.when(lax.div(c, per) != me)
        def _():
            there = xs.at[0, rows_of(c), span(their_q, quarter)]
            remote(there, there, spx_s, spx_r.at[c], "tp", cross).wait_recv()
            here = xs.at[0, rows_of(c), lanes]
            remote(here, here, fresh_s.at[0], fresh_r.at[c], "tp", partner).start()

    def prepare(layer, c):
        rows = rows_of(c)

        def arrived():
            there = xs.at[layer, rows, other]
            remote(there, there, fresh_s.at[layer], fresh_r.at[c], "tp", partner).wait_recv()

        if layer == 0:
            pl.when(lax.div(c, per) != me)(arrived)
        else:
            arrived()
        gain = gain_ref[layer:layer + 1, span(me * width, width)].astype(jnp.float32)
        wide = xs[layer, rows, :].astype(jnp.float32)
        gained = (wide * gain).astype(jnp.bfloat16)
        for way in range(2):
            lo = (1 - way) * cols
            for j, w_ref in enumerate((wq, wk, wv)):
                part[way, rows, j * cols:(j + 1) * cols] = jnp.dot(
                    gained, w_ref[layer, :, lo:lo + cols], preferred_element_type=jnp.float32
                )
        squares = wide * wide
        high = squares.astype(jnp.bfloat16)
        low = (squares - high.astype(jnp.float32)).astype(jnp.bfloat16)
        ones = jnp.ones((8, width), jnp.bfloat16)
        nt = (((1,), (1,)), ((), ()))
        total = lax.dot_general(
            ones, high, nt, preferred_element_type=jnp.float32
        ) + lax.dot_general(ones, low, nt, preferred_element_type=jnp.float32)
        sq_own[layer, c] = jnp.concatenate([total] * (128 // CHUNK), axis=1)
        for e, end in enumerate(ends):
            @pl.when(me != end)
            def _(e=e, end=end):
                remote(
                    sq_own.at[layer, c], sq_in.at[layer, c, me],
                    sq_s.at[layer, e], sq_r.at[c], "sp", end,
                ).start()

    pieces = [slice(i * 3 * cols // PARTS, (i + 1) * 3 * cols // PARTS) for i in range(PARTS)]

    def chain_copy(layer, way, c, i):
        rows = rows_of(c)
        return remote(
            outbox.at[layer, way, rows, pieces[i]], inbox.at[layer, way, rows, pieces[i]],
            ch_s.at[layer, way], ch_r.at[way, c, i], "sp", afters[way],
        )

    def first_link(layer, c):
        for way in range(2):
            @pl.when(places[way] == 0)
            def _(way=way):
                for i, at in enumerate(pieces):
                    outbox[layer, way, rows_of(c), at] = part[way, rows_of(c), at].astype(jnp.bfloat16)
                    chain_copy(layer, way, c, i).start()

    def link(way, layer, c):
        rows = rows_of(c)
        place = places[way]

        def total(i):
            chain_copy(layer, way, c, i).wait_recv()
            return part[way, rows, pieces[i]] + inbox[layer, way, rows, pieces[i]].astype(jnp.float32)

        @pl.when(place < n - 1)
        def _():
            for i, at in enumerate(pieces):
                outbox[layer, way, rows, at] = total(i).astype(jnp.bfloat16)
                chain_copy(layer, way, c, i).start()

        @pl.when(place == n - 1)
        def _():
            squares = sq_own[layer, c]
            others = sq_in.at[layer, c, 0:n - 1]
            remote(others, others, sq_s.at[layer, 0], sq_r.at[c], "sp", n - 1 - me).wait_recv()
            for k in range(1, n):
                squares = squares + sq_in[layer, c, lax.rem(me + k, n)]
            scaled = lax.rsqrt(squares / features + norm_eps)
            inverse = jnp.concatenate([scaled] * 16, axis=0).T[:CHUNK, :1]
            for i, at in enumerate(pieces):
                qkv[layer, rows, at] = (total(i) * inverse).astype(jnp.bfloat16)

    def make_bias(o):
        first_head = jnp.where(me == n - 1, heads, 0)
        lane = lax.broadcasted_iota(jnp.int32, (CHUNK, 2 * GRID_W), 1)
        query = lax.broadcasted_iota(jnp.int32, (CHUNK, 2 * GRID_W), 0)
        key = jnp.where(lane < GRID_W, lane, lane - GRID_W)
        begin = jnp.clip(query - KC // 2, 0, GRID_W - KC)
        inside = (key >= begin) & (key < begin + KC)
        for layer in range(layers):
            for h in range(heads):
                def rolled(i, shift, layer=layer, h=h):
                    row = padded[layer, first_head + h, pl.ds(i, 1), :]
                    return pltpu.roll(
                        jnp.broadcast_to(row, (CHUNK, 2 * GRID_W)), shift, 1, stride=1, stride_axis=0
                    )

                both = jnp.where(
                    lane < GRID_W, rolled(o, 2 * GRID_W - KC + 1), rolled(o + 1, GRID_W - KC + 1)
                )
                bias[layer, h, o] = jnp.where(inside, both, -jnp.inf)

    @pl.when(at_end)
    def _():
        padded[...] = jnp.zeros_like(padded)
        for layer in range(layers):
            for h in range(2 * heads):
                padded[layer, h, 0:2 * KR - 1, 0:2 * KC - 1] = offset_ref[layer, h]

    way_here = jnp.where(me == 0, 0, 1)
    after_here = jnp.where(me == 0, 1, n - 2)

    def attend(layer, r):
        @pl.when(at_end)
        def _():
            first = jnp.clip(r - KR // 2, 0, count - KR)
            a = first - r + KR - 1
            rows = rows_of(r)
            band = pl.ds(pl.multiple_of(first * CHUNK, CHUNK), KR * CHUNK)
            outs = []
            for h in range(heads):
                at = [j * cols + h * HD for j in range(3)]
                q = qkv[layer, rows, at[0]:at[0] + HD]
                k = qkv[layer, band, at[1]:at[1] + HD]
                v = qkv[layer, band, at[2]:at[2] + HD]
                scores = lax.dot_general(
                    q, k, (((1,), (1,)), ((), ())), preferred_element_type=jnp.float32
                )
                table = jnp.concatenate([bias[layer, h, a + 2 * i] for i in range(KR // 2)], axis=1)
                scores = scores * scale + table
                scores = jnp.exp(scores - jnp.max(scores, axis=-1, keepdims=True))
                total = jnp.sum(scores, axis=-1, keepdims=True)
                out = jnp.dot(scores.astype(jnp.bfloat16), v, preferred_element_type=jnp.float32)
                outs.append(out / total)
            box[layer, way_here, rows, :] = jnp.concatenate(outs, axis=1).astype(jnp.bfloat16)
            here = box.at[layer, way_here, rows, :]
            remote(
                here, here, at_s.at[layer, way_here], at_r.at[way_here, r], "sp", after_here
            ).start()

    def box_copy(layer, way, r):
        here = box.at[layer, way, rows_of(r), :]
        return remote(here, here, at_s.at[layer, way], at_r.at[way, r], "sp", afters[way])

    def relay(way, layer, r):
        box_copy(layer, way, r).wait_recv()
        box_copy(layer, way, r).start()

    def give_copy(layer, r):
        rows = rows_of(r)
        return remote(
            give.at[layer, rows, :], take.at[layer, rows, :],
            gv_s.at[layer], gv_r.at[r], "tp", partner,
        )

    def cross_copy(layer, r, whole):
        at = slice(None) if whole else span((1 - side) * quarter, quarter)
        rows = rows_of(r)
        return remote(
            pair.at[layer, rows, at], cross_in.at[layer, rows, at],
            cr_s.at[layer], cr_r.at[layer, r], "tp", cross,
        )

    def multiply(layer, r):
        for way in range(2):
            @pl.when(places[way] == n - 1)
            def _(way=way):
                box_copy(layer, way, r).wait_recv()
        rows = rows_of(r)

        def share(at):
            return jnp.dot(
                box[layer, 0, rows, :], wo[layer, :cols, at], preferred_element_type=jnp.float32
            ) + jnp.dot(box[layer, 1, rows, :], wo[layer, cols:, at], preferred_element_type=jnp.float32)

        give[layer, rows, :] = share(other).astype(jnp.bfloat16)
        give_copy(layer, r).start()
        pair[layer, rows, :] = share(lanes).astype(jnp.bfloat16)

    def meet(layer, r):
        rows = rows_of(r)
        give_copy(layer, r).wait_recv()
        pair[layer, rows, :] = (
            pair[layer, rows, :].astype(jnp.float32) + take[layer, rows, :].astype(jnp.float32)
        ).astype(jnp.bfloat16)
        if layer < layers - 1:
            cross_copy(layer, r, True).start()
            return
        owner = lax.div(r, per)
        pl.when(owner == me)(lambda: cross_copy(layer, r, True).start())
        pl.when(owner != me)(lambda: cross_copy(layer, r, False).start())

    def out_at(q, lane, size):
        return out_ref.at[span(q * CHUNK, CHUNK), span(lane, size)]

    def finish(layer, r):
        rows = rows_of(r)

        def new(at, sub):
            branch = pair[layer, rows, sub].astype(jnp.float32) + cross_in[layer, rows, sub].astype(jnp.float32)
            return (xs[layer, rows, at].astype(jnp.float32) + branch).astype(jnp.bfloat16)

        if layer < layers - 1:
            cross_copy(layer, r, True).wait_recv()
            here = xs.at[layer + 1, rows, lanes]
            here[...] = new(lanes, slice(None))
            remote(here, here, fresh_s.at[layer + 1], fresh_r.at[r], "tp", partner).start()
            return
        owner, q = lax.div(r, per), lax.rem(r, per)
        @pl.when(owner == me)
        def _():
            cross_copy(layer, r, True).wait_recv()
            here = out_at(q, me * width + core * half, half)
            here[...] = new(lanes, slice(None))
            remote(here, here, fp_s, fp_r, "tp", partner).start()

        @pl.when(owner != me)
        def _():
            cross_copy(layer, r, False).wait_recv()
            fin[rows, :] = new(span(mine_q, quarter), span(side * quarter, quarter))
            remote(
                fin.at[rows, :], out_at(q, me * width + mine_q, quarter),
                fin_s, fin_r.at[me, q], "sp", owner,
            ).start()

    def hand_cross(q):
        for k in range(1, n):
            source = lax.rem(me + k, n)
            here = out_at(q, source * width + mine_q, quarter)
            remote(here, here, fin_s, fin_r.at[source, q], "sp", source).wait_recv()
            remote(here, here, fx_s, fx_r.at[q], "tp", cross).start()

    def hand_partner(q):
        every = fin.at[0:(n - 1) * CHUNK, :]
        remote(every, every, fx_s, fx_r.at[q], "tp", cross).wait_recv()
        for k in range(1, n):
            source = lax.rem(me + k, n)
            here = out_at(q, source * width + core * half, half)
            remote(here, here, fp_s, fp_r, "tp", partner).start()

    through = (n - 1) * HOP - HOP_TWO
    share_at = FIRST + (n - 2) * RELAY
    meet_at = share_at + MEET
    finish_at = meet_at + CROSS
    settle = finish_at + FRESH
    last_share = FIRST + (n - 2) * LAST_RELAY
    last_meet = last_share + MEET
    last_finish = last_meet + CROSS
    starts = [layer * (through + KR - 1 + settle) for layer in range(layers)]
    plans = [row_plan(count, layer == layers - 1) for layer in range(layers)]
    final = starts[-1] + through + KR - 1 + len(plans[-1]) + last_finish

    @pl.loop(-LEAD, final)
    def _(tick):
        def chunks(stage, late, layer, extra=True):
            c = tick - late - starts[layer]

            @pl.when((c >= 0) & (c < count) & extra)
            def _():
                stage(layer, c)

        def grid_rows(stage, late, layer, extra=True, plan=None, behind=None):
            j = tick - late - starts[layer] - through - (KR - 1)
            plan = plan or plans[layer]

            @pl.when((j >= 0) & (j < len(plan)) & extra)
            def _():
                if all(size == 1 for _, size in plan):
                    stage(layer, j)
                    return
                first, size = pick([p[0] for p in plan], j), pick([p[1] for p in plan], j)

                @pl.loop(first, first + size)
                def _(r):
                    stage(layer, r)
                    if behind:
                        pl.when(r > first)(lambda: behind(layer, r - 1))

                if behind:
                    behind(layer, first + size - 1)

        lead = per * me + OWN_LEAD if SPREAD == 0 else jnp.where(me == 1, LEAD, per * me + OWN_LEAD)

        def relays(low, high, which):
            for layer in which:
                for way in range(2):
                    place = places[way]
                    inner = (place >= low) & (place < high)
                    grid_rows(functools.partial(relay, way), FIRST + (place - 1) * (RELAY if layer < layers - 1 else LAST_RELAY), layer, inner)

        @pl.when(tick == 0)
        def _():
            for copy in weights:
                copy.wait()

        last = layers - 1
        if FAR == 0:
            relays(2, n - 1, [last])
        relays(1, 2, range(layers))
        if FAR == 1:
            relays(2, n - 1, range(layers))
        chunks(lambda _, c: pass_cross(c), -TURN, 0)
        for layer in range(layers):
            for way in range(2):
                place = places[way]
                early = (place > 0) & (place != 2) if HOP_TWO else place > 0
                chunks(functools.partial(link, way), HOP * place - jnp.where(place >= 2, HOP_TWO, 0), layer, early)
        for layer in range(last):
            grid_rows(finish, finish_at, layer)
        held = plans[last][HOLD + 1:]
        held = [(0, held[0][0])] + held
        grid_rows(finish, last_finish + HOLD, last, plan=held)
        for layer in range(layers):
            grid_rows(attend, 0, layer)
        if FAR != 1:
            relays(2, n - 1, range(last) if FAR == 0 else range(layers))
        if HOP_TWO:
            for layer in range(layers):
                for way in range(2):
                    chunks(functools.partial(link, way), 2 * HOP - HOP_TWO, layer, places[way] == 2)
        for layer in range(last):
            grid_rows(multiply, share_at, layer)
        grid_rows(multiply, last_share, last, behind=meet)

        chunks(lambda _, c: pass_partner(c), -PASS, 0)
        chunks(lambda _, c: scatter(c), -lead, 0)

        @pl.when((tick >= -1) & (tick < 2 * KR - 3) & at_end)
        def _():
            make_bias(tick + 1)

        for layer in range(layers):
            chunks(prepare, jnp.where(at_end, 0, HOP - 1), layer)
            chunks(first_link, 0, layer, at_end)
        for layer in range(last):
            grid_rows(meet, meet_at, layer)

    @pl.loop(0, per)
    def _(q):
        hand_cross(q)

    @pl.loop(0, per)
    def _(q):
        hand_partner(q)

    every = xs.at[0, :, 0:half]
    remote(every, every, fp_s, fp_r, "tp", partner).wait_recv()

    def sent(ref, sem, recv):
        remote(ref, ref, sem, recv, "tp", partner).wait_send()

    away = fin.at[0:tokens - own, :]
    sent(away, sp_s, sp_r.at[0])
    sent(away, spx_s, spx_r.at[0])
    sent(away, fin_s, fin_r.at[0, 0])
    sent(away, fx_s, fx_r.at[0])
    sent(xs.at[0, :, 0:half], fp_s, fp_r)
    sent(xs.at[0, 0:tokens - own, 0:half], fresh_s.at[0], fresh_r.at[0])
    for layer in range(layers):
        if layer > 0:
            sent(xs.at[layer, :, 0:half], fresh_s.at[layer], fresh_r.at[0])
        sent(give.at[layer], gv_s.at[layer], gv_r.at[0])
        if layer < layers - 1:
            sent(pair.at[layer], cr_s.at[layer], cr_r.at[layer, 0])
        else:
            sent(fin, cr_s.at[layer], cr_r.at[layer, 0])
            sent(fin.at[0:own, :], cr_s.at[layer], cr_r.at[layer, 0])
        for way in range(2):
            @pl.when(places[way] < n - 1)
            def _(way=way):
                sent(outbox.at[layer, way], ch_s.at[layer, way], ch_r.at[way, 0, 0])
                sent(box.at[layer, way], at_s.at[layer, way], at_r.at[way, 0])

            @pl.when(me != ends[way])
            def _(way=way):
                sent(sq_own.at[layer], sq_s.at[layer, way], sq_r.at[0])


def store_kernel(mixed_ref, out_ref, sem):
    copy = pltpu.make_async_copy(mixed_ref, out_ref, sem)
    copy.start()
    copy.wait()


def staged(tokens, norm_gain, w_query, w_key, w_value, w_out, offset_bias):
    n, m = lax.axis_size("sp"), lax.axis_size("tp")
    own, features = tokens.shape
    layers = norm_gain.shape[0]
    width, total = features // n, own * n
    heads = offset_bias.shape[1] // 2
    cols = heads * HD
    count, per = total // CHUNK, own // CHUNK
    dma = pltpu.SemaphoreType.DMA
    bf16, f32 = jnp.bfloat16, jnp.float32
    space = pltpu.VMEM
    whole, anywhere = pl.BlockSpec(memory_space=space), pl.BlockSpec(memory_space=pl.ANY)
    mixed = pl.pallas_call(
        functools.partial(pipeline_kernel, n, m),
        out_shape=space((own, features), bf16),
        in_specs=[anywhere] + [whole] * 2 + [anywhere] * 4,
        out_specs=whole,
        scratch_shapes=[
            *[space(w.shape, bf16) for w in (tokens, w_query, w_key, w_value, w_out)],
            space((layers, total, width), bf16),
            space((2, total, 3 * cols), f32),
            space((layers, 2, total, 3 * cols), bf16),
            space((layers, 2, total, 3 * cols), bf16),
            space((layers, total, 3 * cols), bf16),
            space((layers, heads, 2 * KR - 2, CHUNK, 2 * GRID_W), f32),
            space((layers, count, 8, 128), f32),
            space((layers, count, n, 8, 128), f32),
            space((layers, 2, total, cols), bf16),
            *[space((layers, total, width // 2), bf16)] * 4,
            space((total, width // 4), bf16),
            space((layers, 2 * heads, 2 * KR, 2 * GRID_W), f32),
            dma((layers, 5)),
            dma, dma((count,)), dma, dma((count,)), dma((layers,)), dma((count,)),
            dma((layers, 2)), dma((2, count, PARTS)), dma((layers, 2)), dma((count,)),
            dma((layers, 2)), dma((2, count)),
            dma((layers,)), dma((count,)), dma((layers,)), dma((layers, count)),
            dma, dma((n, per)), dma, dma((per,)), dma, dma,
        ],
        compiler_params=pltpu.CompilerParams(
            collective_id=1, has_side_effects=True, vmem_limit_bytes=VMEM_MOST
        ),
        name="pipeline",
    )(tokens, norm_gain, offset_bias, w_query, w_key, w_value, w_out)
    return pl.pallas_call(
        store_kernel,
        out_shape=jax.ShapeDtypeStruct((own, features), bf16),
        in_specs=[whole],
        out_specs=anywhere,
        scratch_shapes=[dma],
        compiler_params=pltpu.CompilerParams(vmem_limit_bytes=2**20),
        name="store",
    )(mixed)


def on_device(tokens, norm_gain, w_query, w_key, w_value, w_out, offset_bias):
    n, m = lax.axis_size("sp"), lax.axis_size("tp")
    own, features = tokens.shape
    total, width = own * n, features // n
    fits = total * (20 * width + 60 * w_query.shape[2]) < VMEM_MOST
    even = offset_bias.shape[1] % 2 == 0 and m == 4 and n > 2
    if fits and even and own % CHUNK == 0 and width % 512 == 0 and total >= KR * GRID_W:
        return staged(tokens, norm_gain, w_query, w_key, w_value, w_out, offset_bias)
    return general(tokens, norm_gain, w_query, w_key, w_value, w_out, offset_bias)


def solution(mesh):
    return jax.shard_map(
        on_device,
        mesh=mesh,
        in_specs=(
            P(("grp", "sp"), None),
            P(),
            P(None, "sp", "tp"),
            P(None, "sp", "tp"),
            P(None, "sp", "tp"),
            P(None, "tp", "sp"),
            P(None, "tp", None, None),
        ),
        out_specs=P(("grp", "sp"), None),
        check_vma=False,
    )
```

```python
import functools

import jax
import jax.numpy as jnp
from jax import lax
from jax.experimental import pallas as pl
from jax.experimental.pallas import tpu as pltpu
from jax.sharding import PartitionSpec as P

HD = 128
GRID_W = 64
KR = 8
KC = 16
LAYERS = 2


norm_eps = 1e-06


def with_halo(block, sides, width):
    for axis, dim in sides:
        count = lax.axis_size(axis)
        forward = [(i, i + 1) for i in range(count - 1)]
        backward = [(target, source) for source, target in forward]
        low = lax.ppermute(
            lax.slice_in_dim(block, block.shape[dim] - width, None, axis=dim), axis, forward
        )
        high = lax.ppermute(lax.slice_in_dim(block, 0, width, axis=dim), axis, backward)
        block = jnp.concatenate([low, block, high], axis=dim)
    return block


def rms_rows(values, gain):
    wide = values.astype(jnp.float32)
    scaled = wide * lax.rsqrt(jnp.mean(wide * wide, axis=-1, keepdims=True) + norm_eps)
    return (scaled * gain.astype(jnp.float32)).astype(jnp.bfloat16)


def general(tokens, norm_gain, w_query, w_key, w_value, w_out, offset_bias):
    sp_count = lax.axis_size("sp")
    sp_index = lax.axis_index("sp")
    tok_rows = tokens.shape[0]
    local_rows = tok_rows // GRID_W
    grid_rows = local_rows * sp_count
    heads_here = offset_bias.shape[1]
    head_width = heads_here * HD
    reach = KR // 2
    scale = HD ** (-0.5)
    columns = jnp.arange(GRID_W, dtype=jnp.int32)
    col_first = jnp.clip(columns - KC // 2, 0, GRID_W - KC)
    col_inside = (columns[None, :] >= col_first[:, None]) & (
        columns[None, :] < col_first[:, None] + KC
    )
    col_offset = jnp.clip(columns[None, :] - columns[:, None], 1 - KC, KC - 1) + KC - 1
    col_onehot = (
        jnp.arange(2 * KC - 1, dtype=jnp.int32)[:, None, None] == col_offset[None, :, :]
    ).astype(jnp.float32)
    first_row = sp_index * local_rows
    own_rows = first_row + jnp.arange(local_rows, dtype=jnp.int32)
    row_first = jnp.clip(own_rows - reach, 0, grid_rows - KR)
    band_start = row_first - first_row + reach
    row_offset = (
        row_first[:, None] + jnp.arange(KR, dtype=jnp.int32)[None, :] - own_rows[:, None] + KR - 1
    )
    row_onehot = (
        row_offset[:, :, None] == jnp.arange(2 * KR - 1, dtype=jnp.int32)[None, None, :]
    ).astype(jnp.float32)
    qkv_weight = jnp.concatenate([w_query, w_key, w_value], axis=2)
    residual = lax.all_to_all(tokens, "sp", split_axis=1, concat_axis=0, tiled=True)
    width = residual.shape[1]
    features = width * sp_count
    for layer_index in range(LAYERS):
        wide = residual.astype(jnp.float32)
        squares = lax.psum_scatter(
            jnp.sum(wide * wide, axis=-1, keepdims=True), "sp", scatter_dimension=0, tiled=True
        )
        inverse = lax.rsqrt(squares / features + norm_eps)
        gain = lax.dynamic_slice_in_dim(norm_gain[layer_index], sp_index * width, width, 0)
        gained = (wide * gain.astype(jnp.float32)).astype(jnp.bfloat16)
        partial = jnp.dot(gained, qkv_weight[layer_index], preferred_element_type=jnp.float32)
        mine = lax.psum_scatter(
            partial.astype(jnp.bfloat16), "sp", scatter_dimension=0, tiled=True
        )
        mine = (mine.astype(jnp.float32) * inverse).astype(jnp.bfloat16)
        queries = mine[:, :head_width].reshape(local_rows, GRID_W, heads_here, HD)
        key_values = mine[:, head_width:].reshape(local_rows, GRID_W, 2 * head_width)
        padded = with_halo(key_values, (("sp", 0),), reach)
        bands = jax.vmap(lambda band_begin: lax.dynamic_slice_in_dim(padded, band_begin, KR, 0))(
            band_start
        )
        band_keys = bands[..., :head_width].reshape(local_rows, KR, GRID_W, heads_here, HD)
        band_values = bands[..., head_width:].reshape(local_rows, KR, GRID_W, heads_here, HD)
        col_bias = jnp.einsum(
            "hro,oqk->hrqk", offset_bias[layer_index], col_onehot, precision=lax.Precision.HIGHEST
        )
        full_bias = jnp.einsum(
            "ijr,hrqk->hiqjk", row_onehot, col_bias, precision=lax.Precision.HIGHEST
        )
        scores = jnp.einsum(
            "iqhd,ijkhd->hiqjk", queries, band_keys, preferred_element_type=jnp.float32
        )
        scores = scores * scale + full_bias
        scores = jnp.where(col_inside[None, None, :, None, :], scores, -jnp.inf)
        flattened = scores.reshape(heads_here, local_rows, GRID_W, KR * GRID_W)
        weights = jax.nn.softmax(flattened, axis=-1).astype(jnp.bfloat16)
        weights = weights.reshape(heads_here, local_rows, GRID_W, KR, GRID_W)
        attended = jnp.einsum(
            "hiqjk,ijkhd->iqhd", weights, band_values, preferred_element_type=jnp.float32
        )
        attended = attended.astype(jnp.bfloat16).reshape(tok_rows, head_width)
        every = lax.all_gather(attended, "sp", axis=0, tiled=True)
        share = jnp.dot(every, w_out[layer_index], preferred_element_type=jnp.float32)
        branch = lax.psum(share.astype(jnp.bfloat16), "tp").astype(jnp.float32)
        residual = (residual.astype(jnp.float32) + branch).astype(jnp.bfloat16)
    return lax.all_to_all(residual, "sp", split_axis=0, concat_axis=1, tiled=True)


MESH = pl.DeviceIdType.MESH
VMEM_MOST = 56 * 2**20
CHUNK = GRID_W
HOP = 2
LEAD, OWN_LEAD, TURN, PASS = 6, 4, 2, 1
PARTS = 3
FIRST, RELAY = 2, 1
MEET, CROSS, FRESH = 0, 2, 0
FAR = 1
SPREAD = 0
HOP_TWO = 0
LAST_RELAY = 1
DIRECT = 0
MORE = 0
GROUPS = [(0, 0, 8), (2, 0, 2), (2, 2, 2), (3, 0, 4)]
LAST_DIRECT = 0
DIRECT_LAG = 2


def greet(peers):
    barrier = pltpu.get_barrier_semaphore()
    for axis, index in peers:
        pl.semaphore_signal(barrier, inc=1, device_id={axis: index}, device_id_type=MESH)
    pl.semaphore_wait(barrier, len(peers))


def remote(src, dst, send, recv, axis, index):
    return pltpu.make_async_remote_copy(
        src_ref=src, dst_ref=dst, send_sem=send, recv_sem=recv,
        device_id={axis: index}, device_id_type=MESH,
    )


def span(start, size):
    return pl.ds(pl.multiple_of(start, size), size)


def row_plan(count, last):
    need = [min(max(r + KR - 1 - KR // 2, KR - 1), count - 1) - KR + 1 for r in range(count)]
    if not last and not DIRECT:
        return [(r, 1) for r in range(count)]
    if not last:
        plan, done = [], 0
        while done < count:
            ready = sum(v <= len(plan) for v in need) - done
            plan.append((done, min(ready, 2)))
            done += plan[-1][1]
        return plan
    ticks = need[-1]
    early = sum(v < ticks for v in need)
    sizes = [early // ticks + (t >= ticks - early % ticks) for t in range(ticks)] + [count - early]
    starts = [sum(sizes[:t]) for t in range(ticks + 1)]
    return list(zip(starts, sizes))


def pick(table, index):
    value = jnp.int32(table[-1])
    for i in range(len(table) - 2, -1, -1):
        value = jnp.where(index <= i, jnp.int32(table[i]), value)
    return value


def pipeline_kernel(
    n, m, tok_any, gain_ref, offset_ref, wq_any, wk_any, wv_any, wo_any, out_ref,
    tok_ref, wq, wk, wv, wo, xs, part, outbox, inbox, qkv, bias, sq_own, sq_in, box,
    give, take, pair, cross_in, fin, padded,
    w_sem, sp_s, sp_r, spx_s, spx_r, fresh_s, fresh_r, ch_s, ch_r, sq_s, sq_r,
    at_s, at_r, gv_s, gv_r, cr_s, cr_r, fin_s, fin_r, fx_s, fx_r, fp_s, fp_r,
):
    me, t = lax.axis_index("sp"), lax.axis_index("tp")
    core = lax.rem(t, 2)
    side = lax.div(t, 2)
    partner = t + 1 - 2 * core
    cross = lax.rem(t + m // 2, m)
    layers, tokens, width = xs.shape
    own, features = tok_ref.shape
    cols = box.shape[3]
    heads = cols // HD
    half, quarter = width // 2, width // 4
    count, per = tokens // CHUNK, own // CHUNK
    scale = HD ** (-0.5)
    at_end = (me == 0) | (me == n - 1)
    ends = (n - 1, 0)
    lanes = span(core * half, half)
    other = span((1 - core) * half, half)
    mine_q = core * half + side * quarter
    their_q = core * half + (1 - side) * quarter
    places = (me, n - 1 - me)
    afters = (me + 1, me - 1)

    loaded = pltpu.make_async_copy(tok_any, tok_ref, w_sem.at[0, 4])
    loaded.start()
    weights = []
    for layer in range(layers):
        for i, (any_ref, ref) in enumerate(((wq_any, wq), (wk_any, wk), (wv_any, wv), (wo_any, wo))):
            copy = pltpu.make_async_copy(any_ref.at[layer], ref.at[layer], w_sem.at[layer, i])
            copy.start()
            weights.append(copy)
    greet(
        [("sp", lax.rem(me + k, n)) for k in range(1, n)] + [("tp", partner), ("tp", cross)]
    )
    loaded.wait()

    def rows_of(c):
        return span(c * CHUNK, CHUNK)

    def scatter(c):
        @pl.when(lax.div(c, per) == me)
        def _():
            here = span((c - me * per) * CHUNK, CHUNK)
            for k in range(1, n):
                to = jnp.where(me < n // 2, n - k + jnp.where(n - k > me, 0, -1), k - 1 + jnp.where(k > me, 1, 0))
                remote(
                    tok_ref.at[here, span(to * width + mine_q, quarter)],
                    xs.at[0, rows_of(c), span(mine_q, quarter)],
                    sp_s, sp_r.at[c], "sp", to,
                ).start()
            xs[0, rows_of(c), :] = tok_ref[here, span(me * width, width)]

    def pass_cross(c):
        @pl.when(lax.div(c, per) != me)
        def _():
            here = xs.at[0, rows_of(c), span(mine_q, quarter)]
            remote(here, here, sp_s, sp_r.at[c], "tp", cross).wait_recv()
            remote(here, here, spx_s, spx_r.at[c], "tp", cross).start()

    def pass_partner(c):
        @pl.when(lax.div(c, per) != me)
        def _():
            there = xs.at[0, rows_of(c), span(their_q, quarter)]
            remote(there, there, spx_s, spx_r.at[c], "tp", cross).wait_recv()
            here = xs.at[0, rows_of(c), lanes]
            remote(here, here, fresh_s.at[0], fresh_r.at[c], "tp", partner).start()

    def prepare(layer, c):
        rows = rows_of(c)

        def arrived():
            there = xs.at[layer, rows, other]
            remote(there, there, fresh_s.at[layer], fresh_r.at[c], "tp", partner).wait_recv()

        if layer == 0:
            pl.when(lax.div(c, per) != me)(arrived)
        else:
            arrived()
        gain = gain_ref[layer:layer + 1, span(me * width, width)].astype(jnp.float32)
        wide = xs[layer, rows, :].astype(jnp.float32)
        gained = (wide * gain).astype(jnp.bfloat16)
        for way in range(2):
            lo = (1 - way) * cols
            for j, w_ref in enumerate((wq, wk, wv)):
                part[way, rows, j * cols:(j + 1) * cols] = jnp.dot(
                    gained, w_ref[layer, :, lo:lo + cols], preferred_element_type=jnp.float32
                )

    def measure(layer, c):
        wide = xs[layer, rows_of(c), :].astype(jnp.float32)
        squares = wide * wide
        high = squares.astype(jnp.bfloat16)
        low = (squares - high.astype(jnp.float32)).astype(jnp.bfloat16)
        ones = jnp.ones((8, width), jnp.bfloat16)
        nt = (((1,), (1,)), ((), ()))
        total = lax.dot_general(
            ones, high, nt, preferred_element_type=jnp.float32
        ) + lax.dot_general(ones, low, nt, preferred_element_type=jnp.float32)
        sq_own[layer, c] = jnp.concatenate([total] * (128 // CHUNK), axis=1)
        for e, end in enumerate(ends):
            @pl.when(me != end)
            def _(e=e, end=end):
                remote(
                    sq_own.at[layer, c], sq_in.at[layer, c, me],
                    sq_s.at[layer, e], sq_r.at[c], "sp", end,
                ).start()

    pieces = [slice(i * 3 * cols // PARTS, (i + 1) * 3 * cols // PARTS) for i in range(PARTS)]

    def chain_copy(layer, way, c, i):
        rows = rows_of(c)
        return remote(
            outbox.at[layer, way, rows, pieces[i]], inbox.at[layer, way, rows, pieces[i]],
            ch_s.at[layer, way], ch_r.at[way, c, i], "sp", afters[way],
        )

    def first_link(layer, c):
        for way in range(2):
            @pl.when(places[way] == 0)
            def _(way=way):
                for i, at in enumerate(pieces):
                    outbox[layer, way, rows_of(c), at] = part[way, rows_of(c), at].astype(jnp.bfloat16)
                    chain_copy(layer, way, c, i).start()

    def link(way, layer, c):
        rows = rows_of(c)
        place = places[way]

        def total(i):
            chain_copy(layer, way, c, i).wait_recv()
            return part[way, rows, pieces[i]] + inbox[layer, way, rows, pieces[i]].astype(jnp.float32)

        @pl.when(place < n - 1)
        def _():
            for i, at in enumerate(pieces):
                outbox[layer, way, rows, at] = total(i).astype(jnp.bfloat16)
                chain_copy(layer, way, c, i).start()

        @pl.when(place == n - 1)
        def _():
            squares = sq_own[layer, c]
            others = sq_in.at[layer, c, 0:n - 1]
            remote(others, others, sq_s.at[layer, 0], sq_r.at[c], "sp", n - 1 - me).wait_recv()
            for k in range(1, n):
                squares = squares + sq_in[layer, c, lax.rem(me + k, n)]
            scaled = lax.rsqrt(squares / features + norm_eps)
            inverse = jnp.concatenate([scaled] * 16, axis=0).T[:CHUNK, :1]
            for i, at in enumerate(pieces):
                qkv[layer, rows, at] = (total(i) * inverse).astype(jnp.bfloat16)

    def make_bias(o):
        first_head = jnp.where(me == n - 1, heads, 0)
        lane = lax.broadcasted_iota(jnp.int32, (CHUNK, 2 * GRID_W), 1)
        query = lax.broadcasted_iota(jnp.int32, (CHUNK, 2 * GRID_W), 0)
        key = jnp.where(lane < GRID_W, lane, lane - GRID_W)
        begin = jnp.clip(query - KC // 2, 0, GRID_W - KC)
        inside = (key >= begin) & (key < begin + KC)
        for layer in range(layers):
            for h in range(heads):
                def rolled(i, shift, layer=layer, h=h):
                    row = padded[layer, first_head + h, pl.ds(i, 1), :]
                    return pltpu.roll(
                        jnp.broadcast_to(row, (CHUNK, 2 * GRID_W)), shift, 1, stride=1, stride_axis=0
                    )

                both = jnp.where(
                    lane < GRID_W, rolled(o, 2 * GRID_W - KC + 1), rolled(o + 1, GRID_W - KC + 1)
                )
                bias[layer, h, o] = jnp.where(inside, both, -jnp.inf)

    @pl.when(at_end)
    def _():
        padded[...] = jnp.zeros_like(padded)
        for layer in range(layers):
            for h in range(2 * heads):
                padded[layer, h, 0:2 * KR - 1, 0:2 * KC - 1] = offset_ref[layer, h]

    way_here = jnp.where(me == 0, 0, 1)
    after_here = jnp.where(me == 0, 1, n - 2)

    def direct(layer, r):
        return r < DIRECT if layer < layers - 1 else r >= count - LAST_DIRECT

    def publish(layer, r):
        here = box.at[layer, way_here, rows_of(r), :]

        def send(to):
            remote(
                here, here, at_s.at[layer, way_here], at_r.at[way_here, r], "sp", to
            ).start()

        @pl.when(direct(layer, r))
        def _():
            for k in range(n - 1, 0, -1):
                send(jnp.where(me == 0, k, n - 1 - k))

        pl.when(jnp.logical_not(direct(layer, r)))(lambda: send(after_here))

    def attend(layer, r, several=1):
        @pl.when(at_end)
        def _():
            jobs = []
            for i in range(several):
                first = jnp.clip(r + i - KR // 2, 0, count - KR)
                band = pl.ds(pl.multiple_of(first * CHUNK, CHUNK), KR * CHUNK)
                for h in range(heads):
                    at = [slice(j * cols + h * HD, j * cols + (h + 1) * HD) for j in range(3)]
                    scores = lax.dot_general(
                        qkv[layer, rows_of(r + i), at[0]], qkv[layer, band, at[1]],
                        (((1,), (1,)), ((), ())), preferred_element_type=jnp.float32,
                    )
                    a = first - r - i + KR - 1
                    table = jnp.concatenate([bias[layer, h, a + 2 * b] for b in range(KR // 2)], axis=1)
                    jobs.append((scores * scale + table, band, at[2]))
            jobs = [(jnp.exp(w - jnp.max(w, axis=-1, keepdims=True)), b, v) for w, b, v in jobs]
            outs = [
                jnp.dot(w.astype(jnp.bfloat16), qkv[layer, b, v], preferred_element_type=jnp.float32)
                / jnp.sum(w, axis=-1, keepdims=True)
                for w, b, v in jobs
            ]
            for i in range(several):
                both = jnp.concatenate(outs[i * heads:(i + 1) * heads], axis=1)
                box[layer, way_here, rows_of(r + i), :] = both.astype(jnp.bfloat16)
                publish(layer, r + i)

    def box_copy(layer, way, r):
        here = box.at[layer, way, rows_of(r), :]
        return remote(here, here, at_s.at[layer, way], at_r.at[way, r], "sp", afters[way])

    def relay(way, layer, r):
        @pl.when(jnp.logical_not(direct(layer, r)))
        def _():
            box_copy(layer, way, r).wait_recv()
            box_copy(layer, way, r).start()

    def give_copy(layer, r):
        rows = rows_of(r)
        return remote(
            give.at[layer, rows, :], take.at[layer, rows, :],
            gv_s.at[layer], gv_r.at[r], "tp", partner,
        )

    def cross_copy(layer, r, whole):
        at = slice(None) if whole else span((1 - side) * quarter, quarter)
        rows = rows_of(r)
        return remote(
            pair.at[layer, rows, at], cross_in.at[layer, rows, at],
            cr_s.at[layer], cr_r.at[layer, r], "tp", cross,
        )

    def multiply(layer, r):
        for way in range(2):
            @pl.when((places[way] == n - 1) | ((places[way] > 0) & direct(layer, r)))
            def _(way=way):
                box_copy(layer, way, r).wait_recv()
        rows = rows_of(r)

        def share(at):
            return jnp.dot(
                box[layer, 0, rows, :], wo[layer, :cols, at], preferred_element_type=jnp.float32
            ) + jnp.dot(box[layer, 1, rows, :], wo[layer, cols:, at], preferred_element_type=jnp.float32)

        give[layer, rows, :] = share(other).astype(jnp.bfloat16)
        give_copy(layer, r).start()
        pair[layer, rows, :] = share(lanes).astype(jnp.bfloat16)

    def meet(layer, r):
        rows = rows_of(r)
        give_copy(layer, r).wait_recv()
        pair[layer, rows, :] = (
            pair[layer, rows, :].astype(jnp.float32) + take[layer, rows, :].astype(jnp.float32)
        ).astype(jnp.bfloat16)
        if layer < layers - 1:
            cross_copy(layer, r, True).start()
            return
        owner = lax.div(r, per)
        pl.when(owner == me)(lambda: cross_copy(layer, r, True).start())
        pl.when(owner != me)(lambda: cross_copy(layer, r, False).start())

    def out_at(q, lane, size):
        return out_ref.at[span(q * CHUNK, CHUNK), span(lane, size)]

    def finish(layer, r):
        rows = rows_of(r)

        def new(at, sub):
            branch = pair[layer, rows, sub].astype(jnp.float32) + cross_in[layer, rows, sub].astype(jnp.float32)
            return (xs[layer, rows, at].astype(jnp.float32) + branch).astype(jnp.bfloat16)

        if layer < layers - 1:
            cross_copy(layer, r, True).wait_recv()
            here = xs.at[layer + 1, rows, lanes]
            here[...] = new(lanes, slice(None))
            remote(here, here, fresh_s.at[layer + 1], fresh_r.at[r], "tp", partner).start()
            return
        owner, q = lax.div(r, per), lax.rem(r, per)
        @pl.when(owner == me)
        def _():
            cross_copy(layer, r, True).wait_recv()
            here = out_at(q, me * width + core * half, half)
            here[...] = new(lanes, slice(None))
            remote(here, here, fp_s, fp_r, "tp", partner).start()

        @pl.when(owner != me)
        def _():
            cross_copy(layer, r, False).wait_recv()
            fin[rows, :] = new(span(mine_q, quarter), span(side * quarter, quarter))
            remote(
                fin.at[rows, :], out_at(q, me * width + mine_q, quarter),
                fin_s, fin_r.at[me, q], "sp", owner,
            ).start()

    def hand_cross(q):
        for k in range(1, n):
            source = lax.rem(me + k, n)
            here = out_at(q, source * width + mine_q, quarter)
            remote(here, here, fin_s, fin_r.at[source, q], "sp", source).wait_recv()
            remote(here, here, fx_s, fx_r.at[q], "tp", cross).start()

    def hand_partner(q):
        every = fin.at[0:(n - 1) * CHUNK, :]
        remote(every, every, fx_s, fx_r.at[q], "tp", cross).wait_recv()
        for k in range(1, n):
            source = lax.rem(me + k, n)
            here = out_at(q, source * width + core * half, half)
            remote(here, here, fp_s, fp_r, "tp", partner).start()

    through = (n - 1) * HOP - HOP_TWO
    plans = [row_plan(count, layer == layers - 1) for layer in range(layers)]
    share_at = 0
    for j, (first, size) in enumerate(plans[0]):
        for row in range(first, first + size):
            late = DIRECT_LAG if row < DIRECT else FIRST + (n - 2) * RELAY
            share_at = max(share_at, j + late - row)
    meet_at = share_at + MEET
    finish_at = meet_at + CROSS
    settle = finish_at + FRESH
    last_share = FIRST + (n - 2) * LAST_RELAY + MORE
    last_finish = last_share + MEET + CROSS
    starts = [layer * (through + KR - 1 + settle) for layer in range(layers)]
    singles = [(row, 1) for row in range(count)]
    shares = plans[-1]
    if LAST_DIRECT:
        shares = shares[:-2] + [(shares[-2][0], shares[-2][1] + shares[-1][1])]
    final = starts[-1] + through + KR - 1 + len(shares) + last_finish

    @pl.loop(-LEAD, final)
    def _(tick):
        def chunks(stage, late, layer, extra=True):
            c = tick - late - starts[layer]

            @pl.when((c >= 0) & (c < count) & extra)
            def _():
                stage(layer, c)

        def grid_rows(stage, late, layer, extra=True, plan=None, behind=None):
            j = tick - late - starts[layer] - through - (KR - 1)
            plan = plan or plans[layer]

            @pl.when((j >= 0) & (j < len(plan)) & extra)
            def _():
                if all(size == 1 for _, size in plan):
                    stage(layer, j)
                    return
                first, size = pick([p[0] for p in plan], j), pick([p[1] for p in plan], j)

                @pl.loop(first, first + size)
                def _(r):
                    stage(layer, r)
                    if behind:
                        pl.when(r > first)(lambda: behind(layer, r - 1))

                if behind:
                    behind(layer, first + size - 1)

        lead = per * me + OWN_LEAD if SPREAD == 0 else jnp.where(me == 1, LEAD, per * me + OWN_LEAD)

        def relays(low, high, which):
            for layer in which:
                for way in range(2):
                    place = places[way]
                    inner = (place >= low) & (place < high)
                    grid_rows(functools.partial(relay, way), FIRST + (place - 1) * (RELAY if layer < layers - 1 else LAST_RELAY), layer, inner)

        @pl.when(tick == 0)
        def _():
            for copy in weights:
                copy.wait()

        last = layers - 1
        if FAR == 0:
            relays(2, n - 1, [last])
        relays(1, 2, range(layers))
        if FAR == 1:
            relays(2, n - 1, range(layers))
        chunks(lambda _, c: pass_cross(c), -TURN, 0)
        for layer in range(layers):
            for way in range(2):
                place = places[way]
                early = (place > 0) & (place != 2) if HOP_TWO else place > 0
                chunks(functools.partial(link, way), HOP * place - jnp.where(place >= 2, HOP_TWO, 0), layer, early)
        for layer in range(last):
            grid_rows(finish, finish_at, layer, plan=singles)
        groups = [(i * per + a, b) for i, a, b in GROUPS]
        waits = len(shares) - len(groups)
        grid_rows(finish, last_finish + waits, last, plan=groups)
        for layer in range(layers):
            grid_rows(attend, 0, layer)
        if FAR != 1:
            relays(2, n - 1, range(last) if FAR == 0 else range(layers))
        if HOP_TWO:
            for layer in range(layers):
                for way in range(2):
                    chunks(functools.partial(link, way), 2 * HOP - HOP_TWO, layer, places[way] == 2)
        for layer in range(last):
            grid_rows(multiply, share_at, layer, plan=singles)
        grid_rows(multiply, last_share, last, plan=shares, behind=meet)
        for layer in range(layers):
            chunks(prepare, jnp.where(at_end, 0, HOP - 1), layer)
            chunks(first_link, 0, layer, at_end)
        for layer in range(last):
            grid_rows(meet, meet_at, layer, plan=singles)
        for layer in range(layers):
            chunks(measure, jnp.where(at_end, 0, HOP - 1), layer)
        chunks(lambda _, c: pass_partner(c), -PASS, 0)
        chunks(lambda _, c: scatter(c), -lead, 0)

        @pl.when((tick >= -1) & (tick < 2 * KR - 3) & at_end)
        def _():
            make_bias(tick + 1)

    pl.loop(0, per)(hand_cross)

    @pl.loop(0, per)
    def _(q):
        hand_partner(q)

    every = xs.at[0, :, 0:half]
    remote(every, every, fp_s, fp_r, "tp", partner).wait_recv()

    def sent(ref, sem, recv):
        remote(ref, ref, sem, recv, "tp", partner).wait_send()

    away = fin.at[0:tokens - own, :]
    sent(away, sp_s, sp_r.at[0])
    sent(away, spx_s, spx_r.at[0])
    sent(away, fin_s, fin_r.at[0, 0])
    sent(away, fx_s, fx_r.at[0])
    sent(xs.at[0, :, 0:half], fp_s, fp_r)
    sent(xs.at[0, 0:tokens - own, 0:half], fresh_s.at[0], fresh_r.at[0])
    for layer in range(layers):
        if layer > 0:
            sent(xs.at[layer, :, 0:half], fresh_s.at[layer], fresh_r.at[0])
        sent(give.at[layer], gv_s.at[layer], gv_r.at[0])
        if layer < layers - 1:
            sent(pair.at[layer], cr_s.at[layer], cr_r.at[layer, 0])
        else:
            sent(fin, cr_s.at[layer], cr_r.at[layer, 0])
            sent(fin.at[0:own, :], cr_s.at[layer], cr_r.at[layer, 0])
        for way in range(2):
            @pl.when(places[way] < n - 1)
            def _(way=way):
                sent(outbox.at[layer, way], ch_s.at[layer, way], ch_r.at[way, 0, 0])
                straight = DIRECT if layer < layers - 1 else LAST_DIRECT
                sent(box.at[layer, way, straight * CHUNK:, :], at_s.at[layer, way], at_r.at[way, 0])
                if straight:
                    @pl.when(places[way] == 0)
                    def _():
                        several = box.at[layer, way, 0:(n - 1) * straight * CHUNK, :]
                        sent(several, at_s.at[layer, way], at_r.at[way, 0])

            @pl.when(me != ends[way])
            def _(way=way):
                sent(sq_own.at[layer], sq_s.at[layer, way], sq_r.at[0])


def store_kernel(mixed_ref, out_ref, sem):
    copy = pltpu.make_async_copy(mixed_ref, out_ref, sem)
    copy.start()
    copy.wait()


def staged(tokens, norm_gain, w_query, w_key, w_value, w_out, offset_bias):
    n, m = lax.axis_size("sp"), lax.axis_size("tp")
    own, features = tokens.shape
    layers = norm_gain.shape[0]
    width, total = features // n, own * n
    heads = offset_bias.shape[1] // 2
    cols = heads * HD
    count, per = total // CHUNK, own // CHUNK
    dma = pltpu.SemaphoreType.DMA
    bf16, f32 = jnp.bfloat16, jnp.float32
    space = pltpu.VMEM
    whole, anywhere = pl.BlockSpec(memory_space=space), pl.BlockSpec(memory_space=pl.ANY)
    mixed = pl.pallas_call(
        functools.partial(pipeline_kernel, n, m),
        out_shape=space((own, features), bf16),
        in_specs=[anywhere] + [whole] * 2 + [anywhere] * 4,
        out_specs=whole,
        scratch_shapes=[
            *[space(w.shape, bf16) for w in (tokens, w_query, w_key, w_value, w_out)],
            space((layers, total, width), bf16),
            space((2, total, 3 * cols), f32),
            space((layers, 2, total, 3 * cols), bf16),
            space((layers, 2, total, 3 * cols), bf16),
            space((layers, total, 3 * cols), bf16),
            space((layers, heads, 2 * KR - 2, CHUNK, 2 * GRID_W), f32),
            space((layers, count, 8, 128), f32),
            space((layers, count, n, 8, 128), f32),
            space((layers, 2, total, cols), bf16),
            *[space((layers, total, width // 2), bf16)] * 4,
            space((total, width // 4), bf16),
            space((layers, 2 * heads, 2 * KR, 2 * GRID_W), f32),
            dma((layers, 5)),
            dma, dma((count,)), dma, dma((count,)), dma((layers,)), dma((count,)),
            dma((layers, 2)), dma((2, count, PARTS)), dma((layers, 2)), dma((count,)),
            dma((layers, 2)), dma((2, count)),
            dma((layers,)), dma((count,)), dma((layers,)), dma((layers, count)),
            dma, dma((n, per)), dma, dma((per,)), dma, dma,
        ],
        compiler_params=pltpu.CompilerParams(
            collective_id=1, has_side_effects=True, vmem_limit_bytes=VMEM_MOST
        ),
        name="pipeline",
    )(tokens, norm_gain, offset_bias, w_query, w_key, w_value, w_out)
    return pl.pallas_call(
        store_kernel,
        out_shape=jax.ShapeDtypeStruct((own, features), bf16),
        in_specs=[whole],
        out_specs=anywhere,
        scratch_shapes=[dma],
        compiler_params=pltpu.CompilerParams(vmem_limit_bytes=2**20),
        name="store",
    )(mixed)


def on_device(tokens, norm_gain, w_query, w_key, w_value, w_out, offset_bias):
    n, m = lax.axis_size("sp"), lax.axis_size("tp")
    own, features = tokens.shape
    total, width = own * n, features // n
    fits = total * (20 * width + 60 * w_query.shape[2]) < VMEM_MOST
    even = offset_bias.shape[1] % 2 == 0 and m == 4 and n > 2
    if fits and even and own % CHUNK == 0 and width % 512 == 0 and total >= KR * GRID_W:
        return staged(tokens, norm_gain, w_query, w_key, w_value, w_out, offset_bias)
    return general(tokens, norm_gain, w_query, w_key, w_value, w_out, offset_bias)


def solution(mesh):
    return jax.shard_map(
        on_device,
        mesh=mesh,
        in_specs=(
            P(("grp", "sp"), None),
            P(),
            P(None, "sp", "tp"),
            P(None, "sp", "tp"),
            P(None, "sp", "tp"),
            P(None, "tp", "sp"),
            P(None, "tp", None, None),
        ),
        out_specs=P(("grp", "sp"), None),
        check_vma=False,
    )
```

```python
import functools

import jax
import jax.numpy as jnp
from jax import lax
from jax.experimental import pallas as pl
from jax.experimental.pallas import tpu as pltpu
from jax.sharding import PartitionSpec as P

HD = 128
GRID_W = 64
KR = 8
KC = 16
LAYERS = 2


norm_eps = 1e-06


def with_halo(block, sides, width):
    for axis, dim in sides:
        count = lax.axis_size(axis)
        forward = [(i, i + 1) for i in range(count - 1)]
        backward = [(target, source) for source, target in forward]
        low = lax.ppermute(
            lax.slice_in_dim(block, block.shape[dim] - width, None, axis=dim), axis, forward
        )
        high = lax.ppermute(lax.slice_in_dim(block, 0, width, axis=dim), axis, backward)
        block = jnp.concatenate([low, block, high], axis=dim)
    return block


def rms_rows(values, gain):
    wide = values.astype(jnp.float32)
    scaled = wide * lax.rsqrt(jnp.mean(wide * wide, axis=-1, keepdims=True) + norm_eps)
    return (scaled * gain.astype(jnp.float32)).astype(jnp.bfloat16)


def general(tokens, norm_gain, w_query, w_key, w_value, w_out, offset_bias):
    sp_count = lax.axis_size("sp")
    sp_index = lax.axis_index("sp")
    tok_rows = tokens.shape[0]
    local_rows = tok_rows // GRID_W
    grid_rows = local_rows * sp_count
    heads_here = offset_bias.shape[1]
    head_width = heads_here * HD
    reach = KR // 2
    scale = HD ** (-0.5)
    columns = jnp.arange(GRID_W, dtype=jnp.int32)
    col_first = jnp.clip(columns - KC // 2, 0, GRID_W - KC)
    col_inside = (columns[None, :] >= col_first[:, None]) & (
        columns[None, :] < col_first[:, None] + KC
    )
    col_offset = jnp.clip(columns[None, :] - columns[:, None], 1 - KC, KC - 1) + KC - 1
    col_onehot = (
        jnp.arange(2 * KC - 1, dtype=jnp.int32)[:, None, None] == col_offset[None, :, :]
    ).astype(jnp.float32)
    first_row = sp_index * local_rows
    own_rows = first_row + jnp.arange(local_rows, dtype=jnp.int32)
    row_first = jnp.clip(own_rows - reach, 0, grid_rows - KR)
    band_start = row_first - first_row + reach
    row_offset = (
        row_first[:, None] + jnp.arange(KR, dtype=jnp.int32)[None, :] - own_rows[:, None] + KR - 1
    )
    row_onehot = (
        row_offset[:, :, None] == jnp.arange(2 * KR - 1, dtype=jnp.int32)[None, None, :]
    ).astype(jnp.float32)
    qkv_weight = jnp.concatenate([w_query, w_key, w_value], axis=2)
    residual = lax.all_to_all(tokens, "sp", split_axis=1, concat_axis=0, tiled=True)
    width = residual.shape[1]
    features = width * sp_count
    for layer_index in range(LAYERS):
        wide = residual.astype(jnp.float32)
        squares = lax.psum_scatter(
            jnp.sum(wide * wide, axis=-1, keepdims=True), "sp", scatter_dimension=0, tiled=True
        )
        inverse = lax.rsqrt(squares / features + norm_eps)
        gain = lax.dynamic_slice_in_dim(norm_gain[layer_index], sp_index * width, width, 0)
        gained = (wide * gain.astype(jnp.float32)).astype(jnp.bfloat16)
        partial = jnp.dot(gained, qkv_weight[layer_index], preferred_element_type=jnp.float32)
        mine = lax.psum_scatter(
            partial.astype(jnp.bfloat16), "sp", scatter_dimension=0, tiled=True
        )
        mine = (mine.astype(jnp.float32) * inverse).astype(jnp.bfloat16)
        queries = mine[:, :head_width].reshape(local_rows, GRID_W, heads_here, HD)
        key_values = mine[:, head_width:].reshape(local_rows, GRID_W, 2 * head_width)
        padded = with_halo(key_values, (("sp", 0),), reach)
        bands = jax.vmap(lambda band_begin: lax.dynamic_slice_in_dim(padded, band_begin, KR, 0))(
            band_start
        )
        band_keys = bands[..., :head_width].reshape(local_rows, KR, GRID_W, heads_here, HD)
        band_values = bands[..., head_width:].reshape(local_rows, KR, GRID_W, heads_here, HD)
        col_bias = jnp.einsum(
            "hro,oqk->hrqk", offset_bias[layer_index], col_onehot, precision=lax.Precision.HIGHEST
        )
        full_bias = jnp.einsum(
            "ijr,hrqk->hiqjk", row_onehot, col_bias, precision=lax.Precision.HIGHEST
        )
        scores = jnp.einsum(
            "iqhd,ijkhd->hiqjk", queries, band_keys, preferred_element_type=jnp.float32
        )
        scores = scores * scale + full_bias
        scores = jnp.where(col_inside[None, None, :, None, :], scores, -jnp.inf)
        flattened = scores.reshape(heads_here, local_rows, GRID_W, KR * GRID_W)
        weights = jax.nn.softmax(flattened, axis=-1).astype(jnp.bfloat16)
        weights = weights.reshape(heads_here, local_rows, GRID_W, KR, GRID_W)
        attended = jnp.einsum(
            "hiqjk,ijkhd->iqhd", weights, band_values, preferred_element_type=jnp.float32
        )
        attended = attended.astype(jnp.bfloat16).reshape(tok_rows, head_width)
        every = lax.all_gather(attended, "sp", axis=0, tiled=True)
        share = jnp.dot(every, w_out[layer_index], preferred_element_type=jnp.float32)
        branch = lax.psum(share.astype(jnp.bfloat16), "tp").astype(jnp.float32)
        residual = (residual.astype(jnp.float32) + branch).astype(jnp.bfloat16)
    return lax.all_to_all(residual, "sp", split_axis=0, concat_axis=1, tiled=True)


MESH = pl.DeviceIdType.MESH
VMEM_MOST = 56 * 2**20
CHUNK = GRID_W
HOP = 2
LEAD, OWN_LEAD, TURN, PASS = 6, 4, 2, 1
PARTS = 3
FIRST, RELAY = 2, 1
MEET, CROSS, FRESH = 0, 2, 0
FAR = 1
SPREAD = 0
HOP_TWO = 0
LAST_RELAY = 1
DIRECT = 0
MORE = 0
GROUPS = [(0, 0, 8), (2, 0, 2), (2, 2, 2), (3, 0, 4)]
LAST_DIRECT = 0
DIRECT_LAG = 2


def greet(peers):
    barrier = pltpu.get_barrier_semaphore()
    for axis, index in peers:
        pl.semaphore_signal(barrier, inc=1, device_id={axis: index}, device_id_type=MESH)
    pl.semaphore_wait(barrier, len(peers))


def remote(src, dst, send, recv, axis, index):
    return pltpu.make_async_remote_copy(
        src_ref=src, dst_ref=dst, send_sem=send, recv_sem=recv,
        device_id={axis: index}, device_id_type=MESH,
    )


def span(start, size):
    return pl.ds(pl.multiple_of(start, size), size)


def row_plan(count, last):
    need = [min(max(r + KR - 1 - KR // 2, KR - 1), count - 1) - KR + 1 for r in range(count)]
    if not last and not DIRECT:
        return [(r, 1) for r in range(count)]
    if not last:
        plan, done = [], 0
        while done < count:
            ready = sum(v <= len(plan) for v in need) - done
            plan.append((done, min(ready, 2)))
            done += plan[-1][1]
        return plan
    ticks = need[-1]
    early = sum(v < ticks for v in need)
    sizes = [early // ticks + (t >= ticks - early % ticks) for t in range(ticks)] + [count - early]
    starts = [sum(sizes[:t]) for t in range(ticks + 1)]
    return list(zip(starts, sizes))


def pick(table, index):
    value = jnp.int32(table[-1])
    for i in range(len(table) - 2, -1, -1):
        value = jnp.where(index <= i, jnp.int32(table[i]), value)
    return value


def pipeline_kernel(
    n, m, tok_any, gain_ref, offset_ref, wq_any, wk_any, wv_any, wo_any, out_ref,
    tok_ref, wq, wk, wv, wo, xs, part, outbox, inbox, qkv, bias, sq_own, sq_in, box,
    give, take, pair, cross_in, fin, padded,
    w_sem, sp_s, sp_r, spx_s, spx_r, fresh_s, fresh_r, ch_s, ch_r, sq_s, sq_r,
    at_s, at_r, gv_s, gv_r, cr_s, cr_r, fin_s, fin_r, fx_s, fx_r, fp_s, fp_r,
):
    me, t = lax.axis_index("sp"), lax.axis_index("tp")
    core = lax.rem(t, 2)
    side = lax.div(t, 2)
    partner = t + 1 - 2 * core
    cross = lax.rem(t + m // 2, m)
    layers, tokens, width = xs.shape
    own, features = tok_ref.shape
    cols = box.shape[3]
    heads = cols // HD
    half, quarter = width // 2, width // 4
    count, per = tokens // CHUNK, own // CHUNK
    scale = HD ** (-0.5)
    at_end = (me == 0) | (me == n - 1)
    ends = (n - 1, 0)
    lanes = span(core * half, half)
    other = span((1 - core) * half, half)
    mine_q = core * half + side * quarter
    their_q = core * half + (1 - side) * quarter
    places = (me, n - 1 - me)
    afters = (me + 1, me - 1)

    loaded = pltpu.make_async_copy(tok_any, tok_ref, w_sem.at[0, 4])
    loaded.start()
    weights = []
    for layer in range(layers):
        for i, (any_ref, ref) in enumerate(((wq_any, wq), (wk_any, wk), (wv_any, wv), (wo_any, wo))):
            copy = pltpu.make_async_copy(any_ref.at[layer], ref.at[layer], w_sem.at[layer, i])
            copy.start()
            weights.append(copy)
    greet(
        [("sp", lax.rem(me + k, n)) for k in range(1, n)] + [("tp", partner), ("tp", cross)]
    )
    loaded.wait()

    def rows_of(c):
        return span(c * CHUNK, CHUNK)

    def scatter(c):
        @pl.when(lax.div(c, per) == me)
        def _():
            here = span((c - me * per) * CHUNK, CHUNK)
            for k in range(1, n):
                to = jnp.where(me < n // 2, n - k + jnp.where(n - k > me, 0, -1), k - 1 + jnp.where(k > me, 1, 0))
                remote(
                    tok_ref.at[here, span(to * width + mine_q, quarter)],
                    xs.at[0, rows_of(c), span(mine_q, quarter)],
                    sp_s, sp_r.at[c], "sp", to,
                ).start()
            xs[0, rows_of(c), :] = tok_ref[here, span(me * width, width)]

    def pass_cross(c):
        @pl.when(lax.div(c, per) != me)
        def _():
            here = xs.at[0, rows_of(c), span(mine_q, quarter)]
            remote(here, here, sp_s, sp_r.at[c], "tp", cross).wait_recv()
            remote(here, here, spx_s, spx_r.at[c], "tp", cross).start()

    def pass_partner(c):
        @pl.when(lax.div(c, per) != me)
        def _():
            there = xs.at[0, rows_of(c), span(their_q, quarter)]
            remote(there, there, spx_s, spx_r.at[c], "tp", cross).wait_recv()
            here = xs.at[0, rows_of(c), lanes]
            remote(here, here, fresh_s.at[0], fresh_r.at[c], "tp", partner).start()

    def prepare(layer, c):
        rows = rows_of(c)

        def arrived():
            there = xs.at[layer, rows, other]
            remote(there, there, fresh_s.at[layer], fresh_r.at[c], "tp", partner).wait_recv()

        if layer == 0:
            pl.when(lax.div(c, per) != me)(arrived)
        else:
            arrived()
        gain = gain_ref[layer:layer + 1, span(me * width, width)].astype(jnp.float32)
        wide = xs[layer, rows, :].astype(jnp.float32)
        gained = (wide * gain).astype(jnp.bfloat16)
        for way in range(2):
            lo = (1 - way) * cols
            for j, w_ref in enumerate((wq, wk, wv)):
                part[way, rows, j * cols:(j + 1) * cols] = jnp.dot(
                    gained, w_ref[layer, :, lo:lo + cols], preferred_element_type=jnp.float32
                )

    def measure(layer, c):
        wide = xs[layer, rows_of(c), :].astype(jnp.float32)
        squares = wide * wide
        high = squares.astype(jnp.bfloat16)
        low = (squares - high.astype(jnp.float32)).astype(jnp.bfloat16)
        ones = jnp.ones((8, width), jnp.bfloat16)
        nt = (((1,), (1,)), ((), ()))
        total = lax.dot_general(
            ones, high, nt, preferred_element_type=jnp.float32
        ) + lax.dot_general(ones, low, nt, preferred_element_type=jnp.float32)
        sq_own[layer, c] = jnp.concatenate([total[:1]] * (128 // CHUNK), axis=1)
        for e, end in enumerate(ends):
            @pl.when(me != end)
            def _(e=e, end=end):
                remote(
                    sq_own.at[layer, c], sq_in.at[layer, c, me],
                    sq_s.at[layer, e], sq_r.at[c], "sp", end,
                ).start()

    pieces = [slice(i * 3 * cols // PARTS, (i + 1) * 3 * cols // PARTS) for i in range(PARTS)]

    def chain_copy(layer, way, c, i):
        rows = rows_of(c)
        return remote(
            outbox.at[layer, way, rows, pieces[i]], inbox.at[layer, way, rows, pieces[i]],
            ch_s.at[layer, way], ch_r.at[way, c, i], "sp", afters[way],
        )

    def first_link(layer, c):
        for way in range(2):
            @pl.when(places[way] == 0)
            def _(way=way):
                for i, at in enumerate(pieces):
                    outbox[layer, way, rows_of(c), at] = part[way, rows_of(c), at].astype(jnp.bfloat16)
                    chain_copy(layer, way, c, i).start()

    def link(way, layer, c):
        rows = rows_of(c)
        place = places[way]

        def total(i):
            chain_copy(layer, way, c, i).wait_recv()
            return part[way, rows, pieces[i]] + inbox[layer, way, rows, pieces[i]].astype(jnp.float32)

        @pl.when(place < n - 1)
        def _():
            for i, at in enumerate(pieces):
                outbox[layer, way, rows, at] = total(i).astype(jnp.bfloat16)
                chain_copy(layer, way, c, i).start()

        @pl.when(place == n - 1)
        def _():
            squares = sq_own[layer, c]
            others = sq_in.at[layer, c, 0:n - 1]
            remote(others, others, sq_s.at[layer, 0], sq_r.at[c], "sp", n - 1 - me).wait_recv()
            for k in range(1, n):
                squares = squares + sq_in[layer, c, lax.rem(me + k, n)]
            scaled = lax.rsqrt(squares / features + norm_eps)
            inverse = jnp.broadcast_to(scaled, (128, 128)).T[:CHUNK, :1]
            for i, at in enumerate(pieces):
                qkv[layer, rows, at] = (total(i) * inverse).astype(jnp.bfloat16)

    def make_bias(o):
        first_head = jnp.where(me == n - 1, heads, 0)
        lane = lax.broadcasted_iota(jnp.int32, (CHUNK, 2 * GRID_W), 1)
        query = lax.broadcasted_iota(jnp.int32, (CHUNK, 2 * GRID_W), 0)
        key = jnp.where(lane < GRID_W, lane, lane - GRID_W)
        begin = jnp.clip(query - KC // 2, 0, GRID_W - KC)
        inside = (key >= begin) & (key < begin + KC)
        for layer in range(layers):
            for h in range(heads):
                def rolled(i, shift, layer=layer, h=h):
                    row = padded[layer, first_head + h, pl.ds(i, 1), :]
                    return pltpu.roll(
                        jnp.broadcast_to(row, (CHUNK, 2 * GRID_W)), shift, 1, stride=1, stride_axis=0
                    )

                both = jnp.where(
                    lane < GRID_W, rolled(o, 2 * GRID_W - KC + 1), rolled(o + 1, GRID_W - KC + 1)
                )
                bias[layer, h, o] = jnp.where(inside, both, -jnp.inf)

    @pl.when(at_end)
    def _():
        padded[...] = jnp.zeros_like(padded)
        for layer in range(layers):
            for h in range(2 * heads):
                padded[layer, h, 0:2 * KR - 1, 0:2 * KC - 1] = offset_ref[layer, h]

    way_here = jnp.where(me == 0, 0, 1)
    after_here = jnp.where(me == 0, 1, n - 2)

    def direct(layer, r):
        return r < DIRECT if layer < layers - 1 else r >= count - LAST_DIRECT

    def publish(layer, r):
        here = box.at[layer, way_here, rows_of(r), :]

        def send(to):
            remote(
                here, here, at_s.at[layer, way_here], at_r.at[way_here, r], "sp", to
            ).start()

        @pl.when(direct(layer, r))
        def _():
            for k in range(n - 1, 0, -1):
                send(jnp.where(me == 0, k, n - 1 - k))

        pl.when(jnp.logical_not(direct(layer, r)))(lambda: send(after_here))

    def attend(layer, r, several=1):
        @pl.when(at_end)
        def _():
            jobs = []
            for i in range(several):
                first = jnp.clip(r + i - KR // 2, 0, count - KR)
                band = pl.ds(pl.multiple_of(first * CHUNK, CHUNK), KR * CHUNK)
                for h in range(heads):
                    at = [slice(j * cols + h * HD, j * cols + (h + 1) * HD) for j in range(3)]
                    scores = lax.dot_general(
                        qkv[layer, rows_of(r + i), at[0]], qkv[layer, band, at[1]],
                        (((1,), (1,)), ((), ())), preferred_element_type=jnp.float32,
                    )
                    a = first - r - i + KR - 1
                    table = jnp.concatenate([bias[layer, h, a + 2 * b] for b in range(KR // 2)], axis=1)
                    jobs.append((scores * scale + table, band, at[2]))
            jobs = [(jnp.exp(w - jnp.max(w, axis=-1, keepdims=True)), b, v) for w, b, v in jobs]
            outs = [
                jnp.dot(w.astype(jnp.bfloat16), qkv[layer, b, v], preferred_element_type=jnp.float32)
                / jnp.sum(w, axis=-1, keepdims=True)
                for w, b, v in jobs
            ]
            for i in range(several):
                both = jnp.concatenate(outs[i * heads:(i + 1) * heads], axis=1)
                box[layer, way_here, rows_of(r + i), :] = both.astype(jnp.bfloat16)
                publish(layer, r + i)

    def box_copy(layer, way, r):
        here = box.at[layer, way, rows_of(r), :]
        return remote(here, here, at_s.at[layer, way], at_r.at[way, r], "sp", afters[way])

    def relay(way, layer, r):
        @pl.when(jnp.logical_not(direct(layer, r)))
        def _():
            box_copy(layer, way, r).wait_recv()
            box_copy(layer, way, r).start()

    def give_copy(layer, r):
        rows = rows_of(r)
        return remote(
            give.at[layer, rows, :], take.at[layer, rows, :],
            gv_s.at[layer], gv_r.at[r], "tp", partner,
        )

    def cross_copy(layer, r, whole):
        at = slice(None) if whole else span((1 - side) * quarter, quarter)
        rows = rows_of(r)
        return remote(
            pair.at[layer, rows, at], cross_in.at[layer, rows, at],
            cr_s.at[layer], cr_r.at[layer, r], "tp", cross,
        )

    def multiply(layer, r):
        for way in range(2):
            @pl.when((places[way] == n - 1) | ((places[way] > 0) & direct(layer, r)))
            def _(way=way):
                box_copy(layer, way, r).wait_recv()
        rows = rows_of(r)

        def share(at):
            return jnp.dot(
                box[layer, 0, rows, :], wo[layer, :cols, at], preferred_element_type=jnp.float32
            ) + jnp.dot(box[layer, 1, rows, :], wo[layer, cols:, at], preferred_element_type=jnp.float32)

        give[layer, rows, :] = share(other).astype(jnp.bfloat16)
        give_copy(layer, r).start()
        pair[layer, rows, :] = share(lanes).astype(jnp.bfloat16)

    def meet(layer, r):
        rows = rows_of(r)
        give_copy(layer, r).wait_recv()
        pair[layer, rows, :] = (
            pair[layer, rows, :].astype(jnp.float32) + take[layer, rows, :].astype(jnp.float32)
        ).astype(jnp.bfloat16)
        if layer < layers - 1:
            cross_copy(layer, r, True).start()
            return
        owner = lax.div(r, per)
        pl.when(owner == me)(lambda: cross_copy(layer, r, True).start())
        pl.when(owner != me)(lambda: cross_copy(layer, r, False).start())

    def out_at(q, lane, size):
        return out_ref.at[span(q * CHUNK, CHUNK), span(lane, size)]

    def finish(layer, r):
        rows = rows_of(r)

        def new(at, sub):
            branch = pair[layer, rows, sub].astype(jnp.float32) + cross_in[layer, rows, sub].astype(jnp.float32)
            return (xs[layer, rows, at].astype(jnp.float32) + branch).astype(jnp.bfloat16)

        if layer < layers - 1:
            cross_copy(layer, r, True).wait_recv()
            here = xs.at[layer + 1, rows, lanes]
            here[...] = new(lanes, slice(None))
            remote(here, here, fresh_s.at[layer + 1], fresh_r.at[r], "tp", partner).start()
            return
        owner, q = lax.div(r, per), lax.rem(r, per)
        @pl.when(owner == me)
        def _():
            cross_copy(layer, r, True).wait_recv()
            here = out_at(q, me * width + core * half, half)
            here[...] = new(lanes, slice(None))
            remote(here, here, fp_s, fp_r, "tp", partner).start()

        @pl.when(owner != me)
        def _():
            cross_copy(layer, r, False).wait_recv()
            fin[rows, :] = new(span(mine_q, quarter), span(side * quarter, quarter))
            remote(
                fin.at[rows, :], out_at(q, me * width + mine_q, quarter),
                fin_s, fin_r.at[me, q], "sp", owner,
            ).start()

    def hand_cross(q):
        for k in range(1, n):
            source = lax.rem(me + k, n)
            here = out_at(q, source * width + mine_q, quarter)
            remote(here, here, fin_s, fin_r.at[source, q], "sp", source).wait_recv()
            remote(here, here, fx_s, fx_r.at[q], "tp", cross).start()

    def hand_partner(q):
        every = fin.at[0:(n - 1) * CHUNK, :]
        remote(every, every, fx_s, fx_r.at[q], "tp", cross).wait_recv()
        for k in range(1, n):
            source = lax.rem(me + k, n)
            here = out_at(q, source * width + core * half, half)
            remote(here, here, fp_s, fp_r, "tp", partner).start()

    through = (n - 1) * HOP - HOP_TWO
    plans = [row_plan(count, layer == layers - 1) for layer in range(layers)]
    share_at = 0
    for j, (first, size) in enumerate(plans[0]):
        for row in range(first, first + size):
            late = DIRECT_LAG if row < DIRECT else FIRST + (n - 2) * RELAY
            share_at = max(share_at, j + late - row)
    meet_at = share_at + MEET
    finish_at = meet_at + CROSS
    settle = finish_at + FRESH
    last_share = FIRST + (n - 2) * LAST_RELAY + MORE
    last_finish = last_share + MEET + CROSS
    starts = [layer * (through + KR - 1 + settle) for layer in range(layers)]
    singles = [(row, 1) for row in range(count)]
    shares = plans[-1]
    if LAST_DIRECT:
        shares = shares[:-2] + [(shares[-2][0], shares[-2][1] + shares[-1][1])]
    final = starts[-1] + through + KR - 1 + len(shares) + last_finish

    @pl.loop(-LEAD, final)
    def _(tick):
        def chunks(stage, late, layer, extra=True):
            c = tick - late - starts[layer]

            @pl.when((c >= 0) & (c < count) & extra)
            def _():
                stage(layer, c)

        def grid_rows(stage, late, layer, extra=True, plan=None, behind=None):
            j = tick - late - starts[layer] - through - (KR - 1)
            plan = plan or plans[layer]

            @pl.when((j >= 0) & (j < len(plan)) & extra)
            def _():
                if all(size == 1 for _, size in plan):
                    stage(layer, j)
                    return
                first, size = pick([p[0] for p in plan], j), pick([p[1] for p in plan], j)

                @pl.loop(first, first + size)
                def _(r):
                    stage(layer, r)
                    if behind:
                        pl.when(r > first)(lambda: behind(layer, r - 1))

                if behind:
                    behind(layer, first + size - 1)

        lead = per * me + OWN_LEAD if SPREAD == 0 else jnp.where(me == 1, LEAD, per * me + OWN_LEAD)

        def relays(low, high, which):
            for layer in which:
                for way in range(2):
                    place = places[way]
                    inner = (place >= low) & (place < high)
                    grid_rows(functools.partial(relay, way), FIRST + (place - 1) * (RELAY if layer < layers - 1 else LAST_RELAY), layer, inner)

        @pl.when(tick == 0)
        def _():
            for copy in weights:
                copy.wait()

        last = layers - 1
        if FAR == 0:
            relays(2, n - 1, [last])
        relays(1, 2, range(layers))
        if FAR == 1:
            relays(2, n - 1, range(layers))
        chunks(lambda _, c: pass_cross(c), -TURN, 0)
        for layer in range(last):
            grid_rows(finish, finish_at, layer, plan=singles)
        groups = [(i * per + a, b) for i, a, b in GROUPS]
        waits = len(shares) - len(groups)
        grid_rows(finish, last_finish + waits, last, plan=groups)
        for layer in range(layers):
            for way in range(2):
                place = places[way]
                early = (place > 0) & (place != 2) if HOP_TWO else place > 0
                chunks(functools.partial(link, way), HOP * place - jnp.where(place >= 2, HOP_TWO, 0), layer, early)
        for layer in range(layers):
            grid_rows(attend, 0, layer)
        if FAR != 1:
            relays(2, n - 1, range(last) if FAR == 0 else range(layers))
        if HOP_TWO:
            for layer in range(layers):
                for way in range(2):
                    chunks(functools.partial(link, way), 2 * HOP - HOP_TWO, layer, places[way] == 2)
        for layer in range(last):
            grid_rows(multiply, share_at, layer, plan=singles)
        grid_rows(multiply, last_share, last, plan=shares, behind=meet)
        for layer in range(layers):
            chunks(prepare, jnp.where(at_end, 0, HOP - 1), layer)
            chunks(first_link, 0, layer, at_end)
        for layer in range(last):
            grid_rows(meet, meet_at, layer, plan=singles)
        for layer in range(layers):
            chunks(measure, jnp.where(at_end, 0, HOP - 1), layer)
        chunks(lambda _, c: pass_partner(c), -PASS, 0)
        chunks(lambda _, c: scatter(c), -lead, 0)

        @pl.when((tick >= -1) & (tick < 2 * KR - 3) & at_end)
        def _():
            make_bias(tick + 1)

    pl.loop(0, per)(hand_cross)

    @pl.loop(0, per)
    def _(q):
        hand_partner(q)

    every = xs.at[0, :, 0:half]
    remote(every, every, fp_s, fp_r, "tp", partner).wait_recv()

    def sent(ref, sem, recv):
        remote(ref, ref, sem, recv, "tp", partner).wait_send()

    away = fin.at[0:tokens - own, :]
    sent(away, sp_s, sp_r.at[0])
    sent(away, spx_s, spx_r.at[0])
    sent(away, fin_s, fin_r.at[0, 0])
    sent(away, fx_s, fx_r.at[0])
    sent(xs.at[0, :, 0:half], fp_s, fp_r)
    sent(xs.at[0, 0:tokens - own, 0:half], fresh_s.at[0], fresh_r.at[0])
    for layer in range(layers):
        if layer > 0:
            sent(xs.at[layer, :, 0:half], fresh_s.at[layer], fresh_r.at[0])
        sent(give.at[layer], gv_s.at[layer], gv_r.at[0])
        if layer < layers - 1:
            sent(pair.at[layer], cr_s.at[layer], cr_r.at[layer, 0])
        else:
            sent(fin, cr_s.at[layer], cr_r.at[layer, 0])
            sent(fin.at[0:own, :], cr_s.at[layer], cr_r.at[layer, 0])
        for way in range(2):
            @pl.when(places[way] < n - 1)
            def _(way=way):
                sent(outbox.at[layer, way], ch_s.at[layer, way], ch_r.at[way, 0, 0])
                straight = DIRECT if layer < layers - 1 else LAST_DIRECT
                sent(box.at[layer, way, straight * CHUNK:, :], at_s.at[layer, way], at_r.at[way, 0])
                if straight:
                    @pl.when(places[way] == 0)
                    def _():
                        several = box.at[layer, way, 0:(n - 1) * straight * CHUNK, :]
                        sent(several, at_s.at[layer, way], at_r.at[way, 0])

            @pl.when(me != ends[way])
            def _(way=way):
                sent(sq_own.at[layer], sq_s.at[layer, way], sq_r.at[0])


def store_kernel(mixed_ref, out_ref, sem):
    copy = pltpu.make_async_copy(mixed_ref, out_ref, sem)
    copy.start()
    copy.wait()


def staged(tokens, norm_gain, w_query, w_key, w_value, w_out, offset_bias):
    n, m = lax.axis_size("sp"), lax.axis_size("tp")
    own, features = tokens.shape
    layers = norm_gain.shape[0]
    width, total = features // n, own * n
    heads = offset_bias.shape[1] // 2
    cols = heads * HD
    count, per = total // CHUNK, own // CHUNK
    dma = pltpu.SemaphoreType.DMA
    bf16, f32 = jnp.bfloat16, jnp.float32
    space = pltpu.VMEM
    whole, anywhere = pl.BlockSpec(memory_space=space), pl.BlockSpec(memory_space=pl.ANY)
    mixed = pl.pallas_call(
        functools.partial(pipeline_kernel, n, m),
        out_shape=space((own, features), bf16),
        in_specs=[anywhere] + [whole] * 2 + [anywhere] * 4,
        out_specs=whole,
        scratch_shapes=[
            *[space(w.shape, bf16) for w in (tokens, w_query, w_key, w_value, w_out)],
            space((layers, total, width), bf16),
            space((2, total, 3 * cols), f32),
            space((layers, 2, total, 3 * cols), bf16),
            space((layers, 2, total, 3 * cols), bf16),
            space((layers, total, 3 * cols), bf16),
            space((layers, heads, 2 * KR - 2, CHUNK, 2 * GRID_W), f32),
            space((layers, count, 1, 128), f32),
            space((layers, count, n, 1, 128), f32),
            space((layers, 2, total, cols), bf16),
            *[space((layers, total, width // 2), bf16)] * 4,
            space((total, width // 4), bf16),
            space((layers, 2 * heads, 2 * KR, 2 * GRID_W), f32),
            dma((layers, 5)),
            dma, dma((count,)), dma, dma((count,)), dma((layers,)), dma((count,)),
            dma((layers, 2)), dma((2, count, PARTS)), dma((layers, 2)), dma((count,)),
            dma((layers, 2)), dma((2, count)),
            dma((layers,)), dma((count,)), dma((layers,)), dma((layers, count)),
            dma, dma((n, per)), dma, dma((per,)), dma, dma,
        ],
        compiler_params=pltpu.CompilerParams(
            collective_id=1, has_side_effects=True, vmem_limit_bytes=VMEM_MOST
        ),
        name="pipeline",
    )(tokens, norm_gain, offset_bias, w_query, w_key, w_value, w_out)
    return pl.pallas_call(
        store_kernel,
        out_shape=jax.ShapeDtypeStruct((own, features), bf16),
        in_specs=[whole],
        out_specs=anywhere,
        scratch_shapes=[dma],
        compiler_params=pltpu.CompilerParams(vmem_limit_bytes=2**20),
        name="store",
    )(mixed)


def on_device(tokens, norm_gain, w_query, w_key, w_value, w_out, offset_bias):
    n, m = lax.axis_size("sp"), lax.axis_size("tp")
    own, features = tokens.shape
    total, width = own * n, features // n
    fits = total * (20 * width + 60 * w_query.shape[2]) < VMEM_MOST
    even = offset_bias.shape[1] % 2 == 0 and m == 4 and n > 2
    if fits and even and own % CHUNK == 0 and width % 512 == 0 and total >= KR * GRID_W:
        return staged(tokens, norm_gain, w_query, w_key, w_value, w_out, offset_bias)
    return general(tokens, norm_gain, w_query, w_key, w_value, w_out, offset_bias)


def solution(mesh):
    return jax.shard_map(
        on_device,
        mesh=mesh,
        in_specs=(
            P(("grp", "sp"), None),
            P(),
            P(None, "sp", "tp"),
            P(None, "sp", "tp"),
            P(None, "sp", "tp"),
            P(None, "tp", "sp"),
            P(None, "tp", None, None),
        ),
        out_specs=P(("grp", "sp"), None),
        check_vma=False,
    )
```

```python
import functools

import jax
import jax.numpy as jnp
from jax import lax
from jax.experimental import pallas as pl
from jax.experimental.pallas import tpu as pltpu
from jax.sharding import PartitionSpec as P

HD = 128
GRID_W = 64
KR = 8
KC = 16
LAYERS = 2


norm_eps = 1e-06


def with_halo(block, sides, width):
    for axis, dim in sides:
        count = lax.axis_size(axis)
        forward = [(i, i + 1) for i in range(count - 1)]
        backward = [(target, source) for source, target in forward]
        low = lax.ppermute(
            lax.slice_in_dim(block, block.shape[dim] - width, None, axis=dim), axis, forward
        )
        high = lax.ppermute(lax.slice_in_dim(block, 0, width, axis=dim), axis, backward)
        block = jnp.concatenate([low, block, high], axis=dim)
    return block


def rms_rows(values, gain):
    wide = values.astype(jnp.float32)
    scaled = wide * lax.rsqrt(jnp.mean(wide * wide, axis=-1, keepdims=True) + norm_eps)
    return (scaled * gain.astype(jnp.float32)).astype(jnp.bfloat16)


def general(tokens, norm_gain, w_query, w_key, w_value, w_out, offset_bias):
    sp_count = lax.axis_size("sp")
    sp_index = lax.axis_index("sp")
    tok_rows = tokens.shape[0]
    local_rows = tok_rows // GRID_W
    grid_rows = local_rows * sp_count
    heads_here = offset_bias.shape[1]
    head_width = heads_here * HD
    reach = KR // 2
    scale = HD ** (-0.5)
    columns = jnp.arange(GRID_W, dtype=jnp.int32)
    col_first = jnp.clip(columns - KC // 2, 0, GRID_W - KC)
    col_inside = (columns[None, :] >= col_first[:, None]) & (
        columns[None, :] < col_first[:, None] + KC
    )
    col_offset = jnp.clip(columns[None, :] - columns[:, None], 1 - KC, KC - 1) + KC - 1
    col_onehot = (
        jnp.arange(2 * KC - 1, dtype=jnp.int32)[:, None, None] == col_offset[None, :, :]
    ).astype(jnp.float32)
    first_row = sp_index * local_rows
    own_rows = first_row + jnp.arange(local_rows, dtype=jnp.int32)
    row_first = jnp.clip(own_rows - reach, 0, grid_rows - KR)
    band_start = row_first - first_row + reach
    row_offset = (
        row_first[:, None] + jnp.arange(KR, dtype=jnp.int32)[None, :] - own_rows[:, None] + KR - 1
    )
    row_onehot = (
        row_offset[:, :, None] == jnp.arange(2 * KR - 1, dtype=jnp.int32)[None, None, :]
    ).astype(jnp.float32)
    qkv_weight = jnp.concatenate([w_query, w_key, w_value], axis=2)
    residual = lax.all_to_all(tokens, "sp", split_axis=1, concat_axis=0, tiled=True)
    width = residual.shape[1]
    features = width * sp_count
    for layer_index in range(LAYERS):
        wide = residual.astype(jnp.float32)
        squares = lax.psum_scatter(
            jnp.sum(wide * wide, axis=-1, keepdims=True), "sp", scatter_dimension=0, tiled=True
        )
        inverse = lax.rsqrt(squares / features + norm_eps)
        gain = lax.dynamic_slice_in_dim(norm_gain[layer_index], sp_index * width, width, 0)
        gained = (wide * gain.astype(jnp.float32)).astype(jnp.bfloat16)
        partial = jnp.dot(gained, qkv_weight[layer_index], preferred_element_type=jnp.float32)
        mine = lax.psum_scatter(
            partial.astype(jnp.bfloat16), "sp", scatter_dimension=0, tiled=True
        )
        mine = (mine.astype(jnp.float32) * inverse).astype(jnp.bfloat16)
        queries = mine[:, :head_width].reshape(local_rows, GRID_W, heads_here, HD)
        key_values = mine[:, head_width:].reshape(local_rows, GRID_W, 2 * head_width)
        padded = with_halo(key_values, (("sp", 0),), reach)
        bands = jax.vmap(lambda band_begin: lax.dynamic_slice_in_dim(padded, band_begin, KR, 0))(
            band_start
        )
        band_keys = bands[..., :head_width].reshape(local_rows, KR, GRID_W, heads_here, HD)
        band_values = bands[..., head_width:].reshape(local_rows, KR, GRID_W, heads_here, HD)
        col_bias = jnp.einsum(
            "hro,oqk->hrqk", offset_bias[layer_index], col_onehot, precision=lax.Precision.HIGHEST
        )
        full_bias = jnp.einsum(
            "ijr,hrqk->hiqjk", row_onehot, col_bias, precision=lax.Precision.HIGHEST
        )
        scores = jnp.einsum(
            "iqhd,ijkhd->hiqjk", queries, band_keys, preferred_element_type=jnp.float32
        )
        scores = scores * scale + full_bias
        scores = jnp.where(col_inside[None, None, :, None, :], scores, -jnp.inf)
        flattened = scores.reshape(heads_here, local_rows, GRID_W, KR * GRID_W)
        weights = jax.nn.softmax(flattened, axis=-1).astype(jnp.bfloat16)
        weights = weights.reshape(heads_here, local_rows, GRID_W, KR, GRID_W)
        attended = jnp.einsum(
            "hiqjk,ijkhd->iqhd", weights, band_values, preferred_element_type=jnp.float32
        )
        attended = attended.astype(jnp.bfloat16).reshape(tok_rows, head_width)
        every = lax.all_gather(attended, "sp", axis=0, tiled=True)
        share = jnp.dot(every, w_out[layer_index], preferred_element_type=jnp.float32)
        branch = lax.psum(share.astype(jnp.bfloat16), "tp").astype(jnp.float32)
        residual = (residual.astype(jnp.float32) + branch).astype(jnp.bfloat16)
    return lax.all_to_all(residual, "sp", split_axis=0, concat_axis=1, tiled=True)


MESH = pl.DeviceIdType.MESH
VMEM_MOST = 56 * 2**20
CHUNK = GRID_W
HOP = 2
LEAD, OWN_LEAD, TURN, PASS = 6, 4, 2, 1
PARTS = 3
FIRST, RELAY = 2, 1
MEET, CROSS, FRESH = 0, 2, 0
FAR = 1
SPREAD = 0
HOP_TWO = 0
LAST_RELAY = 1
DIRECT = 0
MORE = 0
GROUPS = [(0, 0, 8), (2, 0, 2), (2, 2, 2), (3, 0, 4)]
LAST_DIRECT = 0
DIRECT_LAG = 2


def greet(peers):
    barrier = pltpu.get_barrier_semaphore()
    for axis, index in peers:
        pl.semaphore_signal(barrier, inc=1, device_id={axis: index}, device_id_type=MESH)
    pl.semaphore_wait(barrier, len(peers))


def remote(src, dst, send, recv, axis, index):
    return pltpu.make_async_remote_copy(
        src_ref=src, dst_ref=dst, send_sem=send, recv_sem=recv,
        device_id={axis: index}, device_id_type=MESH,
    )


def span(start, size):
    return pl.ds(pl.multiple_of(start, size), size)


def row_plan(count, last):
    need = [min(max(r + KR - 1 - KR // 2, KR - 1), count - 1) - KR + 1 for r in range(count)]
    if not last and not DIRECT:
        return [(r, 1) for r in range(count)]
    if not last:
        plan, done = [], 0
        while done < count:
            ready = sum(v <= len(plan) for v in need) - done
            plan.append((done, min(ready, 2)))
            done += plan[-1][1]
        return plan
    ticks = need[-1]
    early = sum(v < ticks for v in need)
    sizes = [early // ticks + (t >= ticks - early % ticks) for t in range(ticks)] + [count - early]
    starts = [sum(sizes[:t]) for t in range(ticks + 1)]
    return list(zip(starts, sizes))


def pick(table, index):
    value = jnp.int32(table[-1])
    for i in range(len(table) - 2, -1, -1):
        value = jnp.where(index <= i, jnp.int32(table[i]), value)
    return value


def pipeline_kernel(
    n, m, tok_any, gain_ref, offset_ref, wq_any, wk_any, wv_any, wo_any, out_ref,
    tok_ref, wq, wk, wv, wo, xs, part, outbox, inbox, qkv, bias, sq_own, sq_in, box,
    give, take, pair, cross_in, fin, padded,
    w_sem, sp_s, sp_r, spx_s, spx_r, fresh_s, fresh_r, ch_s, ch_r, sq_s, sq_r,
    at_s, at_r, gv_s, gv_r, cr_s, cr_r, fin_s, fin_r, fx_s, fx_r, fp_s, fp_r,
):
    me, t = lax.axis_index("sp"), lax.axis_index("tp")
    core = lax.rem(t, 2)
    side = lax.div(t, 2)
    partner = t + 1 - 2 * core
    cross = lax.rem(t + m // 2, m)
    layers, tokens, width = xs.shape
    own, features = tok_ref.shape
    cols = box.shape[3]
    heads = cols // HD
    half, quarter = width // 2, width // 4
    count, per = tokens // CHUNK, own // CHUNK
    scale = HD ** (-0.5)
    at_end = (me == 0) | (me == n - 1)
    ends = (n - 1, 0)
    lanes = span(core * half, half)
    other = span((1 - core) * half, half)
    mine_q = core * half + side * quarter
    their_q = core * half + (1 - side) * quarter
    places = (me, n - 1 - me)
    afters = (me + 1, me - 1)

    loaded = pltpu.make_async_copy(tok_any, tok_ref, w_sem.at[0, 4])
    loaded.start()
    weights = []
    for layer in range(layers):
        for i, (any_ref, ref) in enumerate(((wq_any, wq), (wk_any, wk), (wv_any, wv), (wo_any, wo))):
            copy = pltpu.make_async_copy(any_ref.at[layer], ref.at[layer], w_sem.at[layer, i])
            copy.start()
            weights.append(copy)
    greet(
        [("sp", lax.rem(me + k, n)) for k in range(1, n)] + [("tp", partner), ("tp", cross)]
    )
    loaded.wait()

    def rows_of(c):
        return span(c * CHUNK, CHUNK)

    def scatter(c):
        @pl.when(lax.div(c, per) == me)
        def _():
            here = span((c - me * per) * CHUNK, CHUNK)
            for k in range(1, n):
                to = jnp.where(me < n // 2, n - k + jnp.where(n - k > me, 0, -1), k - 1 + jnp.where(k > me, 1, 0))
                remote(
                    tok_ref.at[here, span(to * width + mine_q, quarter)],
                    xs.at[0, rows_of(c), span(mine_q, quarter)],
                    sp_s, sp_r.at[c], "sp", to,
                ).start()
            xs[0, rows_of(c), :] = tok_ref[here, span(me * width, width)]

    def pass_cross(c):
        @pl.when(lax.div(c, per) != me)
        def _():
            here = xs.at[0, rows_of(c), span(mine_q, quarter)]
            remote(here, here, sp_s, sp_r.at[c], "tp", cross).wait_recv()
            remote(here, here, spx_s, spx_r.at[c], "tp", cross).start()

    def pass_partner(c):
        @pl.when(lax.div(c, per) != me)
        def _():
            there = xs.at[0, rows_of(c), span(their_q, quarter)]
            remote(there, there, spx_s, spx_r.at[c], "tp", cross).wait_recv()
            here = xs.at[0, rows_of(c), lanes]
            remote(here, here, fresh_s.at[0], fresh_r.at[c], "tp", partner).start()

    def prepare(layer, c):
        rows = rows_of(c)

        def arrived():
            there = xs.at[layer, rows, other]
            remote(there, there, fresh_s.at[layer], fresh_r.at[c], "tp", partner).wait_recv()

        if layer == 0:
            pl.when(lax.div(c, per) != me)(arrived)
        else:
            arrived()
        gain = gain_ref[layer:layer + 1, span(me * width, width)].astype(jnp.float32)
        wide = xs[layer, rows, :].astype(jnp.float32)
        gained = (wide * gain).astype(jnp.bfloat16)
        for way in range(2):
            lo = (1 - way) * cols
            for j, w_ref in enumerate((wq, wk, wv)):
                part[way, rows, j * cols:(j + 1) * cols] = jnp.dot(
                    gained, w_ref[layer, :, lo:lo + cols], preferred_element_type=jnp.float32
                )

    def measure(layer, c):
        wide = xs[layer, rows_of(c), :].astype(jnp.float32)
        squares = wide * wide
        high = squares.astype(jnp.bfloat16)
        low = (squares - high.astype(jnp.float32)).astype(jnp.bfloat16)
        ones = jnp.ones((8, width), jnp.bfloat16)
        nt = (((1,), (1,)), ((), ()))
        total = lax.dot_general(
            ones, high, nt, preferred_element_type=jnp.float32
        ) + lax.dot_general(ones, low, nt, preferred_element_type=jnp.float32)
        sq_own[layer, c] = jnp.concatenate([total[:1]] * (128 // CHUNK), axis=1)
        for e, end in enumerate(ends):
            @pl.when(me != end)
            def _(e=e, end=end):
                remote(
                    sq_own.at[layer, c], sq_in.at[layer, c, me],
                    sq_s.at[layer, e], sq_r.at[c], "sp", end,
                ).start()

    pieces = [slice(i * 3 * cols // PARTS, (i + 1) * 3 * cols // PARTS) for i in range(PARTS)]

    def chain_copy(layer, way, c, i):
        rows = rows_of(c)
        return remote(
            outbox.at[layer, way, rows, pieces[i]], inbox.at[layer, way, rows, pieces[i]],
            ch_s.at[layer, way], ch_r.at[way, c, i], "sp", afters[way],
        )

    def first_link(layer, c):
        for way in range(2):
            @pl.when(places[way] == 0)
            def _(way=way):
                for i, at in enumerate(pieces):
                    outbox[layer, way, rows_of(c), at] = part[way, rows_of(c), at].astype(jnp.bfloat16)
                    chain_copy(layer, way, c, i).start()

    def link(way, layer, c):
        rows = rows_of(c)
        place = places[way]

        def total(i):
            chain_copy(layer, way, c, i).wait_recv()
            return part[way, rows, pieces[i]] + inbox[layer, way, rows, pieces[i]].astype(jnp.float32)

        @pl.when(place < n - 1)
        def _():
            for i, at in enumerate(pieces):
                outbox[layer, way, rows, at] = total(i).astype(jnp.bfloat16)
                chain_copy(layer, way, c, i).start()

        @pl.when(place == n - 1)
        def _():
            squares = sq_own[layer, c]
            others = sq_in.at[layer, c, 0:n - 1]
            remote(others, others, sq_s.at[layer, 0], sq_r.at[c], "sp", n - 1 - me).wait_recv()
            for k in range(1, n):
                squares = squares + sq_in[layer, c, lax.rem(me + k, n)]
            scaled = lax.rsqrt(squares / features + norm_eps)
            inverse = jnp.broadcast_to(scaled, (128, 128)).T[:CHUNK, :1]
            for i, at in enumerate(pieces):
                qkv[layer, rows, at] = (total(i) * inverse).astype(jnp.bfloat16)

    def make_bias(o):
        first_head = jnp.where(me == n - 1, heads, 0)
        lane = lax.broadcasted_iota(jnp.int32, (CHUNK, 2 * GRID_W), 1)
        query = lax.broadcasted_iota(jnp.int32, (CHUNK, 2 * GRID_W), 0)
        key = jnp.where(lane < GRID_W, lane, lane - GRID_W)
        begin = jnp.clip(query - KC // 2, 0, GRID_W - KC)
        inside = (key >= begin) & (key < begin + KC)
        for layer in range(layers):
            for h in range(heads):
                def rolled(i, shift, layer=layer, h=h):
                    row = padded[layer, first_head + h, pl.ds(i, 1), :]
                    return pltpu.roll(
                        jnp.broadcast_to(row, (CHUNK, 2 * GRID_W)), shift, 1, stride=1, stride_axis=0
                    )

                both = jnp.where(
                    lane < GRID_W, rolled(o, 2 * GRID_W - KC + 1), rolled(o + 1, GRID_W - KC + 1)
                )
                bias[layer, h, o] = jnp.where(inside, both, -jnp.inf)

    @pl.when(at_end)
    def _():
        padded[...] = jnp.zeros_like(padded)
        for layer in range(layers):
            for h in range(2 * heads):
                padded[layer, h, 0:2 * KR - 1, 0:2 * KC - 1] = offset_ref[layer, h]

    way_here = jnp.where(me == 0, 0, 1)
    after_here = jnp.where(me == 0, 1, n - 2)

    def direct(layer, r):
        return r < DIRECT if layer < layers - 1 else r >= count - LAST_DIRECT

    def publish(layer, r):
        here = box.at[layer, way_here, rows_of(r), :]

        def send(to):
            remote(
                here, here, at_s.at[layer, way_here], at_r.at[way_here, r], "sp", to
            ).start()

        @pl.when(direct(layer, r))
        def _():
            for k in range(n - 1, 0, -1):
                send(jnp.where(me == 0, k, n - 1 - k))

        pl.when(jnp.logical_not(direct(layer, r)))(lambda: send(after_here))

    def attend(layer, r, several=1):
        @pl.when(at_end)
        def _():
            jobs = []
            for i in range(several):
                first = jnp.clip(r + i - KR // 2, 0, count - KR)
                band = pl.ds(pl.multiple_of(first * CHUNK, CHUNK), KR * CHUNK)
                for h in range(heads):
                    at = [slice(j * cols + h * HD, j * cols + (h + 1) * HD) for j in range(3)]
                    scores = lax.dot_general(
                        qkv[layer, rows_of(r + i), at[0]], qkv[layer, band, at[1]],
                        (((1,), (1,)), ((), ())), preferred_element_type=jnp.float32,
                    )
                    a = first - r - i + KR - 1
                    table = jnp.concatenate([bias[layer, h, a + 2 * b] for b in range(KR // 2)], axis=1)
                    jobs.append((scores * scale + table, band, at[2]))
            jobs = [(jnp.exp(w - jnp.max(w, axis=-1, keepdims=True)), b, v) for w, b, v in jobs]
            outs = [
                jnp.dot(w.astype(jnp.bfloat16), qkv[layer, b, v], preferred_element_type=jnp.float32)
                / jnp.sum(w, axis=-1, keepdims=True)
                for w, b, v in jobs
            ]
            for i in range(several):
                both = jnp.concatenate(outs[i * heads:(i + 1) * heads], axis=1)
                box[layer, way_here, rows_of(r + i), :] = both.astype(jnp.bfloat16)
                publish(layer, r + i)

    def box_copy(layer, way, r):
        here = box.at[layer, way, rows_of(r), :]
        return remote(here, here, at_s.at[layer, way], at_r.at[way, r], "sp", afters[way])

    def relay(way, layer, r):
        @pl.when(jnp.logical_not(direct(layer, r)))
        def _():
            box_copy(layer, way, r).wait_recv()
            box_copy(layer, way, r).start()

    def give_copy(layer, r):
        rows = rows_of(r)
        return remote(
            give.at[layer, rows, :], take.at[layer, rows, :],
            gv_s.at[layer], gv_r.at[r], "tp", partner,
        )

    def cross_copy(layer, r, whole):
        at = slice(None) if whole else span((1 - side) * quarter, quarter)
        rows = rows_of(r)
        return remote(
            pair.at[layer, rows, at], cross_in.at[layer, rows, at],
            cr_s.at[layer], cr_r.at[layer, r], "tp", cross,
        )

    def multiply(layer, r):
        for way in range(2):
            @pl.when((places[way] == n - 1) | ((places[way] > 0) & direct(layer, r)))
            def _(way=way):
                box_copy(layer, way, r).wait_recv()
        rows = rows_of(r)

        def share(at):
            return jnp.dot(
                box[layer, 0, rows, :], wo[layer, :cols, at], preferred_element_type=jnp.float32
            ) + jnp.dot(box[layer, 1, rows, :], wo[layer, cols:, at], preferred_element_type=jnp.float32)

        give[layer, rows, :] = share(other).astype(jnp.bfloat16)
        give_copy(layer, r).start()
        pair[layer, rows, :] = share(lanes).astype(jnp.bfloat16)

    def meet(layer, r):
        rows = rows_of(r)
        give_copy(layer, r).wait_recv()
        pair[layer, rows, :] = (
            pair[layer, rows, :].astype(jnp.float32) + take[layer, rows, :].astype(jnp.float32)
        ).astype(jnp.bfloat16)
        if layer < layers - 1:
            cross_copy(layer, r, True).start()
            return
        owner = lax.div(r, per)
        pl.when(owner == me)(lambda: cross_copy(layer, r, True).start())
        pl.when(owner != me)(lambda: cross_copy(layer, r, False).start())

    def out_at(q, lane, size):
        return out_ref.at[span(q * CHUNK, CHUNK), span(lane, size)]

    def finish(layer, r):
        rows = rows_of(r)

        def new(at, sub):
            branch = pair[layer, rows, sub].astype(jnp.float32) + cross_in[layer, rows, sub].astype(jnp.float32)
            return (xs[layer, rows, at].astype(jnp.float32) + branch).astype(jnp.bfloat16)

        if layer < layers - 1:
            cross_copy(layer, r, True).wait_recv()
            here = xs.at[layer + 1, rows, lanes]
            here[...] = new(lanes, slice(None))
            remote(here, here, fresh_s.at[layer + 1], fresh_r.at[r], "tp", partner).start()
            return
        owner, q = lax.div(r, per), lax.rem(r, per)
        @pl.when(owner == me)
        def _():
            cross_copy(layer, r, True).wait_recv()
            here = out_at(q, me * width + core * half, half)
            here[...] = new(lanes, slice(None))
            remote(here, here, fp_s, fp_r, "tp", partner).start()

        @pl.when(owner != me)
        def _():
            cross_copy(layer, r, False).wait_recv()
            fin[rows, :] = new(span(mine_q, quarter), span(side * quarter, quarter))
            remote(
                fin.at[rows, :], out_at(q, me * width + mine_q, quarter),
                fin_s, fin_r.at[me, q], "sp", owner,
            ).start()

    def hand_cross(q):
        for k in range(1, n):
            source = lax.rem(me + k, n)
            here = out_at(q, source * width + mine_q, quarter)
            remote(here, here, fin_s, fin_r.at[source, q], "sp", source).wait_recv()
            remote(here, here, fx_s, fx_r.at[q], "tp", cross).start()

    def hand_partner(q):
        every = fin.at[0:(n - 1) * CHUNK, :]
        remote(every, every, fx_s, fx_r.at[q], "tp", cross).wait_recv()
        for k in range(1, n):
            source = lax.rem(me + k, n)
            here = out_at(q, source * width + core * half, half)
            remote(here, here, fp_s, fp_r, "tp", partner).start()

    through = (n - 1) * HOP - HOP_TWO
    plans = [row_plan(count, layer == layers - 1) for layer in range(layers)]
    share_at = 0
    for j, (first, size) in enumerate(plans[0]):
        for row in range(first, first + size):
            late = DIRECT_LAG if row < DIRECT else FIRST + (n - 2) * RELAY
            share_at = max(share_at, j + late - row)
    meet_at = share_at + MEET
    finish_at = meet_at + CROSS
    settle = finish_at + FRESH
    last_share = FIRST + (n - 2) * LAST_RELAY + MORE
    last_finish = last_share + MEET + CROSS
    starts = [layer * (through + KR - 1 + settle) for layer in range(layers)]
    singles = [(row, 1) for row in range(count)]
    shares = plans[-1]
    if LAST_DIRECT:
        shares = shares[:-2] + [(shares[-2][0], shares[-2][1] + shares[-1][1])]
    final = starts[-1] + through + KR - 1 + len(shares) + last_finish

    @pl.loop(-LEAD, final)
    def _(tick):
        def chunks(stage, late, layer, extra=True):
            c = tick - late - starts[layer]

            @pl.when((c >= 0) & (c < count) & extra)
            def _():
                stage(layer, c)

        def grid_rows(stage, late, layer, extra=True, plan=None, behind=None):
            j = tick - late - starts[layer] - through - (KR - 1)
            plan = plan or plans[layer]

            @pl.when((j >= 0) & (j < len(plan)) & extra)
            def _():
                if all(size == 1 for _, size in plan):
                    stage(layer, j)
                    return
                first, size = pick([p[0] for p in plan], j), pick([p[1] for p in plan], j)

                @pl.loop(first, first + size)
                def _(r):
                    stage(layer, r)
                    if behind:
                        pl.when(r > first)(lambda: behind(layer, r - 1))

                if behind:
                    behind(layer, first + size - 1)

        lead = per * me + OWN_LEAD if SPREAD == 0 else jnp.where(me == 1, LEAD, per * me + OWN_LEAD)

        def relays(low, high, which):
            for layer in which:
                for way in range(2):
                    place = places[way]
                    inner = (place >= low) & (place < high)
                    grid_rows(functools.partial(relay, way), FIRST + (place - 1) * (RELAY if layer < layers - 1 else LAST_RELAY), layer, inner)

        @pl.when(tick == 0)
        def _():
            for copy in weights:
                copy.wait()

        last = layers - 1
        if FAR == 0:
            relays(2, n - 1, [last])
        relays(1, 2, range(layers))
        if FAR == 1:
            relays(2, n - 1, range(layers))
        chunks(lambda _, c: pass_cross(c), -TURN, 0)
        for layer in range(last):
            grid_rows(finish, finish_at, layer, plan=singles)
        groups = [(i * per + a, b) for i, a, b in GROUPS]
        waits = len(shares) - len(groups)
        grid_rows(finish, last_finish + waits, last, plan=groups)
        for layer in range(layers):
            for way in range(2):
                place = places[way]
                early = (place > 0) & (place != 2) if HOP_TWO else place > 0
                chunks(functools.partial(link, way), HOP * place - jnp.where(place >= 2, HOP_TWO, 0), layer, early)
        for layer in range(layers):
            grid_rows(attend, 0, layer)
        if FAR != 1:
            relays(2, n - 1, range(last) if FAR == 0 else range(layers))
        if HOP_TWO:
            for layer in range(layers):
                for way in range(2):
                    chunks(functools.partial(link, way), 2 * HOP - HOP_TWO, layer, places[way] == 2)
        for layer in range(last):
            grid_rows(multiply, share_at, layer, plan=singles)
        grid_rows(multiply, last_share, last, plan=shares, behind=meet)
        for layer in range(layers):
            chunks(prepare, jnp.where(at_end, 0, HOP - 1), layer)
            chunks(first_link, 0, layer, at_end)
        for layer in range(last):
            grid_rows(meet, meet_at, layer, plan=singles)
        chunks(lambda _, c: pass_partner(c), -PASS, 0)
        chunks(lambda _, c: scatter(c), -lead, 0)

        @pl.when((tick >= -1) & (tick < 2 * KR - 3) & at_end)
        def _():
            make_bias(tick + 1)

        for layer in range(layers):
            chunks(measure, jnp.where(at_end, 0, HOP - 1), layer)

    pl.loop(0, per)(hand_cross)

    @pl.loop(0, per)
    def _(q):
        hand_partner(q)

    every = xs.at[0, :, 0:half]
    remote(every, every, fp_s, fp_r, "tp", partner).wait_recv()

    def sent(ref, sem, recv):
        remote(ref, ref, sem, recv, "tp", partner).wait_send()

    away = fin.at[0:tokens - own, :]
    sent(away, sp_s, sp_r.at[0])
    sent(away, spx_s, spx_r.at[0])
    sent(away, fin_s, fin_r.at[0, 0])
    sent(away, fx_s, fx_r.at[0])
    sent(xs.at[0, :, 0:half], fp_s, fp_r)
    sent(xs.at[0, 0:tokens - own, 0:half], fresh_s.at[0], fresh_r.at[0])
    for layer in range(layers):
        if layer > 0:
            sent(xs.at[layer, :, 0:half], fresh_s.at[layer], fresh_r.at[0])
        sent(give.at[layer], gv_s.at[layer], gv_r.at[0])
        if layer < layers - 1:
            sent(pair.at[layer], cr_s.at[layer], cr_r.at[layer, 0])
        else:
            sent(fin, cr_s.at[layer], cr_r.at[layer, 0])
            sent(fin.at[0:own, :], cr_s.at[layer], cr_r.at[layer, 0])
        for way in range(2):
            @pl.when(places[way] < n - 1)
            def _(way=way):
                sent(outbox.at[layer, way], ch_s.at[layer, way], ch_r.at[way, 0, 0])
                straight = DIRECT if layer < layers - 1 else LAST_DIRECT
                sent(box.at[layer, way, straight * CHUNK:, :], at_s.at[layer, way], at_r.at[way, 0])
                if straight:
                    @pl.when(places[way] == 0)
                    def _():
                        several = box.at[layer, way, 0:(n - 1) * straight * CHUNK, :]
                        sent(several, at_s.at[layer, way], at_r.at[way, 0])

            @pl.when(me != ends[way])
            def _(way=way):
                sent(sq_own.at[layer], sq_s.at[layer, way], sq_r.at[0])


def store_kernel(mixed_ref, out_ref, sem):
    copy = pltpu.make_async_copy(mixed_ref, out_ref, sem)
    copy.start()
    copy.wait()


def staged(tokens, norm_gain, w_query, w_key, w_value, w_out, offset_bias):
    n, m = lax.axis_size("sp"), lax.axis_size("tp")
    own, features = tokens.shape
    layers = norm_gain.shape[0]
    width, total = features // n, own * n
    heads = offset_bias.shape[1] // 2
    cols = heads * HD
    count, per = total // CHUNK, own // CHUNK
    dma = pltpu.SemaphoreType.DMA
    bf16, f32 = jnp.bfloat16, jnp.float32
    space = pltpu.VMEM
    whole, anywhere = pl.BlockSpec(memory_space=space), pl.BlockSpec(memory_space=pl.ANY)
    mixed = pl.pallas_call(
        functools.partial(pipeline_kernel, n, m),
        out_shape=space((own, features), bf16),
        in_specs=[anywhere] + [whole] * 2 + [anywhere] * 4,
        out_specs=whole,
        scratch_shapes=[
            *[space(w.shape, bf16) for w in (tokens, w_query, w_key, w_value, w_out)],
            space((layers, total, width), bf16),
            space((2, total, 3 * cols), f32),
            space((layers, 2, total, 3 * cols), bf16),
            space((layers, 2, total, 3 * cols), bf16),
            space((layers, total, 3 * cols), bf16),
            space((layers, heads, 2 * KR - 2, CHUNK, 2 * GRID_W), f32),
            space((layers, count, 1, 128), f32),
            space((layers, count, n, 1, 128), f32),
            space((layers, 2, total, cols), bf16),
            *[space((layers, total, width // 2), bf16)] * 4,
            space((total, width // 4), bf16),
            space((layers, 2 * heads, 2 * KR, 2 * GRID_W), f32),
            dma((layers, 5)),
            dma, dma((count,)), dma, dma((count,)), dma((layers,)), dma((count,)),
            dma((layers, 2)), dma((2, count, PARTS)), dma((layers, 2)), dma((count,)),
            dma((layers, 2)), dma((2, count)),
            dma((layers,)), dma((count,)), dma((layers,)), dma((layers, count)),
            dma, dma((n, per)), dma, dma((per,)), dma, dma,
        ],
        compiler_params=pltpu.CompilerParams(
            collective_id=1, has_side_effects=True, vmem_limit_bytes=VMEM_MOST
        ),
        name="pipeline",
    )(tokens, norm_gain, offset_bias, w_query, w_key, w_value, w_out)
    return pl.pallas_call(
        store_kernel,
        out_shape=jax.ShapeDtypeStruct((own, features), bf16),
        in_specs=[whole],
        out_specs=anywhere,
        scratch_shapes=[dma],
        compiler_params=pltpu.CompilerParams(vmem_limit_bytes=2**20),
        name="store",
    )(mixed)


def on_device(tokens, norm_gain, w_query, w_key, w_value, w_out, offset_bias):
    n, m = lax.axis_size("sp"), lax.axis_size("tp")
    own, features = tokens.shape
    total, width = own * n, features // n
    fits = total * (20 * width + 60 * w_query.shape[2]) < VMEM_MOST
    even = offset_bias.shape[1] % 2 == 0 and m == 4 and n > 2
    if fits and even and own % CHUNK == 0 and width % 512 == 0 and total >= KR * GRID_W:
        return staged(tokens, norm_gain, w_query, w_key, w_value, w_out, offset_bias)
    return general(tokens, norm_gain, w_query, w_key, w_value, w_out, offset_bias)


def solution(mesh):
    return jax.shard_map(
        on_device,
        mesh=mesh,
        in_specs=(
            P(("grp", "sp"), None),
            P(),
            P(None, "sp", "tp"),
            P(None, "sp", "tp"),
            P(None, "sp", "tp"),
            P(None, "tp", "sp"),
            P(None, "tp", None, None),
        ),
        out_specs=P(("grp", "sp"), None),
        check_vma=False,
    )
```
